32 devices in a mesh: ep: 8 (over z, y), tp: 4 (over x, core).
Axes of the slice: x: 2, y: 2, z: 4, core: 2. Of those that a mesh axis runs over, the one named last changes fastest.
Arguments:
- queries: bfloat16 [1536, 2048], P('ep', 'tp'), may hold values from -8 to 8
- keys: bfloat16 [1536, 512], P('ep', 'tp'), may hold values from -8 to 8
- values: bfloat16 [1536, 512], P('ep', 'tp'), may hold values from -6 to 6
- query_gain: float32 [2048], P('tp'), may hold values from 0.5 to 6
- key_gain: float32 [512], P('tp'), may hold values from 0.7 to 6
- out_weight: bfloat16 [2048, 4096], P('tp'), may hold values from -0.125 to 0.125
- expert_input: bfloat16 [2048, 4096], P(('ep', 'tp')), may hold values from -6 to 6
- norm_gain: float32 [4096], replicated, may hold values from 0.1 to 1.9
- routes: int32 [2048, 2], P(('ep', 'tp')), may hold values from 0 to 7, all different within a row; in each aligned block of 64 rows (0 to 63, 64 to 127, ...) at most 32 rows name the same one
- route_weight: float32 [2048, 2], P(('ep', 'tp')), may hold values from 0.2 to 2
- gate_weight: bfloat16 [8, 4096, 1024], P('ep', None, 'tp'), may hold values from -0.09375 to 0.09375
- up_weight: bfloat16 [8, 4096, 1024], P('ep', None, 'tp'), may hold values from -0.09375 to 0.09375
- down_weight: bfloat16 [8, 1024, 4096], P('ep', 'tp'), may hold values from -0.1875 to 0.1875
Outputs:
- mixed: bfloat16 [1536, 4096], P(('ep', 'tp'))
- moe_out: bfloat16 [2048, 4096], P(('ep', 'tp'))
The draws below stay inside these ranges and needn't reach their ends.
Inputs may be any that keep to these rules, and one draw needn't show every extreme that they name: `routes`: each row names 2 different experts; in the rows of one device no expert is named by more than 32 rows, and in some device one expert is named by exactly 32 rows.
All inputs are finite; a program needn't handle non-finite values.
Results may differ from the reference program's by a relative error of at most 0.013.
The reference program's roundings to bfloat16 on the way count: a program that leaves them out, or rounds other values in their place, can miss the bound.
Values may be sent and summed in bfloat16 or wider, within the bound.
A program may use at most 128 MiB of HBM per device.

```python
import math
import jax
import jax.numpy as jnp
import numpy as np
from jax import lax

D = 4096
HEADS = 32
KV_HEADS = 8
HEAD_DIM = 64
EXPERT_WIDTH = 1024
TOP = 2
GRID_W = 128
TOK_EXP = 64
TOKENS = 1536
EXP_TOKENS = 2048
EXPERTS = 8
CAP = 32
N_EP = 8
N_TP = 4


def attention_fields(key):
    base = jax.random.fold_in(key, 911)
    subkeys = jax.random.split(base, 6)
    query_level = jnp.exp(jax.random.uniform(subkeys[0], (HEADS,), jnp.float32, 0.0, math.log(2.2)))
    key_level = jnp.exp(jax.random.uniform(subkeys[1], (KV_HEADS,), jnp.float32, 0.0, math.log(2.2)))
    query_gain = jnp.repeat(query_level, HEAD_DIM) * jax.random.uniform(subkeys[2], (HEADS * HEAD_DIM,), jnp.float32, 0.7, 1.3)
    key_gain = jnp.repeat(key_level, HEAD_DIM) * jax.random.uniform(subkeys[3], (KV_HEADS * HEAD_DIM,), jnp.float32, 0.7, 1.3)
    queries = jnp.clip(jax.random.normal(subkeys[4], (TOKENS, HEADS * HEAD_DIM), jnp.float32), -6.0, 6.0)
    keys = jnp.clip(jax.random.normal(subkeys[5], (TOKENS, KV_HEADS * HEAD_DIM), jnp.float32), -6.0, 6.0)
    return (queries, keys, query_gain, key_gain)


def draw_queries(key, part):
    return attention_fields(key)[0].astype(jnp.bfloat16)


def draw_keys(key, part):
    return attention_fields(key)[1].astype(jnp.bfloat16)


def draw_query_gain(key, part):
    return attention_fields(key)[2].astype(jnp.float32)


def draw_key_gain(key, part):
    return attention_fields(key)[3].astype(jnp.float32)


def shard_levels(key, shape, shards, least, largest):
    def one(position, shards_of):
        steps = jax.random.uniform(jax.random.fold_in(jax.random.fold_in(key, 6), position), (shards_of,), jnp.float32, least / len(shards), largest / len(shards))
        return jnp.repeat(jnp.exp(steps), shape[position] // shards_of).reshape((-1,) + (1,) * (len(shape) - position - 1))

    level = one(*shards[0])
    for cut in shards[1:]:
        level = level * one(*cut)
    return level


def routed_block(rng, own, number, rows, number_of, top, reach, lean):
    ranking = jax.random.permutation(rng, number_of)
    heavy_load, common = portions_of(number_of, rows * top, reach, lean, True), portions_of(number_of, rows * top, reach, lean, False)
    places = jnp.arange(number_of)

    def named(lengths, turn):
        used = int((lengths > 0).sum())
        fixed = max(1, used // 4)
        shifted = fixed + (places - fixed + turn * (used - fixed)) % max(1, number_of - fixed)
        return jnp.zeros((number_of,), jnp.int32).at[ranking[jnp.where(places < fixed, places, shifted)]].set(jnp.asarray(lengths, jnp.int32))

    lengths = jnp.where(number % 4 == 0, named(heavy_load, number // 4), named(common, number - number // 4 - 1))
    mixed = jax.random.permutation(jax.random.fold_in(own, 3), number_of)
    source_of, receiver = mixed[0:number_of // 2 * 2:2], mixed[1:number_of // 2 * 2:2]
    slack = jnp.minimum(lengths[source_of] - 1, reach - lengths[receiver]) // 2
    slack = jnp.where((source_of == ranking[0]) | (receiver == ranking[0]) | (lengths[receiver] == 0), 0, jnp.maximum(slack, 0))
    shifted = jax.random.randint(jax.random.fold_in(own, 4), (number_of // 2,), 0, 1 << 20) % (slack + 1)
    lengths = lengths.at[source_of].add(-shifted).at[receiver].add(shifted)
    labels = jnp.searchsorted(jnp.cumsum(lengths), jnp.arange(rows * top), side="right").astype(jnp.int32)
    grid = labels.reshape(top, rows).T
    grid = grid[jax.random.permutation(jax.random.fold_in(own, 1), rows)]
    turn = jax.random.randint(jax.random.fold_in(own, 2), (rows, 1), 0, top)
    return jnp.take_along_axis(grid, (jnp.arange(top)[None, :] + turn) % top, axis=1)


def portions_of(number_of, total, reach, slope, full):
    weights = [(1 << 20) // math.isqrt(standing ** slope) + 1 for standing in range(1, number_of + 1)]
    largest = reach if full else min(reach, max(-(-total // number_of), total * weights[0] // sum(weights)))
    least = 1 if total - largest >= number_of - 1 else 0
    given, rest = [largest] + [least] * (number_of - 1), total - largest - least * (number_of - 1)
    while rest > 0:
        movable = [i for i in range(1, number_of) if given[i] < largest] or [i for i in range(1, number_of) if given[i] < reach]
        mass, budget = sum([weights[i] for i in movable]), rest
        for i in movable:
            extra = min(reach - given[i], max(1, budget * weights[i] // mass), rest)
            given[i] = given[i] + extra
            rest = rest - extra
    return np.array(given)


def normal_values(rng, extent, scale, reach, shards=(), kind=jnp.bfloat16):
    values = scale * jax.random.normal(rng, extent, jnp.float32)
    if shards:
        values = values * shard_levels(rng, extent, shards, -0.22, 0.18)
    return jnp.clip(values, -reach, reach).astype(kind)


def setup_inputs(seed: int = 0) -> dict:
    arg_keys = jax.random.split(jax.random.key(seed), 14)
    queries = draw_queries(jax.random.fold_in(arg_keys[13], 71), 0)
    keys = draw_keys(jax.random.fold_in(arg_keys[13], 71), 0)
    values = normal_values(arg_keys[2], (TOKENS, KV_HEADS * HEAD_DIM), 1.0, 6.0, ((0, 8), (1, 4)))
    query_gain = draw_query_gain(jax.random.fold_in(arg_keys[13], 71), 0)
    key_gain = draw_key_gain(jax.random.fold_in(arg_keys[13], 71), 0)
    out_weight = normal_values(arg_keys[5], (HEADS * HEAD_DIM, D), (HEADS * HEAD_DIM) ** -0.5, 0.125, ((0, 4),))
    expert_input = normal_values(arg_keys[6], (EXP_TOKENS, D), 1.0, 6.0, ((0, 32),))
    norm_gain = jnp.clip(1.0 + 0.18 * jax.random.normal(arg_keys[7], (D,), jnp.float32), 0.1, 1.9)
    routes_keys = jax.random.split(jax.random.fold_in(arg_keys[8], 1), EXP_TOKENS // TOK_EXP)
    routes_turns = jax.random.permutation(jax.random.fold_in(arg_keys[8], 3), EXP_TOKENS // TOK_EXP)
    routes = jax.vmap(lambda own, number: routed_block(jax.random.fold_in(arg_keys[8], 2), own, number, TOK_EXP, EXPERTS, TOP, CAP, 2))(routes_keys, routes_turns).reshape((EXP_TOKENS, TOP))
    route_weight = jnp.clip(jnp.exp(math.log(2.0) - 2.3025851 * jax.random.uniform(arg_keys[9], (EXP_TOKENS, TOP), jnp.float32) ** shard_levels(arg_keys[9], (EXP_TOKENS, TOP), ((0, 32),), -0.2, 0.2)), 0.2, 2.0)
    gate_weight = normal_values(arg_keys[10], (EXPERTS, D, EXPERT_WIDTH), D ** -0.5, 0.09375, ((0, 8), (2, 4)))
    up_weight = normal_values(arg_keys[11], (EXPERTS, D, EXPERT_WIDTH), D ** -0.5, 0.09375, ((0, 8), (2, 4)))
    down_weight = normal_values(arg_keys[12], (EXPERTS, EXPERT_WIDTH, D), EXPERT_WIDTH ** -0.5, 0.1875, ((0, 8), (1, 4)))
    return {"queries": queries, "keys": keys, "values": values, "query_gain": query_gain, "key_gain": key_gain, "out_weight": out_weight, "expert_input": expert_input, "norm_gain": norm_gain, "routes": routes, "route_weight": route_weight, "gate_weight": gate_weight, "up_weight": up_weight, "down_weight": down_weight}


NORM_EPS = 1e-06
ROPE_BASE = 10000.0

def round_trip(matrix):
    return lax.optimization_barrier(matrix.astype(jnp.bfloat16)).astype(jnp.float32)

def rotate(vectors, grid_rows, grid_cols):
    quarter = vectors.shape[-1] // 4
    inverse = ROPE_BASE ** (-jnp.arange(quarter, dtype=jnp.float32) / quarter)
    angle_row = grid_rows[:, None] * inverse
    angle_col = grid_cols[:, None] * inverse
    angles = jnp.concatenate([angle_row, angle_row, angle_col, angle_col], axis=-1)[:, None, :]
    part_one, part_two, part_three, part_four = jnp.split(vectors, 4, axis=-1)
    turned = jnp.concatenate([-part_two, part_one, -part_four, part_three], axis=-1)
    return vectors * jnp.cos(angles) + turned * jnp.sin(angles)

def head_norm(raw_rows, gains, head_count, offset):
    row_count = raw_rows.shape[0]
    flat_rows = raw_rows.astype(jnp.float32).reshape(row_count, head_count, -1)
    unit_vec = flat_rows * lax.rsqrt(lax.optimization_barrier(jnp.mean(flat_rows * flat_rows, axis=-1, keepdims=True)) + NORM_EPS)
    unit_vec = unit_vec * gains.reshape(head_count, -1)
    places = offset + jnp.arange(row_count, dtype=jnp.int32)
    grid_rows = (places // GRID_W).astype(jnp.float32)
    grid_cols = (places % GRID_W).astype(jnp.float32)
    return rotate(unit_vec, grid_rows, grid_cols).astype(jnp.bfloat16)

def attend_block(query_block, key_head, value_head, score_scale):
    scores = jnp.einsum('qgd,kd->gqk', query_block.astype(jnp.float32), key_head.astype(jnp.float32)) * score_scale
    row_max = lax.optimization_barrier(jnp.max(scores, axis=-1, keepdims=True))
    weights = jnp.exp(scores - row_max)
    weight_sum = lax.optimization_barrier(jnp.sum(weights, axis=-1))
    rounded = round_trip(weights)
    summed = jnp.einsum('gqk,kd->qgd', rounded, value_head.astype(jnp.float32))
    return (summed / jnp.transpose(weight_sum)[:, :, None]).astype(jnp.bfloat16)

def attention(q_turned, k_turned, values):
    tokens = q_turned.shape[0]
    group_size = HEADS // KV_HEADS
    query_span = math.gcd(tokens, 256)
    score_scale = HEAD_DIM ** (-0.5)
    query_heads = q_turned.reshape(tokens // query_span, query_span, KV_HEADS, group_size, HEAD_DIM)
    query_heads = jnp.transpose(query_heads, (2, 0, 1, 3, 4))
    key_heads = jnp.transpose(k_turned.reshape(tokens, KV_HEADS, HEAD_DIM), (1, 0, 2))
    value_heads = jnp.transpose(values.reshape(tokens, KV_HEADS, HEAD_DIM), (1, 0, 2))

    def per_head(operands):
        query_blocks, key_head, value_head = operands

        def per_block(query_block):
            return attend_block(query_block, key_head, value_head, score_scale)
        return lax.map(per_block, query_blocks)
    attended = lax.map(per_head, (query_heads, key_heads, value_heads))
    return jnp.transpose(attended, (1, 2, 0, 3, 4)).reshape(tokens, HEADS * HEAD_DIM)

def routed_experts(expert_input, norm_gain, routes, route_weight, gate_weight, up_weight, down_weight):
    row_count = expert_input.shape[0]
    as_float = expert_input.astype(jnp.float32)
    normed = (as_float * lax.rsqrt(lax.optimization_barrier(jnp.mean(as_float * as_float, axis=-1, keepdims=True)) + NORM_EPS) * norm_gain).astype(jnp.bfloat16)
    flat_routes = routes.reshape(-1).astype(jnp.int32)
    flat_weight = route_weight.reshape(-1)
    sorted_ids = jnp.argsort(flat_routes, stable=True).astype(jnp.int32)
    counts = lax.optimization_barrier(jnp.sum((flat_routes[:, None] == jnp.arange(EXPERTS, dtype=jnp.int32)[None, :]).astype(jnp.int32), axis=0)).astype(jnp.int32)
    starts = (jnp.cumsum(counts) - counts).astype(jnp.int32)
    most_rows = N_EP * N_TP * CAP
    padded = jnp.concatenate([sorted_ids, jnp.zeros((most_rows,), jnp.int32)])
    part_width = EXPERT_WIDTH // N_TP

    def one_expert(combined, expert_id):
        picked = lax.dynamic_slice(padded, (starts[expert_id],), (most_rows,))
        is_live = jnp.arange(most_rows, dtype=jnp.int32) < counts[expert_id]
        token_ids = (picked // TOP).astype(jnp.int32)
        gathered = normed[token_ids]
        gate_out = jnp.dot(gathered, gate_weight[expert_id], preferred_element_type=jnp.float32)
        up_out = jnp.dot(gathered, up_weight[expert_id], preferred_element_type=jnp.float32)
        hidden = (jax.nn.silu(gate_out) * up_out).astype(jnp.bfloat16)
        down_one = down_weight[expert_id]
        result = jnp.zeros((most_rows, D), jnp.float32)
        for part_id in range(N_TP):
            partial_value = jnp.dot(hidden[:, part_id * part_width:(part_id + 1) * part_width], down_one[part_id * part_width:(part_id + 1) * part_width], preferred_element_type=jnp.float32)
            result = result + round_trip(partial_value)
        result = round_trip(result)
        scaled = jnp.where(is_live[:, None], result * flat_weight[picked][:, None], 0.0)
        return (combined.at[token_ids].add(scaled), None)
    combined, unused = lax.scan(one_expert, jnp.zeros((row_count, D), jnp.float32), jnp.arange(EXPERTS, dtype=jnp.int32))
    return combined.astype(jnp.bfloat16)

def reference(queries, keys, values, query_gain, key_gain, out_weight, expert_input, norm_gain, routes, route_weight, gate_weight, up_weight, down_weight):
    q_turned = head_norm(queries, query_gain, HEADS, 0)
    k_turned = head_norm(keys, key_gain, KV_HEADS, 0)
    attended = attention(q_turned, k_turned, values)
    tokens = attended.shape[0]
    part_width = HEADS * HEAD_DIM // N_TP
    mixed_sum = jnp.zeros((tokens, D), jnp.float32)
    for part_id in range(N_TP):
        partial_value = jnp.dot(attended[:, part_id * part_width:(part_id + 1) * part_width], out_weight[part_id * part_width:(part_id + 1) * part_width], preferred_element_type=jnp.float32)
        mixed_sum = mixed_sum + round_trip(partial_value)
    mixed = mixed_sum.astype(jnp.bfloat16)
    moe_out = routed_experts(expert_input, norm_gain, routes, route_weight, gate_weight, up_weight, down_weight)
    return (mixed, moe_out)
```

```python
import functools

import jax
import jax.numpy as jnp
import numpy as np
from jax import lax
from jax.experimental import pallas as pl
from jax.experimental.pallas import tpu as pltpu
from jax.sharding import PartitionSpec as P

HEAD_DIM = 64
GRID_W = 128


NORM_EPS = 1e-06
ROPE_BASE = 10000.0


def rotate(vectors, grid_rows, grid_cols):
    quarter = vectors.shape[-1] // 4
    inverse = ROPE_BASE ** (-jnp.arange(quarter, dtype=jnp.float32) / quarter)
    angle_row = grid_rows[:, None] * inverse
    angle_col = grid_cols[:, None] * inverse
    angles = jnp.concatenate([angle_row, angle_row, angle_col, angle_col], axis=-1)[:, None, :]
    part_one, part_two, part_three, part_four = jnp.split(vectors, 4, axis=-1)
    turned = jnp.concatenate([-part_two, part_one, -part_four, part_three], axis=-1)
    return vectors * jnp.cos(angles) + turned * jnp.sin(angles)


def head_norm(raw_rows, gains, head_count, offset):
    row_count = raw_rows.shape[0]
    flat_rows = raw_rows.astype(jnp.float32).reshape(row_count, head_count, -1)
    unit_vec = flat_rows * lax.rsqrt(
        jnp.mean(flat_rows * flat_rows, axis=-1, keepdims=True) + NORM_EPS
    )
    unit_vec = unit_vec * gains.reshape(head_count, -1)
    places = offset + jnp.arange(row_count, dtype=jnp.int32)
    grid_rows = (places // GRID_W).astype(jnp.float32)
    grid_cols = (places % GRID_W).astype(jnp.float32)
    return rotate(unit_vec, grid_rows, grid_cols).astype(jnp.bfloat16).reshape(row_count, -1)


def absorb(running, key_block, value_block, grouped, score_scale):
    run_max, weight_sum, summed = running
    kv_count = grouped.shape[1]
    key_heads = key_block.reshape(key_block.shape[0], kv_count, -1)
    value_heads = value_block.reshape(value_block.shape[0], kv_count, -1)
    scores = (
        jnp.einsum("qhgd,khd->hgqk", grouped, key_heads, preferred_element_type=jnp.float32)
        * score_scale
    )
    new_max = jnp.maximum(run_max, jnp.max(scores, axis=-1))
    rescale = jnp.exp(run_max - new_max)
    weights = jnp.exp(scores - new_max[..., None])
    weight_sum = weight_sum * rescale + jnp.sum(weights, axis=-1)
    update = jnp.einsum(
        "hgqk,khd->qhgd",
        weights.astype(jnp.bfloat16),
        value_heads,
        preferred_element_type=jnp.float32,
    )
    summed = summed * jnp.transpose(rescale, (2, 0, 1))[..., None] + update
    return (new_max, weight_sum, summed)


def run_experts(sending, gate_weight, up_weight, down_weight):
    arrived = lax.all_to_all(sending, "ep", split_axis=0, concat_axis=0, tiled=True)
    shard_rows = lax.all_gather(arrived, "tp", axis=0, tiled=True)
    gate_out = jnp.dot(shard_rows, gate_weight[0], preferred_element_type=jnp.float32)
    up_out = jnp.dot(shard_rows, up_weight[0], preferred_element_type=jnp.float32)
    hidden = (jax.nn.silu(gate_out) * up_out).astype(jnp.bfloat16)
    results = lax.psum_scatter(
        jnp.dot(hidden, down_weight[0], preferred_element_type=jnp.float32).astype(jnp.bfloat16),
        "tp",
        scatter_dimension=0,
        tiled=True,
    )
    return lax.all_to_all(results, "ep", split_axis=0, concat_axis=0, tiled=True)


MESH = pl.DeviceIdType.MESH
TILE = 1024


def flip(index, pattern, size):
    result = 0
    bit = 1
    while bit < size:
        both = lax.rem(lax.div(index, bit) + lax.div(pattern, bit), 2)
        result = result + both * bit
        bit = bit * 2
    return result


def fused_kernel(
    n,
    x_ref,
    x_gain,
    routes_row,
    routes_col,
    weight_col,
    q_raw,
    k_raw,
    v_raw,
    q_gain,
    k_gain,
    turn_hbm,
    wg_hbm,
    wu_hbm,
    wd_hbm,
    ow_hbm,
    moe,
    mixed,
    laid,
    back,
    total,
    q_ref,
    kv_ref,
    turn,
    wg,
    wu,
    wd,
    ow,
    rows,
    partial,
    red,
    q_send,
    x_got,
    y_send,
    kv_all,
    attended,
    m_part,
    m_red,
    m_send,
    m_got,
    load_sem,
    kv_sems,
    disp_sems,
    fwd_sems,
    red_sems,
    ret_sems,
    mix_sems,
):
    e = lax.axis_index("ep")
    t = lax.axis_index("tp")
    side = lax.div(t, 2)
    core = lax.rem(t, 2)
    other_side = 1 - side
    other_core = 1 - core
    x_peer = (e, other_side * 2 + core)
    c_peer = (e, side * 2 + other_core)
    cap, width = laid.shape[1], laid.shape[2]
    pairs = attended.shape[0]
    tok = attended.shape[1]

    def remote(src, dst, send, recv, device):
        return pltpu.make_async_remote_copy(
            src_ref=src, dst_ref=dst, send_sem=send, recv_sem=recv, device_id=device, device_id_type=MESH
        )

    loads = [
        pltpu.make_async_copy(a, b, load_sem.at[k])
        for k, (a, b) in enumerate(
            [
                (ow_hbm, ow),
                (wg_hbm, wg),
                (wu_hbm, wu),
                (wd_hbm, wd),
                (turn_hbm.at[pl.ds(pl.multiple_of(e * tok, 8), tok)], turn),
            ]
        )
    ]
    for load in loads:
        load.start()

    barrier = pltpu.get_barrier_semaphore()
    for s in range(1, n):
        pl.semaphore_signal(barrier, inc=1, device_id=(flip(e, s, n), t), device_id_type=MESH)
    pl.semaphore_signal(barrier, inc=1, device_id=x_peer, device_id_type=MESH)
    pl.semaphore_signal(barrier, inc=1, device_id=c_peer, device_id_type=MESH)

    tokens_here = x_ref.shape[0]
    as_float = x_ref[...].astype(jnp.float32)
    mean = jnp.mean(as_float * as_float, axis=1, keepdims=True)
    normed = (as_float * lax.rsqrt(mean + NORM_EPS) * x_gain[...]).astype(jnp.bfloat16)
    row_id = lax.broadcasted_iota(jnp.int32, (tokens_here, tokens_here), 0)
    col_id = lax.broadcasted_iota(jnp.int32, (tokens_here, tokens_here), 1)
    before = (row_id < col_id).astype(jnp.bfloat16)
    after = (col_id < row_id).astype(jnp.bfloat16)

    def place(expert):
        hit = jnp.logical_or(routes_row[0:1] == expert, routes_row[1:2] == expert)
        spread = jnp.broadcast_to(hit.astype(jnp.float32), (cap, tokens_here))
        rank = jnp.dot(spread.astype(jnp.bfloat16), before, preferred_element_type=jnp.float32)
        slot = lax.broadcasted_iota(jnp.int32, rank.shape, 0).astype(jnp.float32)
        return (jnp.where(rank == slot, 1.0, 0.0) * spread).astype(jnp.bfloat16)

    def pick(expert):
        hits = [(routes_col[:, k:k + 1] == expert).astype(jnp.float32) for k in range(routes_col.shape[1])]
        scale = sum(hit * weight_col[:, k:k + 1] for k, hit in enumerate(hits))
        spread = jnp.broadcast_to(sum(hits), (tokens_here, cap))
        rank = jnp.dot(after, spread.astype(jnp.bfloat16), preferred_element_type=jnp.float32)
        slot = lax.broadcasted_iota(jnp.int32, rank.shape, 1).astype(jnp.float32)
        return (jnp.where(rank == slot, 1.0, 0.0) * spread).astype(jnp.bfloat16), scale

    def lay(expert):
        chosen = place(expert)
        for tile in range(0, width, TILE):
            laid[expert, :, tile:tile + TILE] = jnp.dot(
                chosen, normed[:, tile:tile + TILE], preferred_element_type=jnp.float32
            ).astype(jnp.bfloat16)

    lay(e)
    pl.semaphore_wait(barrier, n + 1)

    def kv_direct(s):
        return remote(kv_ref, kv_all.at[:, e], kv_sems.at[0, s], kv_sems.at[1, s], (flip(e, s, n), t))

    def kv_direct_in(s):
        return remote(kv_ref, kv_all.at[:, flip(e, s, n)], kv_sems.at[0, s], kv_sems.at[1, s], (flip(e, s, n), t))

    def kv_relay(s):
        owner = flip(e, s, n)
        return remote(kv_all.at[:, owner], kv_all.at[:, owner], kv_sems.at[0, s + 1], kv_sems.at[1, s + 1], (flip(e, 1, n), t))

    def kv_relay_in(s):
        owner = flip(e, s + 1, n)
        return remote(kv_all.at[:, owner], kv_all.at[:, owner], kv_sems.at[0, s + 1], kv_sems.at[1, s + 1], (flip(e, 1, n), t))

    order = [0, 1] + sorted(range(2, n), key=lambda s: (s < 4, s % 2, -s))

    def pattern(i):
        chosen = order[0]
        for place in range(1, n):
            chosen = jnp.where(i == place, order[place], chosen)
        return chosen

    def dispatch(i):
        s = pattern(i)
        return remote(laid.at[flip(e, s, n)], rows.at[e, t], disp_sems.at[0, i], disp_sems.at[1, i], (flip(e, s, n), t))

    def dispatch_in(i):
        s = pattern(i)
        return remote(laid.at[flip(e, s, n)], rows.at[flip(e, s, n), t], disp_sems.at[0, i], disp_sems.at[1, i], (flip(e, s, n), t))

    def owner_of(i):
        return flip(e, pattern(i), n)

    def to_side(i):
        o = owner_of(i)
        return remote(rows.at[o, t], rows.at[o, t], fwd_sems.at[0, 0, i], fwd_sems.at[1, 0, i], x_peer)

    def from_side(i):
        o = owner_of(i)
        return remote(rows.at[o, t], rows.at[o, other_side * 2 + core], fwd_sems.at[0, 0, i], fwd_sems.at[1, 0, i], x_peer)

    def to_core(i):
        o = owner_of(i)
        return remote(rows.at[o, t], rows.at[o, t], fwd_sems.at[0, 1, i], fwd_sems.at[1, 1, i], c_peer)

    def from_core(i):
        o = owner_of(i)
        return remote(rows.at[o, t], rows.at[o, side * 2 + other_core], fwd_sems.at[0, 1, i], fwd_sems.at[1, 1, i], c_peer)

    def relay_core(i):
        o = owner_of(i)
        slot = other_side * 2 + core
        return remote(rows.at[o, slot], rows.at[o, slot], fwd_sems.at[0, 2, i], fwd_sems.at[1, 2, i], c_peer)

    def relayed_core(i):
        o = owner_of(i)
        slot = other_side * 2 + core
        return remote(rows.at[o, slot], rows.at[o, other_side * 2 + other_core], fwd_sems.at[0, 2, i], fwd_sems.at[1, 2, i], c_peer)

    def reduce_core(i):
        return remote(partial.at[i, :, other_core], red.at[i], red_sems.at[0, 0, i], red_sems.at[1, 0, i], c_peer)

    def reduce_side(i):
        return remote(q_send.at[i], x_got.at[i], red_sems.at[0, 1, i], red_sems.at[1, 1, i], x_peer)

    def give_back(i):
        o = owner_of(i)
        return remote(y_send.at[i], back.at[e], ret_sems.at[0, i], ret_sems.at[1, i], (o, t))

    def get_back(i):
        o = owner_of(i)
        return remote(y_send.at[i], back.at[o], ret_sems.at[0, i], ret_sems.at[1, i], (o, t))

    mix_core = remote(m_part.at[:, other_core], m_red, mix_sems.at[0, 0], mix_sems.at[1, 0], c_peer)
    mix_side = remote(m_send, m_got, mix_sems.at[0, 1], mix_sems.at[1, 1], x_peer)

    own = pltpu.make_async_copy(laid.at[e], rows.at[e, t], load_sem.at[5])
    own_kv = pltpu.make_async_copy(kv_ref, kv_all.at[:, e], load_sem.at[6])
    own.start()
    for i in range(1, n):
        lay(flip(e, order[i], n))
        dispatch(i).start()
    own.wait()
    to_side(0).start()
    to_core(0).start()

    loads[4].wait()
    lane = lax.broadcasted_iota(jnp.int32, (tok, 128), 1)
    low = lane < HEAD_DIM
    even = lax.rem(lax.div(lane, HEAD_DIM // 4), 2) == 0
    table = turn[...]
    swapped = pltpu.roll(table, HEAD_DIM, 1)
    cosine = jnp.where(low, table, swapped)
    sine = jnp.where(low, swapped, table)

    def turned(raw, gain):
        flat = raw.astype(jnp.float32)
        square = flat * flat
        left = jnp.sum(jnp.where(low, square, 0.0), axis=1, keepdims=True)
        right = jnp.sum(jnp.where(low, 0.0, square), axis=1, keepdims=True)
        mean_square = jnp.where(low, left, right) * (1.0 / HEAD_DIM)
        unit = flat * lax.rsqrt(mean_square + NORM_EPS) * gain
        partner = jnp.where(
            even, -pltpu.roll(unit, 128 - HEAD_DIM // 4, 1), pltpu.roll(unit, HEAD_DIM // 4, 1)
        )
        return unit * cosine + partner * sine

    for pair in range(kv_ref.shape[0] // 2):
        span = slice(pair * 128, (pair + 1) * 128)
        k_rows = turned(k_raw[:, span], k_gain[:, span])
        v_rows = v_raw[:, span].astype(jnp.float32)
        kv_ref[2 * pair] = jnp.where(low, k_rows, pltpu.roll(v_rows, HEAD_DIM, 1)).astype(jnp.bfloat16)
        kv_ref[2 * pair + 1] = jnp.where(low, pltpu.roll(k_rows, HEAD_DIM, 1), v_rows).astype(jnp.bfloat16)
    own_kv.start()
    for s in range(2, n, 2):
        kv_direct(s).start()
    kv_direct(1).start()

    for pair in range(pairs):
        span = slice(pair * 128, (pair + 1) * 128)
        q_rows = turned(q_raw[:, span], q_gain[:, span])
        q_ref[2 * pair] = jnp.where(low, q_rows, 0.0).astype(jnp.bfloat16)
        q_ref[2 * pair + 1] = jnp.where(low, pltpu.roll(q_rows, HEAD_DIM, 1), 0.0).astype(jnp.bfloat16)
    own_kv.wait()

    def attend(pair):
        kv = kv_all[lax.div(pair * 2 * kv_all.shape[0], pairs * 2)].reshape(n * tok, 128)
        halves = []
        for h in range(2):
            scores = lax.dot_general(
                q_ref[pair * 2 + h], kv, (((1,), (1,)), ((), ())), preferred_element_type=jnp.float32
            ) * (HEAD_DIM ** (-0.5))
            peak = jnp.max(scores, axis=1, keepdims=True)
            weights = jnp.exp(scores - peak)
            total = jnp.sum(weights, axis=1, keepdims=True)
            summed = jnp.dot(weights.astype(jnp.bfloat16), kv, preferred_element_type=jnp.float32)
            halves.append(summed / total)
        joined = jnp.where(low, pltpu.roll(halves[0], HEAD_DIM, 1), halves[1])
        attended[pair] = joined.astype(jnp.bfloat16)

    def f32(value):
        return value.astype(jnp.float32)

    def gather(expert, first):
        chosen, scale = pick(expert)
        for tile in range(0, width, TILE):
            span = slice(tile, tile + TILE)
            found = jnp.dot(chosen, back[expert, :, span], preferred_element_type=jnp.float32) * scale
            total[:, span] = found if first else total[:, span] + found

    def step(i, carry):
        @pl.when(jnp.logical_and(i > 0, i < n))
        def _():
            dispatch_in(i).wait_recv()
            to_side(i).start()
            to_core(i).start()

        @pl.when(i == 6)
        def _():
            for s in range(2, n, 2):
                kv_direct_in(s).wait_recv()
                kv_relay(s).start()

        @pl.when(jnp.logical_and(i >= 1, i <= n))
        def _():
            from_side(i - 1).wait_recv()
            relay_core(i - 1).start()

        @pl.when(i == 7)
        def _():
            kv_direct_in(1).wait_recv()
            for s in range(2, n, 2):
                kv_relay_in(s).wait_recv()

        @pl.when(jnp.logical_and(i >= 7, i < 7 + pairs // 2))
        def _():
            attend(2 * (i - 7))
            attend(2 * (i - 7) + 1)

        @pl.when(i == 7 + pairs // 2)
        def _():
            loads[0].wait()
            for tile in range(0, width, TILE):
                product = jnp.dot(attended[0], ow[0, :, tile:tile + TILE], preferred_element_type=jnp.float32)
                for p in range(1, pairs):
                    product += jnp.dot(attended[p], ow[p, :, tile:tile + TILE], preferred_element_type=jnp.float32)
                m_part[:, :, :, tile:tile + TILE] = product.astype(jnp.bfloat16).reshape(2, 2, tok // 4, TILE)
            mix_core.start()

        @pl.when(jnp.logical_and(i >= 1, i <= n))
        def _():
            k = i - 1

            @pl.when(k == 0)
            def _():
                for load in loads[1:4]:
                    load.wait()

            from_core(k).wait_recv()
            relayed_core(k).wait_recv()
            tokens = rows[owner_of(k)].reshape(4 * cap, width)
            gate = jnp.dot(tokens, wg[...], preferred_element_type=jnp.float32)
            up = jnp.dot(tokens, wu[...], preferred_element_type=jnp.float32)
            hidden = (gate / (1.0 + jnp.exp(-gate)) * up).astype(jnp.bfloat16)
            for tile in range(0, width, TILE):
                product = jnp.dot(hidden, wd[:, tile:tile + TILE], preferred_element_type=jnp.float32)
                partial[k, :, :, :, tile:tile + TILE] = product.astype(jnp.bfloat16).reshape(2, 2, cap, TILE)
            reduce_core(k).start()

        @pl.when(i == 7 + pairs // 2)
        def _():
            mix_core.wait_recv()
            m_send[...] = (f32(m_part[other_side, core]) + f32(m_red[other_side])).astype(jnp.bfloat16)
            mix_side.start()

        @pl.when(jnp.logical_and(i >= 2, i < n + 2))
        def _():
            k = i - 2
            reduce_side(k).wait_recv()
            y = (f32(partial[k, side, core]) + f32(red[k, side]) + f32(x_got[k])).astype(jnp.bfloat16)

            @pl.when(k == 0)
            def _():
                back[e] = y
                gather(e, True)

            @pl.when(k > 0)
            def _():
                y_send[k] = y
                give_back(k).start()

        @pl.when(jnp.logical_and(i >= 1, i <= n))
        def _():
            k = i - 1
            reduce_core(k).wait_recv()
            q_send[k] = (f32(partial[k, other_side, core]) + f32(red[k, other_side])).astype(jnp.bfloat16)
            reduce_side(k).start()

        @pl.when(i >= 5)
        def _():
            k = i - 4
            get_back(k).wait_recv()
            gather(owner_of(k), False)

        return carry

    lax.fori_loop(0, n + 4, step, 0)
    moe[...] = total[...].astype(jnp.bfloat16)

    mix_side.wait_recv()
    mixed[...] = (f32(m_part[side, core]) + f32(m_red[side]) + f32(m_got[...])).astype(jnp.bfloat16)
    mix_core.wait_send()
    mix_side.wait_send()
    for s in range(2, n, 2):
        kv_direct(s).wait_send()
        kv_relay(s).wait_send()
    kv_direct(1).wait_send()

    def drain(i, carry):
        @pl.when(i > 0)
        def _():
            dispatch(i).wait_send()
            give_back(i).wait_send()

        to_side(i).wait_send()
        to_core(i).wait_send()
        relay_core(i).wait_send()
        reduce_core(i).wait_send()
        reduce_side(i).wait_send()
        return carry

    lax.fori_loop(0, n, drain, 0)


def turn_table(tokens):
    quarter = HEAD_DIM // 4
    inverse = np.power(ROPE_BASE, -np.arange(quarter, dtype=np.float64) / quarter)
    places = np.arange(tokens)
    row = (places // GRID_W)[:, None] * inverse
    col = (places % GRID_W)[:, None] * inverse
    angles = np.concatenate([row, row, col, col], axis=1)
    return np.concatenate([np.cos(angles), np.sin(angles)], axis=1).astype(np.float32)


def fused(x, x_gain, routes, route_weight, queries, keys, values, q_gain, k_gain, gate_weight, up_weight, down_weight, out_weight):
    n = lax.axis_size("ep")
    tok_exp, width = x.shape
    cap = 2 * routes.shape[1] * tok_exp // n
    tok = queries.shape[0]
    heads = queries.shape[1] // HEAD_DIM
    kv_count = keys.shape[1] // HEAD_DIM
    pairs = heads // 2
    hidden = gate_weight.shape[1]
    bf = jnp.bfloat16
    vmem = pl.BlockSpec(memory_space=pltpu.VMEM)
    anywhere = pl.BlockSpec(memory_space=pl.ANY)
    dma = pltpu.SemaphoreType.DMA
    return pl.pallas_call(
        functools.partial(fused_kernel, n),
        out_shape=(
            jax.ShapeDtypeStruct((tok_exp, width), bf),
            jax.ShapeDtypeStruct((tok // 4, width), bf),
        ),
        in_specs=[vmem] * 10 + [anywhere] * 5,
        out_specs=(vmem, vmem),
        scratch_shapes=[
            pltpu.VMEM((n, cap, width), bf),
            pltpu.VMEM((n, cap, width), bf),
            pltpu.VMEM((tok_exp, width), jnp.float32),
            pltpu.VMEM((heads, tok, 128), bf),
            pltpu.VMEM((kv_count, tok, 128), bf),
            pltpu.VMEM((tok, 128), jnp.float32),
            pltpu.VMEM((width, hidden), bf),
            pltpu.VMEM((width, hidden), bf),
            pltpu.VMEM((hidden, width), bf),
            pltpu.VMEM((pairs, 128, width), bf),
            pltpu.VMEM((n, 4, cap, width), bf),
            pltpu.VMEM((n, 2, 2, cap, width), bf),
            pltpu.VMEM((n, 2, cap, width), bf),
            pltpu.VMEM((n, cap, width), bf),
            pltpu.VMEM((n, cap, width), bf),
            pltpu.VMEM((n, cap, width), bf),
            pltpu.VMEM((kv_count, n, tok, 128), bf),
            pltpu.VMEM((pairs, tok, 128), bf),
            pltpu.VMEM((2, 2, tok // 4, width), bf),
            pltpu.VMEM((2, tok // 4, width), bf),
            pltpu.VMEM((tok // 4, width), bf),
            pltpu.VMEM((tok // 4, width), bf),
            dma((7,)),
            dma((2, n)),
            dma((2, n)),
            dma((2, 3, n)),
            dma((2, 2, n)),
            dma((2, n)),
            dma((2, 2)),
        ],
        compiler_params=pltpu.CompilerParams(
            collective_id=0, has_side_effects=True, vmem_limit_bytes=62 * 1024 * 1024
        ),
    )(
        x,
        x_gain.reshape(1, width),
        jnp.transpose(routes),
        routes,
        route_weight,
        queries,
        keys,
        values,
        q_gain.reshape(1, -1),
        k_gain.reshape(1, -1),
        jnp.asarray(turn_table(n * tok)),
        gate_weight,
        up_weight,
        down_weight,
        out_weight.reshape(pairs, 128, width),
    )


def plain_shards(
    queries,
    keys,
    values,
    query_gain,
    key_gain,
    out_weight,
    expert_input,
    norm_gain,
    routes,
    route_weight,
    gate_weight,
    up_weight,
    down_weight,
):
    tok_mix = queries.shape[0]
    head_count = query_gain.shape[0] // HEAD_DIM
    kv_count = key_gain.shape[0] // HEAD_DIM
    group_size = head_count // kv_count
    offset = lax.axis_index("ep") * tok_mix
    q_turned = head_norm(queries, query_gain, head_count, offset)
    k_turned = head_norm(keys, key_gain, kv_count, offset)
    grouped = q_turned.reshape(tok_mix, kv_count, group_size, HEAD_DIM)
    score_scale = HEAD_DIM ** (-0.5)
    start_state = (
        jnp.full((kv_count, group_size, tok_mix), -jnp.inf, jnp.float32),
        jnp.zeros((kv_count, group_size, tok_mix), jnp.float32),
        jnp.zeros((tok_mix, kv_count, group_size, HEAD_DIM), jnp.float32),
    )
    running = start_state
    key_piece = lax.all_gather(k_turned, "ep", axis=0, tiled=True)
    value_piece = lax.all_gather(values, "ep", axis=0, tiled=True)
    length = key_piece.shape[0]
    block_len = length
    while block_len > 2048 and block_len % 2 == 0:
        block_len = block_len // 2
    key_blocks = key_piece.reshape(length // block_len, block_len, key_piece.shape[1])
    value_blocks = value_piece.reshape(length // block_len, block_len, value_piece.shape[1])

    def advance(inner_state, key_value):
        return (absorb(inner_state, key_value[0], key_value[1], grouped, score_scale), None)

    running, unused = lax.scan(advance, running, (key_blocks, value_blocks))
    final_max, weight_sum, summed = running
    attended = (
        (summed / jnp.transpose(weight_sum, (2, 0, 1))[..., None])
        .reshape(tok_mix, -1)
        .astype(jnp.bfloat16)
    )
    mixed = lax.psum_scatter(
        jnp.dot(attended, out_weight, preferred_element_type=jnp.float32).astype(jnp.bfloat16),
        "tp",
        scatter_dimension=0,
        tiled=True,
    )
    tok_exp = expert_input.shape[0]
    top_count = routes.shape[1]
    expert_count = lax.axis_size("ep")
    capacity = 2 * top_count * tok_exp // expert_count
    as_float = expert_input.astype(jnp.float32)
    normed = (
        as_float
        * lax.rsqrt(jnp.mean(as_float * as_float, axis=-1, keepdims=True) + NORM_EPS)
        * norm_gain
    ).astype(jnp.bfloat16)
    flat_routes = routes.reshape(-1)
    route_hits = (
        flat_routes[:, None] == jnp.arange(expert_count, dtype=jnp.int32)[None, :]
    ).astype(jnp.int32)
    slot_rank = jnp.sum((jnp.cumsum(route_hits, axis=0) - route_hits) * route_hits, axis=1)
    slot_ids = flat_routes * capacity + slot_rank
    placed = jnp.arange(expert_count * capacity, dtype=jnp.int32)[:, None] == slot_ids[None, :]
    placed = jnp.any(placed.reshape(expert_count * capacity, tok_exp, top_count), axis=2).astype(
        jnp.bfloat16
    )
    outbound = jnp.dot(placed, normed, preferred_element_type=jnp.float32).astype(jnp.bfloat16)
    model_width = outbound.shape[1]
    half_cap = capacity // 2
    laid = outbound.reshape(expert_count, capacity, model_width)
    first_half = run_experts(
        laid[:, :half_cap].reshape(expert_count * half_cap, model_width),
        gate_weight,
        up_weight,
        down_weight,
    )
    second_half = run_experts(
        laid[:, half_cap:].reshape(expert_count * half_cap, model_width),
        gate_weight,
        up_weight,
        down_weight,
    )
    back_rows = jnp.concatenate(
        [
            first_half.reshape(expert_count, half_cap, model_width),
            second_half.reshape(expert_count, half_cap, model_width),
        ],
        axis=1,
    )
    back_rows = back_rows.reshape(expert_count * capacity, model_width)
    picked = back_rows[slot_ids.reshape(tok_exp, top_count)]
    moe_out = jnp.sum(picked.astype(jnp.float32) * route_weight[:, :, None], axis=1).astype(
        jnp.bfloat16
    )
    return (mixed, moe_out)


def shards(
    queries,
    keys,
    values,
    query_gain,
    key_gain,
    out_weight,
    expert_input,
    norm_gain,
    routes,
    route_weight,
    gate_weight,
    up_weight,
    down_weight,
):
    tok_exp = expert_input.shape[0]
    top_count = routes.shape[1]
    expert_count = lax.axis_size("ep")
    capacity = 2 * top_count * tok_exp // expert_count
    if capacity % 16 != 0 or lax.axis_size("tp") != 4:
        return plain_shards(
            queries,
            keys,
            values,
            query_gain,
            key_gain,
            out_weight,
            expert_input,
            norm_gain,
            routes,
            route_weight,
            gate_weight,
            up_weight,
            down_weight,
        )
    moe_out, mixed = fused(
        expert_input,
        norm_gain,
        routes,
        route_weight,
        queries,
        keys,
        values,
        query_gain,
        key_gain,
        gate_weight[0],
        up_weight[0],
        down_weight[0],
        out_weight,
    )
    return (mixed, moe_out)


def solution(mesh):
    placed = (
        P("ep", "tp"),
        P("ep", "tp"),
        P("ep", "tp"),
        P("tp"),
        P("tp"),
        P("tp", None),
        P(("ep", "tp"), None),
        P(),
        P(("ep", "tp"), None),
        P(("ep", "tp"), None),
        P("ep", None, "tp"),
        P("ep", None, "tp"),
        P("ep", "tp", None),
    )
    return jax.shard_map(
        shards,
        mesh=mesh,
        in_specs=placed,
        out_specs=(P(("ep", "tp"), None), P(("ep", "tp"), None)),
        check_vma=False,
    )
```

```python
import functools

import jax
import jax.numpy as jnp
import numpy as np
from jax import lax
from jax.experimental import pallas as pl
from jax.experimental.pallas import tpu as pltpu
from jax.sharding import PartitionSpec as P

HEAD_DIM = 64
GRID_W = 128


NORM_EPS = 1e-06
ROPE_BASE = 10000.0


def rotate(vectors, grid_rows, grid_cols):
    quarter = vectors.shape[-1] // 4
    inverse = ROPE_BASE ** (-jnp.arange(quarter, dtype=jnp.float32) / quarter)
    angle_row = grid_rows[:, None] * inverse
    angle_col = grid_cols[:, None] * inverse
    angles = jnp.concatenate([angle_row, angle_row, angle_col, angle_col], axis=-1)[:, None, :]
    part_one, part_two, part_three, part_four = jnp.split(vectors, 4, axis=-1)
    turned = jnp.concatenate([-part_two, part_one, -part_four, part_three], axis=-1)
    return vectors * jnp.cos(angles) + turned * jnp.sin(angles)


def head_norm(raw_rows, gains, head_count, offset):
    row_count = raw_rows.shape[0]
    flat_rows = raw_rows.astype(jnp.float32).reshape(row_count, head_count, -1)
    unit_vec = flat_rows * lax.rsqrt(
        jnp.mean(flat_rows * flat_rows, axis=-1, keepdims=True) + NORM_EPS
    )
    unit_vec = unit_vec * gains.reshape(head_count, -1)
    places = offset + jnp.arange(row_count, dtype=jnp.int32)
    grid_rows = (places // GRID_W).astype(jnp.float32)
    grid_cols = (places % GRID_W).astype(jnp.float32)
    return rotate(unit_vec, grid_rows, grid_cols).astype(jnp.bfloat16).reshape(row_count, -1)


def absorb(running, key_block, value_block, grouped, score_scale):
    run_max, weight_sum, summed = running
    kv_count = grouped.shape[1]
    key_heads = key_block.reshape(key_block.shape[0], kv_count, -1)
    value_heads = value_block.reshape(value_block.shape[0], kv_count, -1)
    scores = (
        jnp.einsum("qhgd,khd->hgqk", grouped, key_heads, preferred_element_type=jnp.float32)
        * score_scale
    )
    new_max = jnp.maximum(run_max, jnp.max(scores, axis=-1))
    rescale = jnp.exp(run_max - new_max)
    weights = jnp.exp(scores - new_max[..., None])
    weight_sum = weight_sum * rescale + jnp.sum(weights, axis=-1)
    update = jnp.einsum(
        "hgqk,khd->qhgd",
        weights.astype(jnp.bfloat16),
        value_heads,
        preferred_element_type=jnp.float32,
    )
    summed = summed * jnp.transpose(rescale, (2, 0, 1))[..., None] + update
    return (new_max, weight_sum, summed)


def run_experts(sending, gate_weight, up_weight, down_weight):
    arrived = lax.all_to_all(sending, "ep", split_axis=0, concat_axis=0, tiled=True)
    shard_rows = lax.all_gather(arrived, "tp", axis=0, tiled=True)
    gate_out = jnp.dot(shard_rows, gate_weight[0], preferred_element_type=jnp.float32)
    up_out = jnp.dot(shard_rows, up_weight[0], preferred_element_type=jnp.float32)
    hidden = (jax.nn.silu(gate_out) * up_out).astype(jnp.bfloat16)
    results = lax.psum_scatter(
        jnp.dot(hidden, down_weight[0], preferred_element_type=jnp.float32).astype(jnp.bfloat16),
        "tp",
        scatter_dimension=0,
        tiled=True,
    )
    return lax.all_to_all(results, "ep", split_axis=0, concat_axis=0, tiled=True)


MESH = pl.DeviceIdType.MESH
TILE = 1024
CHUNKS = 2


def flip(index, pattern, size):
    result = 0
    bit = 1
    while bit < size:
        both = lax.rem(lax.div(index, bit) + lax.div(pattern, bit), 2)
        result = result + both * bit
        bit = bit * 2
    return result


def f32(value):
    return value.astype(jnp.float32)


ORDER = (0, 1, 4, 6, 5, 2, 7, 3)


def fused_kernel(
    n,
    x_ref,
    x_gain,
    routes_row,
    weight_row,
    q_raw,
    k_raw,
    v_raw,
    q_gain,
    k_gain,
    turn_hbm,
    wg_hbm,
    wu_hbm,
    wd_hbm,
    ow_hbm,
    moe,
    mixed,
    dense,
    meta,
    rows,
    y_send,
    partial,
    red,
    x_got,
    y_got,
    hold,
    sent,
    z_got,
    m_got,
    p_got,
    o_got,
    q_ref,
    kv_ref,
    turn,
    wg,
    wu,
    wd,
    ow,
    kv_all,
    attended,
    a_part,
    a_red,
    a_send,
    a_got,
    load_sem,
    kv_sems,
    dn_out,
    dn_in,
    meta_sems,
    row_y,
    row_c,
    row_x,
    red_sems,
    sum_x,
    sum_y,
    t_out,
    z_in,
    m_in,
    p_in,
    o_in,
    mix_sems,
):
    e = lax.axis_index("ep")
    t = lax.axis_index("tp")
    side = lax.div(t, 2)
    core = lax.rem(t, 2)
    other_side = 1 - side
    other_core = 1 - core
    layer = lax.div(e, 2)
    y = lax.rem(e, 2)
    other_y = 1 - y
    near = layer + 1 - 2 * lax.rem(layer, 2)
    last = n // 2 - 1
    across = last - layer
    inner = jnp.logical_and(layer > 0, layer < last)
    outer = jnp.logical_not(inner)
    half = lax.div(layer, 2)
    far_inner = 2 - half
    far_outer = last * (1 - half)
    x_tp = other_side * 2 + core
    x_peer = (e, x_tp)
    c_peer = (e, side * 2 + other_core)
    y_expert = layer * 2 + other_y
    y_peer = (y_expert, t)
    z_peer = (near * 2 + y, t)
    m_peer = (across * 2 + y, t)
    corner = (near * 2 + y, x_tp)
    cap, width = rows.shape[3], rows.shape[4]
    pairs = attended.shape[0]
    tok = attended.shape[1]
    tokens_here = x_ref.shape[0]
    chunks = dn_in.shape[1]
    part = width // chunks

    def remote(src, dst, send, recv, device):
        return pltpu.make_async_remote_copy(
            src_ref=src, dst_ref=dst, send_sem=send, recv_sem=recv, device_id=device, device_id_type=MESH
        )

    def cols(c):
        return pl.ds(c * part, part)

    loads = [
        pltpu.make_async_copy(a, b, load_sem.at[k])
        for k, (a, b) in enumerate(
            [
                (turn_hbm.at[pl.ds(pl.multiple_of(e * tok, 8), tok)], turn),
                (wg_hbm, wg),
                (wu_hbm, wu),
                (wd_hbm, wd),
                (ow_hbm, ow),
            ]
        )
    ]
    for load in loads:
        load.start()

    barrier = pltpu.get_barrier_semaphore()
    for s in range(1, n):
        pl.semaphore_signal(barrier, inc=1, device_id=(flip(e, s, n), t), device_id_type=MESH)
    for peer in (x_peer, c_peer, corner):
        pl.semaphore_signal(barrier, inc=1, device_id=peer, device_id_type=MESH)

    def kv_direct(s):
        return remote(kv_ref, kv_all.at[:, e], kv_sems.at[0, s], kv_sems.at[1, s], (flip(e, s, n), t))

    def kv_direct_in(s):
        return remote(kv_ref, kv_all.at[:, flip(e, s, n)], kv_sems.at[0, s], kv_sems.at[1, s], (flip(e, s, n), t))

    def kv_relay(s):
        owner = flip(e, s, n)
        return remote(kv_all.at[:, owner], kv_all.at[:, owner], kv_sems.at[0, s + 1], kv_sems.at[1, s + 1], (flip(e, 1, n), t))

    def kv_relay_in(s):
        owner = flip(e, s + 1, n)
        return remote(kv_all.at[:, owner], kv_all.at[:, owner], kv_sems.at[0, s + 1], kv_sems.at[1, s + 1], (flip(e, 1, n), t))

    own_kv = pltpu.make_async_copy(kv_ref, kv_all.at[:, e], load_sem.at[5])

    def block(source, target, number, c, device):
        return remote(
            dense.at[source, :, cols(c)],
            dense.at[target, :, cols(c)],
            dn_out.at[number, c],
            dn_in.at[target, c],
            device,
        )

    def to_x(c):
        return block(0, 1, 1, c, x_peer)

    def to_near(c):
        return block(0, 2, 2, c, z_peer)

    def x_to_near(c):
        return block(1, 3, 3, c, z_peer)

    def to_across(c):
        return block(0, 4, 4, c, m_peer)

    def near_to_across(c):
        return block(2, 5, 5, c, m_peer)

    def far_to_near(k, c):
        return block(4 + k, 4 + k, 6 + k, c, z_peer)

    def arrived(slot, c):
        block(slot, slot, 0, c, x_peer).wait_recv()

    far_slot = jnp.where(inner, 4, 5)

    def card(slot, number, device):
        return remote(meta.at[0], meta.at[slot], meta_sems.at[0, number], meta_sems.at[1, slot], device)

    cards = [
        card(1, 1, x_peer),
        card(2, 2, z_peer),
        card(3, 3, corner),
        card(far_slot, 4, (far_inner * 2 + y, t)),
        card(far_slot, 5, (far_outer * 2 + y, t)),
    ]

    def row_to_y(b):
        return remote(y_send.at[b], rows.at[b, core, y], row_y.at[0, b], row_y.at[1, b], y_peer)

    def row_from_y(b):
        return remote(y_send.at[b], rows.at[b, core, other_y], row_y.at[0, b], row_y.at[1, b], y_peer)

    def row_to_c(b, g):
        return remote(rows.at[b, core, g], rows.at[b, core, g], row_c.at[0, b, g], row_c.at[1, b, g], c_peer)

    def row_from_c(b, g):
        return remote(rows.at[b, core, g], rows.at[b, other_core, g], row_c.at[0, b, g], row_c.at[1, b, g], c_peer)

    def row_to_x(k, g):
        return remote(rows.at[4 + k, core, g], rows.at[6 + k, core, g], row_x.at[0, k, g], row_x.at[1, k, g], x_peer)

    def reduce_c(b):
        return remote(partial.at[b, other_core], red.at[b], red_sems.at[0, b], red_sems.at[1, b], c_peer)

    def reduce_x(k):
        return remote(partial.at[6 + k, core], x_got.at[k], sum_x.at[0, k], sum_x.at[1, k], x_peer)

    def give_y(b):
        return remote(partial.at[b, core, other_y], y_got.at[b], sum_y.at[0, b], sum_y.at[1, b], y_peer)

    def pass_on(b, place, where, arrive, c, device):
        return remote(sent.at[b, :, cols(c)], where.at[place, :, cols(c)], t_out.at[b, c], arrive.at[place, c], device)

    mix_core = remote(a_part.at[:, other_core], a_red, mix_sems.at[0, 0], mix_sems.at[1, 0], c_peer)
    mix_side = remote(a_send, a_got, mix_sems.at[0, 1], mix_sems.at[1, 1], x_peer)

    row_id = lax.broadcasted_iota(jnp.int32, (tokens_here, tokens_here), 0)
    col_id = lax.broadcasted_iota(jnp.int32, (tokens_here, tokens_here), 1)
    before = (row_id < col_id).astype(jnp.bfloat16)
    after = (col_id < row_id).astype(jnp.bfloat16)

    def tiles(size, body):
        def run(j, carry):
            body(pl.ds(pl.multiple_of(j * size, size), size))
            return carry

        lax.fori_loop(0, width // size, run, 0)

    def select(b):
        named = meta[b]
        spread = []
        for expert in (e, y_expert):
            wanted = expert.astype(jnp.float32)
            hit = jnp.logical_or(named[0:1] == wanted, named[1:2] == wanted)
            spread.append(jnp.broadcast_to(hit.astype(jnp.float32)[:, :tokens_here], (cap, tokens_here)))
        spread = jnp.concatenate(spread, axis=0)
        rank = jnp.dot(spread.astype(jnp.bfloat16), before, preferred_element_type=jnp.float32)
        slot = f32(lax.rem(lax.broadcasted_iota(jnp.int32, rank.shape, 0), cap))
        chosen = (jnp.where(rank == slot, 1.0, 0.0) * spread).astype(jnp.bfloat16)

        def body(span):
            found = jnp.dot(chosen, dense[b, :, span], preferred_element_type=jnp.float32).astype(jnp.bfloat16)
            rows[b, core, y, :, span] = found[:cap]
            y_send[b, :, span] = found[cap:]

        tiles(512, body)
        row_to_y(b).start()
        row_to_c(b, y).start()
        if b >= 4:
            row_to_x(b - 4, y).start()

    def arrive(b):
        if b < 6:
            row_from_y(b).wait_recv()
            if b >= 4:
                row_to_x(b - 4, other_y).start()
            row_to_c(b, other_y).start()
        else:
            for g in (y, other_y):
                remote(
                    rows.at[b - 2, core, g], rows.at[b, core, g], row_x.at[0, b - 6, g], row_x.at[1, b - 6, g], x_peer
                ).wait_recv()
                row_to_c(b, g).start()

    def finish(b):
        reduce_c(b).wait_recv()
        if b in (4, 5):
            reduce_x(b - 4).wait_recv()

        def body(span):
            value = f32(partial[b, core, :, :, span]) + f32(red[b, :, :, span])
            if b in (4, 5):
                value = value + f32(x_got[b - 4, :, :, span])
            partial[b, core, :, :, span] = value.astype(jnp.bfloat16)

        tiles(512, body)
        if b >= 6:
            reduce_x(b - 6).start()
        else:
            give_y(b).start()

    def gather(b):
        remote(partial.at[b, core, other_y], y_got.at[b], sum_y.at[0, b], sum_y.at[1, b], y_peer).wait_recv()
        turned_meta = jnp.transpose(meta[b])[:tokens_here]
        parts = []
        for expert in (e, y_expert):
            wanted = expert.astype(jnp.float32)
            hits = [(turned_meta[:, k:k + 1] == wanted).astype(jnp.float32) for k in range(2)]
            scale = hits[0] * turned_meta[:, 2:3] + hits[1] * turned_meta[:, 3:4]
            spread = jnp.broadcast_to(hits[0] + hits[1], (tokens_here, cap))
            rank = jnp.dot(after, spread.astype(jnp.bfloat16), preferred_element_type=jnp.float32)
            slot = f32(lax.broadcasted_iota(jnp.int32, rank.shape, 1))
            parts.append(((jnp.where(rank == slot, 1.0, 0.0) * spread).astype(jnp.bfloat16), scale))

        def body(span):
            mine = jnp.dot(parts[0][0], partial[b, core, y, :, span], preferred_element_type=jnp.float32)
            theirs = jnp.dot(parts[1][0], y_got[b, :, span], preferred_element_type=jnp.float32)
            hold[b, :, span] = mine * parts[0][1] + theirs * parts[1][1]

        tiles(512, body)

    def release(b, sources, place, where, arrive_sem, device):
        for c in range(chunks):
            for got, at, sem in sources:
                remote(got.at[at, :, cols(c)], got.at[at, :, cols(c)], t_out.at[0, c], sem.at[at, c], device).wait_recv()

            def run(j, carry):
                span = pl.ds(pl.multiple_of(c * part + j * 512, 512), 512)
                value = hold[b, :, span]
                for got, at, sem in sources:
                    value = value + f32(got[at, :, span])
                sent[b, :, span] = value.astype(jnp.bfloat16)
                return carry

            lax.fori_loop(0, part // 512, run, 0)
            pass_on(b, place, where, arrive_sem, c, device).start()

    as_float = f32(x_ref[...])
    mean = jnp.mean(as_float * as_float, axis=1, keepdims=True)
    dense[0] = (as_float * lax.rsqrt(mean + NORM_EPS) * x_gain[...]).astype(jnp.bfloat16)
    meta[0] = jnp.zeros(meta.shape[1:], jnp.float32)
    meta[0, 0:2, 0:tokens_here] = f32(routes_row[...])
    meta[0, 2:4, 0:tokens_here] = weight_row[...]

    pl.semaphore_wait(barrier, n + 2)
    for item in cards:
        item.start()
    for c in range(chunks):
        to_x(c).start()

        @pl.when(inner)
        def _():
            to_across(c).start()

        if c == 0:
            to_near(c).start()
        else:
            @pl.when(outer)
            def _():
                to_near(c).start()

    select(0)

    loads[0].wait()
    lane = lax.broadcasted_iota(jnp.int32, (tok, 128), 1)
    low = lane < HEAD_DIM
    even = lax.rem(lax.div(lane, HEAD_DIM // 4), 2) == 0
    table = turn[...]
    swapped = pltpu.roll(table, HEAD_DIM, 1)
    cosine = jnp.where(low, table, swapped)
    sine = jnp.where(low, swapped, table)

    def turned(raw, gain):
        flat = f32(raw)
        square = flat * flat
        left = jnp.sum(jnp.where(low, square, 0.0), axis=1, keepdims=True)
        right = jnp.sum(jnp.where(low, 0.0, square), axis=1, keepdims=True)
        mean_square = jnp.where(low, left, right) * (1.0 / HEAD_DIM)
        unit = flat * lax.rsqrt(mean_square + NORM_EPS) * gain
        partner = jnp.where(
            even, -pltpu.roll(unit, 128 - HEAD_DIM // 4, 1), pltpu.roll(unit, HEAD_DIM // 4, 1)
        )
        return unit * cosine + partner * sine

    for pair in range(kv_ref.shape[0] // 2):
        span = slice(pair * 128, (pair + 1) * 128)
        k_rows = turned(k_raw[:, span], k_gain[:, span])
        v_rows = f32(v_raw[:, span])
        kv_ref[2 * pair] = jnp.where(low, k_rows, pltpu.roll(v_rows, HEAD_DIM, 1)).astype(jnp.bfloat16)
        kv_ref[2 * pair + 1] = jnp.where(low, pltpu.roll(k_rows, HEAD_DIM, 1), v_rows).astype(jnp.bfloat16)
    own_kv.start()
    for s in range(2, n, 2):
        kv_direct(s).start()
    kv_direct(1).start()

    for pair in range(pairs):
        span = slice(pair * 128, (pair + 1) * 128)
        q_rows = turned(q_raw[:, span], q_gain[:, span])
        q_ref[2 * pair] = jnp.where(low, q_rows, 0.0).astype(jnp.bfloat16)
        q_ref[2 * pair + 1] = jnp.where(low, pltpu.roll(q_rows, HEAD_DIM, 1), 0.0).astype(jnp.bfloat16)
    own_kv.wait()

    for slot in range(1, 6):
        remote(meta.at[0], meta.at[slot], meta_sems.at[0, 0], meta_sems.at[1, slot], x_peer).wait_recv()
    for c in range(chunks):
        arrived(1, c)

        @pl.when(outer)
        def _():
            x_to_near(c).start()

        @pl.when(inner)
        def _():
            arrived(4, c)
            far_to_near(0, c).start()
            arrived(2, c)
            near_to_across(c).start()

    select(1)

    def attend(pair):
        kv = kv_all[lax.div(pair * 2 * kv_all.shape[0], pairs * 2)].reshape(n * tok, 128)
        halves = []
        for h in range(2):
            scores = lax.dot_general(
                q_ref[pair * 2 + h], kv, (((1,), (1,)), ((), ())), preferred_element_type=jnp.float32
            ) * (HEAD_DIM ** (-0.5))
            peak = jnp.max(scores, axis=1, keepdims=True)
            weights = jnp.exp(scores - peak)
            total = jnp.sum(weights, axis=1, keepdims=True)
            summed = jnp.dot(weights.astype(jnp.bfloat16), kv, preferred_element_type=jnp.float32)
            halves.append(summed / total)
        joined = jnp.where(low, pltpu.roll(halves[0], HEAD_DIM, 1), halves[1])
        attended[pair] = joined.astype(jnp.bfloat16)

    def mix_product():
        loads[4].wait()
        for tile in range(0, width, TILE):
            product = jnp.dot(attended[0], ow[0, :, tile:tile + TILE], preferred_element_type=jnp.float32)
            for p in range(1, pairs):
                product += jnp.dot(attended[p], ow[p, :, tile:tile + TILE], preferred_element_type=jnp.float32)
            a_part[:, :, :, tile:tile + TILE] = product.astype(jnp.bfloat16).reshape(2, 2, tok // 4, TILE)
        mix_core.start()

    def mix_sum():
        mix_core.wait_recv()
        a_send[...] = (f32(a_part[other_side, core]) + f32(a_red[other_side])).astype(jnp.bfloat16)
        mix_side.start()

    def unit_of(s):
        chosen = ORDER[0]
        for place in range(1, len(ORDER)):
            chosen = jnp.where(s == place, ORDER[place], chosen)
        return chosen

    def step(s, carry):
        u = unit_of(s)

        def at(number):
            return pl.when(s == number)

        @at(1)
        def _():
            @pl.when(inner)
            def _():
                arrived(5, 0)
                far_to_near(1, 0).start()

        for place, b in enumerate(ORDER):
            @at(place)
            def _(b=b):
                arrive(b)

        @at(0)
        def _():
            for load in loads[1:4]:
                load.wait()

        @at(1)
        def _():
            for s2 in range(2, n, 2):
                kv_direct_in(s2).wait_recv()
                kv_relay(s2).start()
            finish(0)

        @at(2)
        def _():
            finish(1)

        @at(3)
        def _():
            gather(0)

        @at(4)
        def _():
            finish(6)
            mix_product()

        @at(5)
        def _():
            mix_sum()
            gather(1)

        @at(6)
        def _():
            finish(4)
            finish(2)

        @at(7)
        def _():
            finish(7)
            gather(4)

            @pl.when(outer)
            def _():
                release(4, [], 0, z_got, z_in, z_peer)

        for g in range(2):
            row_from_c(u, g).wait_recv()
        tokens = rows[u].reshape(4 * cap, width)
        gate = jnp.dot(tokens, wg[...], preferred_element_type=jnp.float32)
        up = jnp.dot(tokens, wu[...], preferred_element_type=jnp.float32)
        hidden = (gate / (1.0 + jnp.exp(-gate)) * up).astype(jnp.bfloat16)
        for tile in range(0, width, TILE):
            product = jnp.dot(hidden, wd[:, tile:tile + TILE], preferred_element_type=jnp.float32)
            partial[u, :, :, :, tile:tile + TILE] = product.astype(jnp.bfloat16).reshape(2, 2, cap, TILE)
        reduce_c(u).start()

        @at(0)
        def _():
            @pl.when(outer)
            def _():
                for c in range(chunks):
                    arrived(4, c)

            select(4)

        @at(1)
        def _():
            @pl.when(inner)
            def _():
                for c in range(1, chunks):
                    arrived(5, c)
                    far_to_near(1, c).start()
                    to_near(c).start()
                for c in range(chunks):
                    x_to_near(c).start()

            kv_direct_in(1).wait_recv()
            for s2 in range(2, n, 2):
                kv_relay_in(s2).wait_recv()

        @pl.when(jnp.logical_or(s == 1, s == 2))
        def _():
            attend(2 * (s - 1))
            attend(2 * (s - 1) + 1)

        @at(2)
        def _():
            @pl.when(outer)
            def _():
                for c in range(chunks):
                    arrived(5, c)

            select(5)

        @at(3)
        def _():
            @pl.when(outer)
            def _():
                for c in range(chunks):
                    arrived(2, c)

            select(2)

        @at(5)
        def _():
            for c in range(chunks):
                arrived(3, c)
            select(3)

        return carry

    lax.fori_loop(0, len(ORDER), step, 0)

    finish(5)
    finish(3)
    gather(2)
    gather(5)

    @pl.when(outer)
    def _():
        release(5, [], 1, z_got, z_in, z_peer)

    @pl.when(inner)
    def _():
        release(4, [(z_got, 0, z_in)], 0, m_got, m_in, m_peer)

    gather(3)
    release(3, [], 1, p_got, p_in, z_peer)

    @pl.when(inner)
    def _():
        release(5, [(z_got, 1, z_in)], 1, m_got, m_in, m_peer)

    mix_side.wait_recv()
    mixed[...] = (f32(a_part[side, core]) + f32(a_red[side]) + f32(a_got[...])).astype(jnp.bfloat16)

    release(1, [(p_got, 1, p_in)], 0, o_got, o_in, x_peer)

    @pl.when(outer)
    def _():
        release(2, [], 0, p_got, p_in, z_peer)

    @pl.when(inner)
    def _():
        release(2, [(m_got, 1, m_in)], 0, p_got, p_in, z_peer)
        for c in range(chunks):
            remote(m_got.at[0, :, cols(c)], m_got.at[0, :, cols(c)], t_out.at[0, c], m_in.at[0, c], m_peer).wait_recv()

        def fold(span):
            hold[0, :, span] = hold[0, :, span] + f32(m_got[0, :, span])

        tiles(512, fold)

    for c in range(chunks):
        for got, sem in ((o_got, o_in), (p_got, p_in)):
            remote(got.at[0, :, cols(c)], got.at[0, :, cols(c)], t_out.at[0, c], sem.at[0, c], x_peer).wait_recv()

        def final(j, carry):
            span = pl.ds(pl.multiple_of(c * part + j * 512, 512), 512)
            value = hold[0, :, span] + f32(o_got[0, :, span]) + f32(p_got[0, :, span])
            moe[:, span] = value.astype(jnp.bfloat16)
            return carry

        lax.fori_loop(0, part // 512, final, 0)

    mix_core.wait_send()
    mix_side.wait_send()
    for s in range(2, n, 2):
        kv_direct(s).wait_send()
        kv_relay(s).wait_send()
    kv_direct(1).wait_send()
    for item in cards:
        item.wait_send()
    for c in range(chunks):
        to_x(c).wait_send()
        to_near(c).wait_send()
        x_to_near(c).wait_send()

        @pl.when(inner)
        def _():
            to_across(c).wait_send()
            near_to_across(c).wait_send()
            far_to_near(0, c).wait_send()
            far_to_near(1, c).wait_send()

        for b in range(1, 6):
            pass_on(b, 0, o_got, o_in, c, x_peer).wait_send()
    for k in range(2):
        for g in range(2):
            row_to_x(k, g).wait_send()
        reduce_x(k).wait_send()
    for b in range(6):
        row_to_y(b).wait_send()
        give_y(b).wait_send()
    for b in range(8):
        for g in range(2):
            row_to_c(b, g).wait_send()
        reduce_c(b).wait_send()


def turn_table(tokens):
    quarter = HEAD_DIM // 4
    inverse = np.power(ROPE_BASE, -np.arange(quarter, dtype=np.float64) / quarter)
    places = np.arange(tokens)
    row = (places // GRID_W)[:, None] * inverse
    col = (places % GRID_W)[:, None] * inverse
    angles = np.concatenate([row, row, col, col], axis=1)
    return np.concatenate([np.cos(angles), np.sin(angles)], axis=1).astype(np.float32)


def fused(x, x_gain, routes, route_weight, queries, keys, values, q_gain, k_gain, gate_weight, up_weight, down_weight, out_weight):
    n = lax.axis_size("ep")
    tok_exp, width = x.shape
    cap = 2 * routes.shape[1] * tok_exp // n
    tok = queries.shape[0]
    heads = queries.shape[1] // HEAD_DIM
    kv_count = keys.shape[1] // HEAD_DIM
    pairs = heads // 2
    hidden = gate_weight.shape[1]
    bf = jnp.bfloat16
    vmem = pl.BlockSpec(memory_space=pltpu.VMEM)
    anywhere = pl.BlockSpec(memory_space=pl.ANY)
    dma = pltpu.SemaphoreType.DMA
    return pl.pallas_call(
        functools.partial(fused_kernel, n),
        out_shape=(
            jax.ShapeDtypeStruct((tok_exp, width), bf),
            jax.ShapeDtypeStruct((tok // 4, width), bf),
        ),
        in_specs=[vmem] * 9 + [anywhere] * 5,
        out_specs=(vmem, vmem),
        scratch_shapes=[
            pltpu.VMEM((6, tok_exp, width), bf),
            pltpu.VMEM((6, 8, 128), jnp.float32),
            pltpu.VMEM((8, 2, 2, cap, width), bf),
            pltpu.VMEM((6, cap, width), bf),
            pltpu.VMEM((8, 2, 2, cap, width), bf),
            pltpu.VMEM((8, 2, cap, width), bf),
            pltpu.VMEM((2, 2, cap, width), bf),
            pltpu.VMEM((6, cap, width), bf),
            pltpu.VMEM((6, tok_exp, width), jnp.float32),
            pltpu.VMEM((6, tok_exp, width), bf),
            pltpu.VMEM((2, tok_exp, width), bf),
            pltpu.VMEM((2, tok_exp, width), bf),
            pltpu.VMEM((2, tok_exp, width), bf),
            pltpu.VMEM((1, tok_exp, width), bf),
            pltpu.VMEM((heads, tok, 128), bf),
            pltpu.VMEM((kv_count, tok, 128), bf),
            pltpu.VMEM((tok, 128), jnp.float32),
            pltpu.VMEM((width, hidden), bf),
            pltpu.VMEM((width, hidden), bf),
            pltpu.VMEM((hidden, width), bf),
            pltpu.VMEM((pairs, 128, width), bf),
            pltpu.VMEM((kv_count, n, tok, 128), bf),
            pltpu.VMEM((pairs, tok, 128), bf),
            pltpu.VMEM((2, 2, tok // 4, width), bf),
            pltpu.VMEM((2, tok // 4, width), bf),
            pltpu.VMEM((tok // 4, width), bf),
            pltpu.VMEM((tok // 4, width), bf),
            dma((6,)),
            dma((2, n)),
            dma((8, CHUNKS)),
            dma((6, CHUNKS)),
            dma((2, 6)),
            dma((2, 6)),
            dma((2, 8, 2)),
            dma((2, 2, 2)),
            dma((2, 8)),
            dma((2, 2)),
            dma((2, 6)),
            dma((6, CHUNKS)),
            dma((2, CHUNKS)),
            dma((2, CHUNKS)),
            dma((2, CHUNKS)),
            dma((1, CHUNKS)),
            dma((2, 2)),
        ],
        compiler_params=pltpu.CompilerParams(
            collective_id=0, has_side_effects=True, vmem_limit_bytes=62 * 1024 * 1024
        ),
    )(
        x,
        x_gain.reshape(1, width),
        jnp.transpose(routes),
        jnp.transpose(route_weight),
        queries,
        keys,
        values,
        q_gain.reshape(1, -1),
        k_gain.reshape(1, -1),
        jnp.asarray(turn_table(n * tok)),
        gate_weight,
        up_weight,
        down_weight,
        out_weight.reshape(pairs, 128, width),
    )


def plain_shards(
    queries,
    keys,
    values,
    query_gain,
    key_gain,
    out_weight,
    expert_input,
    norm_gain,
    routes,
    route_weight,
    gate_weight,
    up_weight,
    down_weight,
):
    tok_mix = queries.shape[0]
    head_count = query_gain.shape[0] // HEAD_DIM
    kv_count = key_gain.shape[0] // HEAD_DIM
    group_size = head_count // kv_count
    offset = lax.axis_index("ep") * tok_mix
    q_turned = head_norm(queries, query_gain, head_count, offset)
    k_turned = head_norm(keys, key_gain, kv_count, offset)
    grouped = q_turned.reshape(tok_mix, kv_count, group_size, HEAD_DIM)
    score_scale = HEAD_DIM ** (-0.5)
    start_state = (
        jnp.full((kv_count, group_size, tok_mix), -jnp.inf, jnp.float32),
        jnp.zeros((kv_count, group_size, tok_mix), jnp.float32),
        jnp.zeros((tok_mix, kv_count, group_size, HEAD_DIM), jnp.float32),
    )
    running = start_state
    key_piece = lax.all_gather(k_turned, "ep", axis=0, tiled=True)
    value_piece = lax.all_gather(values, "ep", axis=0, tiled=True)
    length = key_piece.shape[0]
    block_len = length
    while block_len > 2048 and block_len % 2 == 0:
        block_len = block_len // 2
    key_blocks = key_piece.reshape(length // block_len, block_len, key_piece.shape[1])
    value_blocks = value_piece.reshape(length // block_len, block_len, value_piece.shape[1])

    def advance(inner_state, key_value):
        return (absorb(inner_state, key_value[0], key_value[1], grouped, score_scale), None)

    running, unused = lax.scan(advance, running, (key_blocks, value_blocks))
    final_max, weight_sum, summed = running
    attended = (
        (summed / jnp.transpose(weight_sum, (2, 0, 1))[..., None])
        .reshape(tok_mix, -1)
        .astype(jnp.bfloat16)
    )
    mixed = lax.psum_scatter(
        jnp.dot(attended, out_weight, preferred_element_type=jnp.float32).astype(jnp.bfloat16),
        "tp",
        scatter_dimension=0,
        tiled=True,
    )
    tok_exp = expert_input.shape[0]
    top_count = routes.shape[1]
    expert_count = lax.axis_size("ep")
    capacity = 2 * top_count * tok_exp // expert_count
    as_float = expert_input.astype(jnp.float32)
    normed = (
        as_float
        * lax.rsqrt(jnp.mean(as_float * as_float, axis=-1, keepdims=True) + NORM_EPS)
        * norm_gain
    ).astype(jnp.bfloat16)
    flat_routes = routes.reshape(-1)
    route_hits = (
        flat_routes[:, None] == jnp.arange(expert_count, dtype=jnp.int32)[None, :]
    ).astype(jnp.int32)
    slot_rank = jnp.sum((jnp.cumsum(route_hits, axis=0) - route_hits) * route_hits, axis=1)
    slot_ids = flat_routes * capacity + slot_rank
    placed = jnp.arange(expert_count * capacity, dtype=jnp.int32)[:, None] == slot_ids[None, :]
    placed = jnp.any(placed.reshape(expert_count * capacity, tok_exp, top_count), axis=2).astype(
        jnp.bfloat16
    )
    outbound = jnp.dot(placed, normed, preferred_element_type=jnp.float32).astype(jnp.bfloat16)
    model_width = outbound.shape[1]
    half_cap = capacity // 2
    laid = outbound.reshape(expert_count, capacity, model_width)
    first_half = run_experts(
        laid[:, :half_cap].reshape(expert_count * half_cap, model_width),
        gate_weight,
        up_weight,
        down_weight,
    )
    second_half = run_experts(
        laid[:, half_cap:].reshape(expert_count * half_cap, model_width),
        gate_weight,
        up_weight,
        down_weight,
    )
    back_rows = jnp.concatenate(
        [
            first_half.reshape(expert_count, half_cap, model_width),
            second_half.reshape(expert_count, half_cap, model_width),
        ],
        axis=1,
    )
    back_rows = back_rows.reshape(expert_count * capacity, model_width)
    picked = back_rows[slot_ids.reshape(tok_exp, top_count)]
    moe_out = jnp.sum(picked.astype(jnp.float32) * route_weight[:, :, None], axis=1).astype(
        jnp.bfloat16
    )
    return (mixed, moe_out)


def shards(
    queries,
    keys,
    values,
    query_gain,
    key_gain,
    out_weight,
    expert_input,
    norm_gain,
    routes,
    route_weight,
    gate_weight,
    up_weight,
    down_weight,
):
    tok_exp = expert_input.shape[0]
    top_count = routes.shape[1]
    expert_count = lax.axis_size("ep")
    capacity = 2 * top_count * tok_exp // expert_count
    if capacity % 16 != 0 or lax.axis_size("tp") != 4 or expert_count != 8:
        return plain_shards(
            queries,
            keys,
            values,
            query_gain,
            key_gain,
            out_weight,
            expert_input,
            norm_gain,
            routes,
            route_weight,
            gate_weight,
            up_weight,
            down_weight,
        )
    moe_out, mixed = fused(
        expert_input,
        norm_gain,
        routes,
        route_weight,
        queries,
        keys,
        values,
        query_gain,
        key_gain,
        gate_weight[0],
        up_weight[0],
        down_weight[0],
        out_weight,
    )
    return (mixed, moe_out)


def solution(mesh):
    placed = (
        P("ep", "tp"),
        P("ep", "tp"),
        P("ep", "tp"),
        P("tp"),
        P("tp"),
        P("tp", None),
        P(("ep", "tp"), None),
        P(),
        P(("ep", "tp"), None),
        P(("ep", "tp"), None),
        P("ep", None, "tp"),
        P("ep", None, "tp"),
        P("ep", "tp", None),
    )
    return jax.shard_map(
        shards,
        mesh=mesh,
        in_specs=placed,
        out_specs=(P(("ep", "tp"), None), P(("ep", "tp"), None)),
        check_vma=False,
    )
```

```python
import functools

import jax
import jax.numpy as jnp
import numpy as np
from jax import lax
from jax.experimental import pallas as pl
from jax.experimental.pallas import tpu as pltpu
from jax.sharding import PartitionSpec as P

HEAD_DIM = 64
GRID_W = 128


NORM_EPS = 1e-06
ROPE_BASE = 10000.0


def rotate(vectors, grid_rows, grid_cols):
    quarter = vectors.shape[-1] // 4
    inverse = ROPE_BASE ** (-jnp.arange(quarter, dtype=jnp.float32) / quarter)
    angle_row = grid_rows[:, None] * inverse
    angle_col = grid_cols[:, None] * inverse
    angles = jnp.concatenate([angle_row, angle_row, angle_col, angle_col], axis=-1)[:, None, :]
    part_one, part_two, part_three, part_four = jnp.split(vectors, 4, axis=-1)
    turned = jnp.concatenate([-part_two, part_one, -part_four, part_three], axis=-1)
    return vectors * jnp.cos(angles) + turned * jnp.sin(angles)


def head_norm(raw_rows, gains, head_count, offset):
    row_count = raw_rows.shape[0]
    flat_rows = raw_rows.astype(jnp.float32).reshape(row_count, head_count, -1)
    unit_vec = flat_rows * lax.rsqrt(
        jnp.mean(flat_rows * flat_rows, axis=-1, keepdims=True) + NORM_EPS
    )
    unit_vec = unit_vec * gains.reshape(head_count, -1)
    places = offset + jnp.arange(row_count, dtype=jnp.int32)
    grid_rows = (places // GRID_W).astype(jnp.float32)
    grid_cols = (places % GRID_W).astype(jnp.float32)
    return rotate(unit_vec, grid_rows, grid_cols).astype(jnp.bfloat16).reshape(row_count, -1)


def absorb(running, key_block, value_block, grouped, score_scale):
    run_max, weight_sum, summed = running
    kv_count = grouped.shape[1]
    key_heads = key_block.reshape(key_block.shape[0], kv_count, -1)
    value_heads = value_block.reshape(value_block.shape[0], kv_count, -1)
    scores = (
        jnp.einsum("qhgd,khd->hgqk", grouped, key_heads, preferred_element_type=jnp.float32)
        * score_scale
    )
    new_max = jnp.maximum(run_max, jnp.max(scores, axis=-1))
    rescale = jnp.exp(run_max - new_max)
    weights = jnp.exp(scores - new_max[..., None])
    weight_sum = weight_sum * rescale + jnp.sum(weights, axis=-1)
    update = jnp.einsum(
        "hgqk,khd->qhgd",
        weights.astype(jnp.bfloat16),
        value_heads,
        preferred_element_type=jnp.float32,
    )
    summed = summed * jnp.transpose(rescale, (2, 0, 1))[..., None] + update
    return (new_max, weight_sum, summed)


def run_experts(sending, gate_weight, up_weight, down_weight):
    arrived = lax.all_to_all(sending, "ep", split_axis=0, concat_axis=0, tiled=True)
    shard_rows = lax.all_gather(arrived, "tp", axis=0, tiled=True)
    gate_out = jnp.dot(shard_rows, gate_weight[0], preferred_element_type=jnp.float32)
    up_out = jnp.dot(shard_rows, up_weight[0], preferred_element_type=jnp.float32)
    hidden = (jax.nn.silu(gate_out) * up_out).astype(jnp.bfloat16)
    results = lax.psum_scatter(
        jnp.dot(hidden, down_weight[0], preferred_element_type=jnp.float32).astype(jnp.bfloat16),
        "tp",
        scatter_dimension=0,
        tiled=True,
    )
    return lax.all_to_all(results, "ep", split_axis=0, concat_axis=0, tiled=True)


MESH = pl.DeviceIdType.MESH
TILE = 1024
CHUNKS = 2


def flip(index, pattern, size):
    result = 0
    bit = 1
    while bit < size:
        both = lax.rem(lax.div(index, bit) + lax.div(pattern, bit), 2)
        result = result + both * bit
        bit = bit * 2
    return result


def f32(value):
    return value.astype(jnp.float32)


INNER_ORDER = (
    ("meta",), ("F6", 0), ("arr", 0, 0), ("F5", 0), ("sel", 4, 0), ("F6", 1), ("F3", 0), ("sel", 1, 1),
    ("sel", 4, 1), ("sel", 5, 0), ("F5", 1), ("sel", 3, 0), ("F3", 1), ("arr", 4, 1), ("sel", 3, 1),
    ("sel", 1, 0), ("arr", 5, 0), ("arx", 0, 0, 1), ("kvf", 0), ("arr", 0, 1), ("arr", 3, 0), ("F7", 1),
    ("arr", 4, 0), ("arr", 3, 1), ("F7", 0), ("sel", 5, 1), ("kvs",), ("cmp", 0), ("kvf", 2),
    ("arx", 0, 1, 0), ("D2", 1), ("arr", 5, 1), ("arx", 1, 0, 0), ("arx", 1, 1, 0), ("cmp", 3), ("fin", 0, 1),
    ("sel", 2, 1), ("fin", 3, 0), ("cmp", 4), ("arx", 1, 0, 1), ("arx", 1, 1, 1), ("sel", 2, 0),
    ("arr", 1, 0), ("arx", 0, 1, 1), ("arx", 0, 0, 0), ("fin", 3, 1), ("cmp", 7), ("fin", 7, 1),
    ("arr", 1, 1), ("kvf", 1), ("cmp", 6), ("cmp", 5), ("fin", 6, 1), ("fin", 7, 0), ("cmp", 1),
    ("arr", 2, 1), ("fin", 6, 0), ("gat", 3, 1), ("gat", 0, 1), ("att", 0), ("fin", 5, 1), ("gat", 3, 0),
    ("fin", 1, 1), ("fin", 4, 1), ("rel", 3, 0), ("rel", 3, 1), ("att", 1), ("mixp",), ("fin", 5, 0),
    ("arr", 2, 0), ("cmp", 2), ("gat", 4, 1), ("rel", 4, 1), ("fin", 1, 0), ("gat", 5, 0), ("mixs",),
    ("fin", 2, 1), ("gat", 5, 1), ("rel", 5, 1), ("gat", 1, 1), ("gat", 1, 0), ("fin", 0, 0), ("rel", 1, 0),
    ("fin", 4, 0), ("rel", 5, 0), ("fin", 2, 0), ("gat", 2, 1), ("rel", 2, 1), ("mixf",), ("gat", 0, 0),
    ("gat", 4, 0), ("gat", 2, 0), ("rel", 2, 0), ("rel", 4, 0), ("rel", 1, 1), ("final", 1), ("final", 0),
)
OUTER_ORDER = (
    ("meta",), ("F3", 0), ("sel", 1, 0), ("sel", 1, 1), ("sel", 4, 0), ("F3", 1), ("sel", 2, 0), ("kvs",),
    ("sel", 4, 1), ("arx", 0, 0, 1), ("arr", 1, 0), ("arr", 4, 1), ("arr", 1, 1), ("sel", 3, 0),
    ("arr", 0, 1), ("arx", 0, 1, 1), ("arr", 4, 0), ("arr", 3, 0), ("sel", 3, 1), ("sel", 5, 1), ("cmp", 1),
    ("arx", 0, 0, 0), ("arx", 0, 1, 0), ("arr", 3, 1), ("arr", 5, 1), ("sel", 5, 0), ("cmp", 3), ("cmp", 6),
    ("arr", 0, 0), ("fin", 3, 0), ("arr", 5, 0), ("fin", 6, 1), ("fin", 3, 1), ("cmp", 0), ("kvf", 0),
    ("cmp", 4), ("gat", 3, 0), ("arx", 1, 0, 1), ("kvf", 2), ("arx", 1, 1, 1), ("arx", 1, 0, 0),
    ("arx", 1, 1, 0), ("rel", 3, 0), ("sel", 2, 1), ("cmp", 7), ("gat", 3, 1), ("fin", 7, 1), ("arr", 2, 0),
    ("rel", 3, 1), ("fin", 7, 0), ("fin", 4, 1), ("arr", 2, 1), ("kvf", 1), ("cmp", 5), ("gat", 4, 1),
    ("fin", 6, 0), ("rel", 4, 1), ("fin", 5, 1), ("fin", 1, 1), ("att", 0), ("gat", 5, 1), ("rel", 5, 1),
    ("fin", 5, 0), ("fin", 1, 0), ("att", 1), ("gat", 1, 1), ("rel", 1, 1), ("gat", 5, 0), ("rel", 5, 0),
    ("fin", 4, 0), ("cmp", 2), ("fin", 2, 1), ("gat", 4, 0), ("rel", 4, 0), ("gat", 1, 0), ("rel", 1, 0),
    ("fin", 2, 0), ("fin", 0, 0), ("mixp",), ("gat", 2, 1), ("rel", 2, 1), ("mixs",), ("fin", 0, 1),
    ("gat", 2, 0), ("gat", 0, 0), ("rel", 2, 0), ("gat", 0, 1), ("final", 1), ("mixf",), ("final", 0),
)


BIG = {"cmp": 0, "att": 8, "mixp": 10}


def fused_kernel(
    n,
    x_ref,
    x_gain,
    routes_row,
    weight_row,
    q_raw,
    k_raw,
    v_raw,
    q_gain,
    k_gain,
    turn_hbm,
    wg_hbm,
    wu_hbm,
    wd_hbm,
    ow_hbm,
    moe,
    mixed,
    dense,
    meta,
    chosen,
    picks,
    scales,
    rows,
    y_send,
    partial,
    red,
    x_got,
    y_got,
    hold,
    sent,
    z_got,
    m_got,
    p_got,
    o_got,
    q_ref,
    turn,
    wg,
    wu,
    wd,
    ow,
    kv_all,
    attended,
    a_part,
    a_red,
    a_send,
    a_got,
    load_sem,
    kvz_out,
    kvz_in,
    kvy_sems,
    dn_out,
    dn_in,
    meta_sems,
    row_y,
    row_c,
    row_x,
    red_sems,
    sum_x,
    sum_y,
    t_out,
    z_in,
    m_in,
    p_in,
    o_in,
    mix_sems,
):
    e = lax.axis_index("ep")
    t = lax.axis_index("tp")
    side = lax.div(t, 2)
    core = lax.rem(t, 2)
    other_side = 1 - side
    other_core = 1 - core
    layer = lax.div(e, 2)
    y = lax.rem(e, 2)
    other_y = 1 - y
    near = layer + 1 - 2 * lax.rem(layer, 2)
    last = n // 2 - 1
    across = last - layer
    inner = jnp.logical_and(layer > 0, layer < last)
    outer = jnp.logical_not(inner)
    half = lax.div(layer, 2)
    far_inner = 2 - half
    far_outer = last * (1 - half)
    x_tp = other_side * 2 + core
    x_peer = (e, x_tp)
    c_peer = (e, side * 2 + other_core)
    y_expert = layer * 2 + other_y
    y_peer = (y_expert, t)
    z_peer = (near * 2 + y, t)
    m_peer = (across * 2 + y, t)
    corner = (near * 2 + y, x_tp)
    cap, width = rows.shape[3], rows.shape[4]
    pairs = attended.shape[0]
    tok = attended.shape[1]
    tokens_here = x_ref.shape[0]
    chunks = dn_in.shape[1]
    part = width // chunks
    groups = (y, other_y)

    def remote(src, dst, send, recv, device):
        return pltpu.make_async_remote_copy(
            src_ref=src, dst_ref=dst, send_sem=send, recv_sem=recv, device_id=device, device_id_type=MESH
        )

    def cols(c):
        return pl.ds(c * part, part)

    loads = [
        pltpu.make_async_copy(a, b, load_sem.at[k])
        for k, (a, b) in enumerate(
            [
                (turn_hbm.at[pl.ds(pl.multiple_of(e * tok, 8), tok)], turn),
                (wg_hbm, wg),
                (wu_hbm, wu),
                (wd_hbm, wd),
                (ow_hbm, ow),
            ]
        )
    ]
    for load in loads:
        load.start()

    far_peers = [(far_inner * 2 + y, t), (far_outer * 2 + y, t)]
    barrier = pltpu.get_barrier_semaphore()
    greeted = [x_peer, c_peer, y_peer, z_peer, corner] + far_peers
    for peer in greeted:
        pl.semaphore_signal(barrier, inc=1, device_id=peer, device_id_type=MESH)

    def kv_z(owner, out, place, device):
        return remote(kv_all.at[:, owner], kv_all.at[:, owner], kvz_out.at[out], kvz_in.at[place], device)

    stops = [layer, near, far_inner, far_outer]

    def kv_y(j):
        owner = stops[j] * 2 + y
        return remote(kv_all.at[:, owner], kv_all.at[:, owner], kvy_sems.at[0, j], kvy_sems.at[1, j], y_peer)

    kv_sends = [
        kv_z(e, 0, 0, z_peer),
        kv_z(e, 1, 1, m_peer),
        kv_z(near * 2 + y, 2, 2, m_peer),
        kv_z(far_inner * 2 + y, 3, 1, z_peer),
        kv_z(far_outer * 2 + y, 4, 2, z_peer),
    ]

    def block(source, target, number, c, device):
        return remote(
            dense.at[source, :, cols(c)],
            dense.at[target, :, cols(c)],
            dn_out.at[number, c],
            dn_in.at[target, c],
            device,
        )

    def to_x(c):
        return block(0, 1, 1, c, x_peer)

    def to_near(c):
        return block(0, 2, 2, c, z_peer)

    def x_to_near(c):
        return block(1, 3, 3, c, z_peer)

    def to_across(c):
        return block(0, 4, 4, c, m_peer)

    def near_to_across(c):
        return block(2, 5, 5, c, m_peer)

    def far_to_near(k, c):
        return block(4 + k, 4 + k, 6 + k, c, z_peer)

    far_slot = jnp.where(inner, 4, 5)

    def card(slot, number, device):
        return remote(meta.at[0], meta.at[slot], meta_sems.at[0, number], meta_sems.at[1, slot], device)

    cards = [
        card(1, 1, x_peer),
        card(2, 2, z_peer),
        card(3, 3, corner),
        card(far_slot, 4, far_peers[0]),
        card(far_slot, 5, far_peers[1]),
    ]

    def row_to_y(b, c):
        return remote(
            y_send.at[b, :, cols(c)], rows.at[b, core, y, :, cols(c)], row_y.at[0, b, c], row_y.at[1, b, c], y_peer
        )

    def row_to_c(b, g, c):
        here = rows.at[b, core, g, :, cols(c)]
        return remote(here, here, row_c.at[0, b, g, c], row_c.at[1, b, g, c], c_peer)

    def row_to_x(k, g, c):
        return remote(
            rows.at[4 + k, core, g, :, cols(c)],
            rows.at[6 + k, core, g, :, cols(c)],
            row_x.at[0, k, g, c],
            row_x.at[1, k, g, c],
            x_peer,
        )

    def reduce_c(b, c):
        return remote(
            partial.at[b, other_core, :, :, cols(c)],
            red.at[b, :, :, cols(c)],
            red_sems.at[0, b, c],
            red_sems.at[1, b, c],
            c_peer,
        )

    def reduce_x(k, c):
        return remote(
            partial.at[6 + k, core, :, :, cols(c)],
            x_got.at[k, :, :, cols(c)],
            sum_x.at[0, k, c],
            sum_x.at[1, k, c],
            x_peer,
        )

    def give_y(b, c):
        return remote(
            partial.at[b, core, other_y, :, cols(c)],
            y_got.at[b, :, cols(c)],
            sum_y.at[0, b, c],
            sum_y.at[1, b, c],
            y_peer,
        )

    def pass_on(b, place, where, arrive, c, device):
        return remote(sent.at[b, :, cols(c)], where.at[place, :, cols(c)], t_out.at[b, c], arrive.at[place, c], device)

    mix_core = remote(a_part.at[:, other_core], a_red, mix_sems.at[0, 0], mix_sems.at[1, 0], c_peer)
    mix_side = remote(a_send, a_got, mix_sems.at[0, 1], mix_sems.at[1, 1], x_peer)

    def wait_for(message):
        kind = message[0]
        c = message[-1]
        k = message[1] if len(message) > 1 else 0
        if kind == "d":
            block(k, k, 0, c, x_peer).wait_recv()
        elif kind == "ry":
            remote(
                y_send.at[k, :, cols(c)],
                rows.at[k, core, other_y, :, cols(c)],
                row_y.at[0, k, c],
                row_y.at[1, k, c],
                y_peer,
            ).wait_recv()
        elif kind == "rc":
            g = groups[message[2]]
            there = rows.at[k, other_core, g, :, cols(c)]
            remote(there, there, row_c.at[0, k, g, c], row_c.at[1, k, g, c], c_peer).wait_recv()
        elif kind == "rx":
            row_to_x(k, groups[message[2]], c).wait_recv()
        elif kind == "red":
            reduce_c(k, c).wait_recv()
        elif kind == "xg":
            reduce_x(k, c).wait_recv()
        elif kind == "gy":
            give_y(k, c).wait_recv()
        elif kind == "zg":
            pass_on(1, k, z_got, z_in, c, z_peer).wait_recv()
        elif kind == "mg":
            pass_on(1, k, m_got, m_in, c, z_peer).wait_recv()
        elif kind == "pg":
            pass_on(1, k, p_got, p_in, c, z_peer).wait_recv()
        elif kind == "og":
            pass_on(1, 0, o_got, o_in, c, z_peer).wait_recv()
        elif kind == "kvz":
            kv_z(stops[k + 1] * 2 + y, 0, k, z_peer).wait_recv()
        elif kind == "kvy":
            owner = stops[k] * 2 + other_y
            remote(
                kv_all.at[:, owner], kv_all.at[:, owner], kvy_sems.at[0, k], kvy_sems.at[1, k], y_peer
            ).wait_recv()
        elif kind == "mc":
            mix_core.wait_recv()
        else:
            mix_side.wait_recv()

    row_id = lax.broadcasted_iota(jnp.int32, (tokens_here, tokens_here), 0)
    col_id = lax.broadcasted_iota(jnp.int32, (tokens_here, tokens_here), 1)
    before = (row_id < col_id).astype(jnp.bfloat16)
    after = (col_id < row_id).astype(jnp.bfloat16)

    def tiles(c, body):
        def run(j, carry):
            body(pl.ds(pl.multiple_of(c * part + j * 512, 512), 512))
            return carry

        lax.fori_loop(0, part // 512, run, 0)

    def build(b):
        named = meta[b]
        spread = []
        for expert in (e, y_expert):
            wanted = expert.astype(jnp.float32)
            hit = jnp.logical_or(named[0:1] == wanted, named[1:2] == wanted)
            spread.append(jnp.broadcast_to(hit.astype(jnp.float32)[:, :tokens_here], (cap, tokens_here)))
        spread = jnp.concatenate(spread, axis=0)
        rank = jnp.dot(spread.astype(jnp.bfloat16), before, preferred_element_type=jnp.float32)
        slot = f32(lax.rem(lax.broadcasted_iota(jnp.int32, rank.shape, 0), cap))
        chosen[b] = (jnp.where(rank == slot, 1.0, 0.0) * spread).astype(jnp.bfloat16)
        columns = jnp.transpose(named)[:tokens_here]
        for place, expert in enumerate((e, y_expert)):
            wanted = expert.astype(jnp.float32)
            hits = [(columns[:, k:k + 1] == wanted).astype(jnp.float32) for k in range(2)]
            scale = hits[0] * columns[:, 2:3] + hits[1] * columns[:, 3:4]
            spread = jnp.broadcast_to(hits[0] + hits[1], (tokens_here, cap))
            rank = jnp.dot(after, spread.astype(jnp.bfloat16), preferred_element_type=jnp.float32)
            slot = f32(lax.broadcasted_iota(jnp.int32, rank.shape, 1))
            picks[b, place] = (jnp.where(rank == slot, 1.0, 0.0) * spread).astype(jnp.bfloat16)
            scales[b, place] = jnp.broadcast_to(scale, (tokens_here, 128))

    def select(b, c):
        table = chosen[b]

        def body(span):
            found = jnp.dot(table, dense[b, :, span], preferred_element_type=jnp.float32).astype(jnp.bfloat16)
            rows[b, core, y, :, span] = found[:cap]
            y_send[b, :, span] = found[cap:]

        tiles(c, body)
        row_to_y(b, c).start()
        row_to_c(b, y, c).start()
        if b >= 4:
            row_to_x(b - 4, y, c).start()

    def finish(b, c):
        def body(span):
            value = f32(partial[b, core, :, :, span]) + f32(red[b, :, :, span])
            if b in (4, 5):
                value = value + f32(x_got[b - 4, :, :, span])
            partial[b, core, :, :, span] = value.astype(jnp.bfloat16)

        tiles(c, body)
        if b >= 6:
            reduce_x(b - 6, c).start()
        else:
            give_y(b, c).start()

    def gather(b, c):
        mine, theirs = picks[b, 0], picks[b, 1]
        scale_mine, scale_theirs = scales[b, 0, :, 0:1], scales[b, 1, :, 0:1]

        def body(span):
            first = jnp.dot(mine, partial[b, core, y, :, span], preferred_element_type=jnp.float32)
            second = jnp.dot(theirs, y_got[b, :, span], preferred_element_type=jnp.float32)
            hold[b, :, span] = first * scale_mine + second * scale_theirs

        tiles(c, body)

    def release(b, c, sources, place, where, arrive, device):
        def body(span):
            value = hold[b, :, span]
            for got, at in sources:
                value = value + f32(got[at, :, span])
            sent[b, :, span] = value.astype(jnp.bfloat16)

        tiles(c, body)
        pass_on(b, place, where, arrive, c, device).start()

    def messages(task, is_inner):
        kind = task[0]
        c = task[-1]
        b = task[1] if len(task) > 1 else 0
        whole = range(chunks)
        if kind in ("F3", "F6", "F5", "F7"):
            return [("d", {"F3": 1, "F6": 4, "F5": 2, "F7": 5}[kind], c)]
        if kind == "sel":
            return [("d", b, c)]
        if kind == "arr":
            return [("ry", b, c)]
        if kind == "arx":
            return [("rx", b, task[2], c)]
        if kind == "cmp":
            return [("rc", b, g, c) for g in range(2) for c in whole]
        if kind == "fin":
            return [("red", b, c)] + ([("xg", b - 4, c)] if b in (4, 5) else [])
        if kind == "gat":
            return [("gy", b, c)]
        if kind == "rel":
            if b == 1:
                return [("pg", 1, c)]
            if is_inner and b in (4, 5):
                return [("zg", b - 4, c)]
            return [("mg", 1, c)] if is_inner and b == 2 else []
        if kind == "final":
            return [("og", c), ("pg", 0, c)] + ([("mg", 0, c)] if is_inner else [])
        if kind == "kvf":
            return [("kvz", b)]
        if kind == "att":
            return [("kvy", j) for j in range(4)]
        return {"mixs": [("mc",)], "mixf": [("mx",)]}.get(kind, [])

    def perform(task, is_inner):
        kind = task[0]
        c = task[-1]
        b = task[1] if len(task) > 1 else 0
        if kind == "D2":
            to_near(c).start()
        elif kind == "F3":
            x_to_near(c).start()
        elif kind == "F6":
            far_to_near(0, c).start()
        elif kind == "F5":
            near_to_across(c).start()
        elif kind == "F7":
            far_to_near(1, c).start()
        elif kind == "meta":
            for slot in range(1, 6):
                card(slot, 0, x_peer).wait_recv()

            def run(slot, carry):
                build(slot)
                return carry

            lax.fori_loop(1, 6, run, 0)
        elif kind == "sel":
            select(b, c)
        elif kind == "arr":
            row_to_c(b, other_y, c).start()
            if b >= 4:
                row_to_x(b - 4, other_y, c).start()
        elif kind == "arx":
            row_to_c(6 + b, groups[task[2]], c).start()
        elif kind == "fin":
            finish(b, c)
        elif kind == "gat":
            gather(b, c)
        elif kind == "rel":
            if b == 1:
                release(b, c, [(p_got, 1)], 0, o_got, o_in, x_peer)
            elif b == 2:
                release(b, c, [(m_got, 1)] if is_inner else [], 0, p_got, p_in, z_peer)
            elif b == 3:
                release(b, c, [], 1, p_got, p_in, z_peer)
            elif is_inner:
                release(b, c, [(z_got, b - 4)], b - 4, m_got, m_in, m_peer)
            else:
                release(b, c, [], b - 4, z_got, z_in, z_peer)
        elif kind == "final":
            def body(span):
                value = hold[0, :, span] + f32(o_got[0, :, span]) + f32(p_got[0, :, span])
                if is_inner:
                    value = value + f32(m_got[0, :, span])
                moe[:, span] = value.astype(jnp.bfloat16)

            tiles(c, body)
        elif kind == "kvs":
            kv_sends[0].start()
            if is_inner:
                kv_sends[1].start()
            kv_y(0).start()
        elif kind == "kvf":
            if is_inner:
                kv_sends[2 + b].start()
            kv_y(b + 1).start()
        elif kind == "mixs":
            a_send[...] = (f32(a_part[other_side, core]) + f32(a_red[other_side])).astype(jnp.bfloat16)
            mix_side.start()
        elif kind == "mixf":
            mixed[...] = (f32(a_part[side, core]) + f32(a_red[side]) + f32(a_got[...])).astype(jnp.bfloat16)

    def plan(order, is_inner):
        seen = {("d", 0, c) for c in range(chunks)}
        pieces, kinds = [[]], []
        for task in order:
            fresh = [message for message in messages(task, is_inner) if message not in seen]
            seen.update(fresh)
            pieces[-1].append((fresh, task))
            if task[0] in BIG:
                kinds.append(BIG[task[0]] + (task[1] if len(task) > 1 else 0))
                pieces.append([])
        return pieces, kinds

    def emit(piece, is_inner):
        for fresh, task in piece:
            for message in fresh:
                wait_for(message)
            if task[0] not in BIG:
                perform(task, is_inner)

    as_float = f32(x_ref[...])
    mean = jnp.mean(as_float * as_float, axis=1, keepdims=True)
    dense[0] = (as_float * lax.rsqrt(mean + NORM_EPS) * x_gain[...]).astype(jnp.bfloat16)
    meta[0] = jnp.zeros(meta.shape[1:], jnp.float32)
    meta[0, 0:2, 0:tokens_here] = f32(routes_row[...])
    meta[0, 2:4, 0:tokens_here] = weight_row[...]

    pl.semaphore_wait(barrier, len(greeted))
    for item in cards:
        item.start()
    for c in range(chunks):
        to_x(c).start()

        @pl.when(inner)
        def _():
            to_across(c).start()

        if c == 0:
            to_near(c).start()
        else:
            @pl.when(outer)
            def _():
                to_near(c).start()

    build(0)
    for c in range(chunks):
        select(0, c)

    loads[0].wait()
    lane = lax.broadcasted_iota(jnp.int32, (tok, 128), 1)
    low = lane < HEAD_DIM
    even = lax.rem(lax.div(lane, HEAD_DIM // 4), 2) == 0
    table = turn[...]
    swapped = pltpu.roll(table, HEAD_DIM, 1)
    cosine = jnp.where(low, table, swapped)
    sine = jnp.where(low, swapped, table)

    def turned(raw, gain):
        flat = f32(raw)
        square = flat * flat
        left = jnp.sum(jnp.where(low, square, 0.0), axis=1, keepdims=True)
        right = jnp.sum(jnp.where(low, 0.0, square), axis=1, keepdims=True)
        mean_square = jnp.where(low, left, right) * (1.0 / HEAD_DIM)
        unit = flat * lax.rsqrt(mean_square + NORM_EPS) * gain
        partner = jnp.where(
            even, -pltpu.roll(unit, 128 - HEAD_DIM // 4, 1), pltpu.roll(unit, HEAD_DIM // 4, 1)
        )
        return unit * cosine + partner * sine

    for pair in range(kv_all.shape[0] // 2):
        span = slice(pair * 128, (pair + 1) * 128)
        k_rows = turned(k_raw[:, span], k_gain[:, span])
        v_rows = f32(v_raw[:, span])
        kv_all[2 * pair, e] = jnp.where(low, k_rows, pltpu.roll(v_rows, HEAD_DIM, 1)).astype(jnp.bfloat16)
        kv_all[2 * pair + 1, e] = jnp.where(low, pltpu.roll(k_rows, HEAD_DIM, 1), v_rows).astype(jnp.bfloat16)

    for pair in range(pairs):
        span = slice(pair * 128, (pair + 1) * 128)
        q_rows = turned(q_raw[:, span], q_gain[:, span])
        q_ref[2 * pair] = jnp.where(low, q_rows, 0.0).astype(jnp.bfloat16)
        q_ref[2 * pair + 1] = jnp.where(low, pltpu.roll(q_rows, HEAD_DIM, 1), 0.0).astype(jnp.bfloat16)

    for load in loads[1:]:
        load.wait()

    def attend(pair):
        kv = kv_all[lax.div(pair * 2 * kv_all.shape[0], pairs * 2)].reshape(n * tok, 128)
        halves = []
        for h in range(2):
            scores = lax.dot_general(
                q_ref[pair * 2 + h], kv, (((1,), (1,)), ((), ())), preferred_element_type=jnp.float32
            ) * (HEAD_DIM ** (-0.5))
            peak = jnp.max(scores, axis=1, keepdims=True)
            weights = jnp.exp(scores - peak)
            total = jnp.sum(weights, axis=1, keepdims=True)
            summed = jnp.dot(weights.astype(jnp.bfloat16), kv, preferred_element_type=jnp.float32)
            halves.append(summed / total)
        joined = jnp.where(low, pltpu.roll(halves[0], HEAD_DIM, 1), halves[1])
        attended[pair] = joined.astype(jnp.bfloat16)

    inner_pieces, inner_kinds = plan(INNER_ORDER, True)
    outer_pieces, outer_kinds = plan(OUTER_ORDER, False)
    count = len(inner_kinds)

    def step(s, carry):
        u = jnp.where(inner, inner_kinds[0], outer_kinds[0])
        for place in range(1, count):
            u = jnp.where(s == place, jnp.where(inner, inner_kinds[place], outer_kinds[place]), u)
        for place in range(count):
            @pl.when(jnp.logical_and(s == place, inner))
            def _():
                emit(inner_pieces[place], True)

            @pl.when(jnp.logical_and(s == place, outer))
            def _():
                emit(outer_pieces[place], False)

        @pl.when(u < 8)
        def _():
            tokens = rows[u].reshape(4 * cap, width)
            gate = jnp.dot(tokens, wg[...], preferred_element_type=jnp.float32)
            up = jnp.dot(tokens, wu[...], preferred_element_type=jnp.float32)
            hidden = (gate / (1.0 + jnp.exp(-gate)) * up).astype(jnp.bfloat16)
            for tile in range(0, width, TILE):
                product = jnp.dot(hidden, wd[:, tile:tile + TILE], preferred_element_type=jnp.float32)
                partial[u, :, :, :, tile:tile + TILE] = product.astype(jnp.bfloat16).reshape(2, 2, cap, TILE)
                if (tile + TILE) % part == 0:
                    reduce_c(u, tile // part).start()

        @pl.when(jnp.logical_and(u >= 8, u < 10))
        def _():
            attend(2 * (u - 8))
            attend(2 * (u - 8) + 1)

        @pl.when(u == 10)
        def _():
            for tile in range(0, width, TILE):
                product = jnp.dot(attended[0], ow[0, :, tile:tile + TILE], preferred_element_type=jnp.float32)
                for p in range(1, pairs):
                    product += jnp.dot(attended[p], ow[p, :, tile:tile + TILE], preferred_element_type=jnp.float32)
                a_part[:, :, :, tile:tile + TILE] = product.astype(jnp.bfloat16).reshape(2, 2, tok // 4, TILE)
            mix_core.start()

        return carry

    lax.fori_loop(0, count, step, 0)

    @pl.when(inner)
    def _():
        emit(inner_pieces[count], True)

    @pl.when(outer)
    def _():
        emit(outer_pieces[count], False)

    mix_core.wait_send()
    mix_side.wait_send()
    for j in range(4):
        kv_y(j).wait_send()
    kv_sends[0].wait_send()
    for item in cards:
        item.wait_send()

    @pl.when(inner)
    def _():
        for item in kv_sends[1:]:
            item.wait_send()

    for c in range(chunks):
        to_x(c).wait_send()
        to_near(c).wait_send()
        x_to_near(c).wait_send()

        @pl.when(inner)
        def _():
            to_across(c).wait_send()
            near_to_across(c).wait_send()
            far_to_near(0, c).wait_send()
            far_to_near(1, c).wait_send()

        for b in range(1, 6):
            pass_on(b, 0, o_got, o_in, c, x_peer).wait_send()
        for k in range(2):
            for g in range(2):
                row_to_x(k, g, c).wait_send()
            reduce_x(k, c).wait_send()
        for b in range(6):
            row_to_y(b, c).wait_send()
            give_y(b, c).wait_send()
        for b in range(8):
            for g in range(2):
                row_to_c(b, g, c).wait_send()
            reduce_c(b, c).wait_send()


def turn_table(tokens):
    quarter = HEAD_DIM // 4
    inverse = np.power(ROPE_BASE, -np.arange(quarter, dtype=np.float64) / quarter)
    places = np.arange(tokens)
    row = (places // GRID_W)[:, None] * inverse
    col = (places % GRID_W)[:, None] * inverse
    angles = np.concatenate([row, row, col, col], axis=1)
    return np.concatenate([np.cos(angles), np.sin(angles)], axis=1).astype(np.float32)


def fused(x, x_gain, routes, route_weight, queries, keys, values, q_gain, k_gain, gate_weight, up_weight, down_weight, out_weight):
    n = lax.axis_size("ep")
    tok_exp, width = x.shape
    cap = 2 * routes.shape[1] * tok_exp // n
    tok = queries.shape[0]
    heads = queries.shape[1] // HEAD_DIM
    kv_count = keys.shape[1] // HEAD_DIM
    pairs = heads // 2
    hidden = gate_weight.shape[1]
    bf = jnp.bfloat16
    vmem = pl.BlockSpec(memory_space=pltpu.VMEM)
    anywhere = pl.BlockSpec(memory_space=pl.ANY)
    dma = pltpu.SemaphoreType.DMA
    return pl.pallas_call(
        functools.partial(fused_kernel, n),
        out_shape=(
            jax.ShapeDtypeStruct((tok_exp, width), bf),
            jax.ShapeDtypeStruct((tok // 4, width), bf),
        ),
        in_specs=[vmem] * 9 + [anywhere] * 5,
        out_specs=(vmem, vmem),
        scratch_shapes=[
            pltpu.VMEM((6, tok_exp, width), bf),
            pltpu.VMEM((6, 8, 128), jnp.float32),
            pltpu.VMEM((6, 2 * cap, tok_exp), bf),
            pltpu.VMEM((6, 2, tok_exp, cap), bf),
            pltpu.VMEM((6, 2, tok_exp, 128), jnp.float32),
            pltpu.VMEM((8, 2, 2, cap, width), bf),
            pltpu.VMEM((6, cap, width), bf),
            pltpu.VMEM((8, 2, 2, cap, width), bf),
            pltpu.VMEM((8, 2, cap, width), bf),
            pltpu.VMEM((2, 2, cap, width), bf),
            pltpu.VMEM((6, cap, width), bf),
            pltpu.VMEM((6, tok_exp, width), jnp.float32),
            pltpu.VMEM((6, tok_exp, width), bf),
            pltpu.VMEM((2, tok_exp, width), bf),
            pltpu.VMEM((2, tok_exp, width), bf),
            pltpu.VMEM((2, tok_exp, width), bf),
            pltpu.VMEM((1, tok_exp, width), bf),
            pltpu.VMEM((heads, tok, 128), bf),
            pltpu.VMEM((tok, 128), jnp.float32),
            pltpu.VMEM((width, hidden), bf),
            pltpu.VMEM((width, hidden), bf),
            pltpu.VMEM((hidden, width), bf),
            pltpu.VMEM((pairs, 128, width), bf),
            pltpu.VMEM((kv_count, n, tok, 128), bf),
            pltpu.VMEM((pairs, tok, 128), bf),
            pltpu.VMEM((2, 2, tok // 4, width), bf),
            pltpu.VMEM((2, tok // 4, width), bf),
            pltpu.VMEM((tok // 4, width), bf),
            pltpu.VMEM((tok // 4, width), bf),
            dma((5,)),
            dma((5,)),
            dma((3,)),
            dma((2, 4)),
            dma((8, CHUNKS)),
            dma((6, CHUNKS)),
            dma((2, 6)),
            dma((2, 6, CHUNKS)),
            dma((2, 8, 2, CHUNKS)),
            dma((2, 2, 2, CHUNKS)),
            dma((2, 8, CHUNKS)),
            dma((2, 2, CHUNKS)),
            dma((2, 6, CHUNKS)),
            dma((6, CHUNKS)),
            dma((2, CHUNKS)),
            dma((2, CHUNKS)),
            dma((2, CHUNKS)),
            dma((1, CHUNKS)),
            dma((2, 2)),
        ],
        compiler_params=pltpu.CompilerParams(
            collective_id=0, has_side_effects=True, vmem_limit_bytes=62 * 1024 * 1024
        ),
    )(
        x,
        x_gain.reshape(1, width),
        jnp.transpose(routes),
        jnp.transpose(route_weight),
        queries,
        keys,
        values,
        q_gain.reshape(1, -1),
        k_gain.reshape(1, -1),
        jnp.asarray(turn_table(n * tok)),
        gate_weight,
        up_weight,
        down_weight,
        out_weight.reshape(pairs, 128, width),
    )


def plain_shards(
    queries,
    keys,
    values,
    query_gain,
    key_gain,
    out_weight,
    expert_input,
    norm_gain,
    routes,
    route_weight,
    gate_weight,
    up_weight,
    down_weight,
):
    tok_mix = queries.shape[0]
    head_count = query_gain.shape[0] // HEAD_DIM
    kv_count = key_gain.shape[0] // HEAD_DIM
    group_size = head_count // kv_count
    offset = lax.axis_index("ep") * tok_mix
    q_turned = head_norm(queries, query_gain, head_count, offset)
    k_turned = head_norm(keys, key_gain, kv_count, offset)
    grouped = q_turned.reshape(tok_mix, kv_count, group_size, HEAD_DIM)
    score_scale = HEAD_DIM ** (-0.5)
    start_state = (
        jnp.full((kv_count, group_size, tok_mix), -jnp.inf, jnp.float32),
        jnp.zeros((kv_count, group_size, tok_mix), jnp.float32),
        jnp.zeros((tok_mix, kv_count, group_size, HEAD_DIM), jnp.float32),
    )
    running = start_state
    key_piece = lax.all_gather(k_turned, "ep", axis=0, tiled=True)
    value_piece = lax.all_gather(values, "ep", axis=0, tiled=True)
    length = key_piece.shape[0]
    block_len = length
    while block_len > 2048 and block_len % 2 == 0:
        block_len = block_len // 2
    key_blocks = key_piece.reshape(length // block_len, block_len, key_piece.shape[1])
    value_blocks = value_piece.reshape(length // block_len, block_len, value_piece.shape[1])

    def advance(inner_state, key_value):
        return (absorb(inner_state, key_value[0], key_value[1], grouped, score_scale), None)

    running, unused = lax.scan(advance, running, (key_blocks, value_blocks))
    final_max, weight_sum, summed = running
    attended = (
        (summed / jnp.transpose(weight_sum, (2, 0, 1))[..., None])
        .reshape(tok_mix, -1)
        .astype(jnp.bfloat16)
    )
    mixed = lax.psum_scatter(
        jnp.dot(attended, out_weight, preferred_element_type=jnp.float32).astype(jnp.bfloat16),
        "tp",
        scatter_dimension=0,
        tiled=True,
    )
    tok_exp = expert_input.shape[0]
    top_count = routes.shape[1]
    expert_count = lax.axis_size("ep")
    capacity = 2 * top_count * tok_exp // expert_count
    as_float = expert_input.astype(jnp.float32)
    normed = (
        as_float
        * lax.rsqrt(jnp.mean(as_float * as_float, axis=-1, keepdims=True) + NORM_EPS)
        * norm_gain
    ).astype(jnp.bfloat16)
    flat_routes = routes.reshape(-1)
    route_hits = (
        flat_routes[:, None] == jnp.arange(expert_count, dtype=jnp.int32)[None, :]
    ).astype(jnp.int32)
    slot_rank = jnp.sum((jnp.cumsum(route_hits, axis=0) - route_hits) * route_hits, axis=1)
    slot_ids = flat_routes * capacity + slot_rank
    placed = jnp.arange(expert_count * capacity, dtype=jnp.int32)[:, None] == slot_ids[None, :]
    placed = jnp.any(placed.reshape(expert_count * capacity, tok_exp, top_count), axis=2).astype(
        jnp.bfloat16
    )
    outbound = jnp.dot(placed, normed, preferred_element_type=jnp.float32).astype(jnp.bfloat16)
    model_width = outbound.shape[1]
    half_cap = capacity // 2
    laid = outbound.reshape(expert_count, capacity, model_width)
    first_half = run_experts(
        laid[:, :half_cap].reshape(expert_count * half_cap, model_width),
        gate_weight,
        up_weight,
        down_weight,
    )
    second_half = run_experts(
        laid[:, half_cap:].reshape(expert_count * half_cap, model_width),
        gate_weight,
        up_weight,
        down_weight,
    )
    back_rows = jnp.concatenate(
        [
            first_half.reshape(expert_count, half_cap, model_width),
            second_half.reshape(expert_count, half_cap, model_width),
        ],
        axis=1,
    )
    back_rows = back_rows.reshape(expert_count * capacity, model_width)
    picked = back_rows[slot_ids.reshape(tok_exp, top_count)]
    moe_out = jnp.sum(picked.astype(jnp.float32) * route_weight[:, :, None], axis=1).astype(
        jnp.bfloat16
    )
    return (mixed, moe_out)


def shards(
    queries,
    keys,
    values,
    query_gain,
    key_gain,
    out_weight,
    expert_input,
    norm_gain,
    routes,
    route_weight,
    gate_weight,
    up_weight,
    down_weight,
):
    tok_exp = expert_input.shape[0]
    top_count = routes.shape[1]
    expert_count = lax.axis_size("ep")
    capacity = 2 * top_count * tok_exp // expert_count
    if capacity % 16 != 0 or lax.axis_size("tp") != 4 or expert_count != 8:
        return plain_shards(
            queries,
            keys,
            values,
            query_gain,
            key_gain,
            out_weight,
            expert_input,
            norm_gain,
            routes,
            route_weight,
            gate_weight,
            up_weight,
            down_weight,
        )
    moe_out, mixed = fused(
        expert_input,
        norm_gain,
        routes,
        route_weight,
        queries,
        keys,
        values,
        query_gain,
        key_gain,
        gate_weight[0],
        up_weight[0],
        down_weight[0],
        out_weight,
    )
    return (mixed, moe_out)


def solution(mesh):
    placed = (
        P("ep", "tp"),
        P("ep", "tp"),
        P("ep", "tp"),
        P("tp"),
        P("tp"),
        P("tp", None),
        P(("ep", "tp"), None),
        P(),
        P(("ep", "tp"), None),
        P(("ep", "tp"), None),
        P("ep", None, "tp"),
        P("ep", None, "tp"),
        P("ep", "tp", None),
    )
    return jax.shard_map(
        shards,
        mesh=mesh,
        in_specs=placed,
        out_specs=(P(("ep", "tp"), None), P(("ep", "tp"), None)),
        check_vma=False,
    )
```

```python
import functools

import jax
import jax.numpy as jnp
import numpy as np
from jax import lax
from jax.experimental import pallas as pl
from jax.experimental.pallas import tpu as pltpu
from jax.sharding import PartitionSpec as P

HEAD_DIM = 64
GRID_W = 128


NORM_EPS = 1e-06
ROPE_BASE = 10000.0


def rotate(vectors, grid_rows, grid_cols):
    quarter = vectors.shape[-1] // 4
    inverse = ROPE_BASE ** (-jnp.arange(quarter, dtype=jnp.float32) / quarter)
    angle_row = grid_rows[:, None] * inverse
    angle_col = grid_cols[:, None] * inverse
    angles = jnp.concatenate([angle_row, angle_row, angle_col, angle_col], axis=-1)[:, None, :]
    part_one, part_two, part_three, part_four = jnp.split(vectors, 4, axis=-1)
    turned = jnp.concatenate([-part_two, part_one, -part_four, part_three], axis=-1)
    return vectors * jnp.cos(angles) + turned * jnp.sin(angles)


def head_norm(raw_rows, gains, head_count, offset):
    row_count = raw_rows.shape[0]
    flat_rows = raw_rows.astype(jnp.float32).reshape(row_count, head_count, -1)
    unit_vec = flat_rows * lax.rsqrt(
        jnp.mean(flat_rows * flat_rows, axis=-1, keepdims=True) + NORM_EPS
    )
    unit_vec = unit_vec * gains.reshape(head_count, -1)
    places = offset + jnp.arange(row_count, dtype=jnp.int32)
    grid_rows = (places // GRID_W).astype(jnp.float32)
    grid_cols = (places % GRID_W).astype(jnp.float32)
    return rotate(unit_vec, grid_rows, grid_cols).astype(jnp.bfloat16).reshape(row_count, -1)


def absorb(running, key_block, value_block, grouped, score_scale):
    run_max, weight_sum, summed = running
    kv_count = grouped.shape[1]
    key_heads = key_block.reshape(key_block.shape[0], kv_count, -1)
    value_heads = value_block.reshape(value_block.shape[0], kv_count, -1)
    scores = (
        jnp.einsum("qhgd,khd->hgqk", grouped, key_heads, preferred_element_type=jnp.float32)
        * score_scale
    )
    new_max = jnp.maximum(run_max, jnp.max(scores, axis=-1))
    rescale = jnp.exp(run_max - new_max)
    weights = jnp.exp(scores - new_max[..., None])
    weight_sum = weight_sum * rescale + jnp.sum(weights, axis=-1)
    update = jnp.einsum(
        "hgqk,khd->qhgd",
        weights.astype(jnp.bfloat16),
        value_heads,
        preferred_element_type=jnp.float32,
    )
    summed = summed * jnp.transpose(rescale, (2, 0, 1))[..., None] + update
    return (new_max, weight_sum, summed)


def run_experts(sending, gate_weight, up_weight, down_weight):
    arrived = lax.all_to_all(sending, "ep", split_axis=0, concat_axis=0, tiled=True)
    shard_rows = lax.all_gather(arrived, "tp", axis=0, tiled=True)
    gate_out = jnp.dot(shard_rows, gate_weight[0], preferred_element_type=jnp.float32)
    up_out = jnp.dot(shard_rows, up_weight[0], preferred_element_type=jnp.float32)
    hidden = (jax.nn.silu(gate_out) * up_out).astype(jnp.bfloat16)
    results = lax.psum_scatter(
        jnp.dot(hidden, down_weight[0], preferred_element_type=jnp.float32).astype(jnp.bfloat16),
        "tp",
        scatter_dimension=0,
        tiled=True,
    )
    return lax.all_to_all(results, "ep", split_axis=0, concat_axis=0, tiled=True)


MESH = pl.DeviceIdType.MESH
TILE = 1024
CHUNKS = 4


def flip(index, pattern, size):
    result = 0
    bit = 1
    while bit < size:
        both = lax.rem(lax.div(index, bit) + lax.div(pattern, bit), 2)
        result = result + both * bit
        bit = bit * 2
    return result


def f32(value):
    return value.astype(jnp.float32)


INNER_ORDER = (
    ("F6", 0), ("meta",), ("sel", 2, 0), ("F6", 1), ("sel", 2, 1), ("sel", 4, 0), ("F5", 0), ("F6", 2),
    ("F5", 2), ("sel", 4, 1), ("F5", 1), ("sel", 1, 1), ("sel", 4, 2), ("arr", 2, 0), ("F3", 0),
    ("arr", 0, 1), ("arr", 0, 2), ("arr", 0, 0), ("sel", 1, 3), ("F3", 1), ("sel", 5, 0), ("F3", 3),
    ("sel", 2, 3), ("arr", 4, 1), ("arr", 1, 3), ("sel", 3, 0), ("arr", 1, 1), ("arx", 0, 0, 1), ("F3", 2),
    ("sel", 2, 2), ("sel", 4, 3), ("arr", 5, 0), ("sel", 1, 0), ("F6", 3), ("sel", 5, 2), ("F5", 3),
    ("sel", 1, 2), ("F7", 3), ("F7", 0), ("sel", 5, 3), ("F7", 2), ("sel", 3, 1), ("arr", 0, 3),
    ("arr", 2, 3), ("arr", 4, 3), ("sel", 3, 2), ("F7", 1), ("sel", 5, 1), ("arr", 1, 2), ("arr", 5, 2),
    ("sel", 3, 3), ("arr", 4, 0), ("arr", 4, 2), ("arr", 1, 0), ("arx", 0, 1, 1), ("arx", 0, 1, 3),
    ("cmp", 4), ("kvf", 0), ("arx", 1, 1, 0), ("arr", 2, 2), ("kvs",), ("arx", 0, 1, 0), ("arr", 2, 1),
    ("cmp", 0), ("arx", 0, 0, 2), ("arr", 3, 1), ("arr", 3, 2), ("cmp", 1), ("arx", 0, 0, 3), ("arr", 3, 0),
    ("arx", 0, 1, 2), ("arx", 1, 0, 1), ("arx", 0, 0, 0), ("arr", 3, 3), ("arr", 5, 3), ("kvf", 1),
    ("kvf", 2), ("arx", 1, 1, 2), ("arx", 1, 0, 3), ("fin", 1, 3), ("arx", 1, 0, 0), ("arr", 5, 1),
    ("cmp", 6), ("fin", 1, 2), ("D2", 1), ("cmp", 3), ("fin", 6, 2), ("fin", 6, 1), ("D2", 2), ("fin", 6, 3),
    ("cmp", 2), ("arx", 1, 1, 3), ("cmp", 5), ("fin", 3, 2), ("arx", 1, 1, 1), ("fin", 3, 0), ("att", 0),
    ("fin", 1, 0), ("arx", 1, 0, 2), ("fin", 6, 0), ("gat", 1, 3), ("fin", 4, 1), ("fin", 3, 1),
    ("fin", 4, 2), ("fin", 3, 3), ("fin", 2, 0), ("cmp", 7), ("fin", 7, 2), ("gat", 3, 2), ("D2", 3),
    ("fin", 7, 0), ("fin", 4, 0), ("fin", 2, 2), ("att", 1), ("fin", 2, 3), ("fin", 4, 3), ("rel", 3, 2),
    ("fin", 7, 1), ("gat", 3, 1), ("gat", 4, 2), ("gat", 3, 3), ("rel", 3, 3), ("gat", 2, 0), ("fin", 7, 3),
    ("fin", 5, 0), ("mixp",), ("gat", 1, 2), ("fin", 0, 0), ("gat", 3, 0), ("rel", 4, 2), ("rel", 1, 2),
    ("rel", 3, 0), ("fin", 2, 1), ("fin", 5, 1), ("gat", 5, 0), ("rel", 3, 1), ("fin", 5, 2), ("gat", 4, 3),
    ("rel", 5, 0), ("gat", 1, 0), ("gat", 4, 0), ("mixs",), ("gat", 2, 2), ("gat", 2, 1), ("fin", 5, 3),
    ("fin", 1, 1), ("fin", 0, 2), ("fin", 0, 1), ("rel", 4, 3), ("gat", 5, 2), ("gat", 0, 0), ("rel", 2, 0),
    ("rel", 1, 0), ("gat", 5, 1), ("rel", 5, 2), ("gat", 5, 3), ("rel", 5, 1), ("gat", 0, 1), ("rel", 2, 2),
    ("rel", 5, 3), ("mixf",), ("gat", 4, 1), ("gat", 2, 3), ("rel", 1, 3), ("gat", 1, 1), ("fin", 0, 3),
    ("rel", 2, 1), ("rel", 4, 0), ("rel", 1, 1), ("rel", 2, 3), ("rel", 4, 1), ("gat", 0, 3), ("gat", 0, 2),
    ("final", 2), ("final", 1), ("final", 0), ("final", 3),
)
OUTER_ORDER = (
    ("F3", 0), ("meta",), ("arr", 0, 0), ("sel", 1, 0), ("F3", 1), ("sel", 4, 0), ("F3", 2), ("sel", 2, 0),
    ("arr", 0, 3), ("sel", 1, 2), ("arr", 0, 2), ("kvs",), ("arr", 0, 1), ("sel", 4, 1), ("sel", 1, 3),
    ("sel", 1, 1), ("arr", 1, 0), ("F3", 3), ("sel", 3, 0), ("arr", 4, 0), ("sel", 4, 2), ("cmp", 0),
    ("arx", 0, 0, 0), ("arr", 1, 2), ("sel", 3, 1), ("sel", 3, 3), ("arr", 4, 1), ("fin", 0, 3),
    ("sel", 3, 2), ("arr", 1, 3), ("arr", 4, 2), ("arr", 3, 1), ("fin", 0, 0), ("sel", 4, 3), ("arr", 3, 0),
    ("arr", 3, 2), ("fin", 0, 2), ("arx", 0, 1, 2), ("arr", 3, 3), ("sel", 5, 3), ("cmp", 3),
    ("arx", 0, 0, 3), ("arr", 4, 3), ("arx", 0, 1, 0), ("sel", 5, 0), ("arx", 0, 0, 2), ("arr", 5, 3),
    ("fin", 3, 1), ("arx", 0, 1, 3), ("fin", 3, 3), ("arx", 0, 1, 1), ("arx", 0, 0, 1), ("gat", 0, 3),
    ("sel", 5, 2), ("arr", 5, 0), ("cmp", 6), ("fin", 3, 0), ("gat", 3, 1), ("sel", 5, 1), ("fin", 3, 2),
    ("fin", 6, 2), ("cmp", 4), ("kvf", 0), ("rel", 3, 1), ("arr", 1, 1), ("arx", 1, 0, 3), ("gat", 3, 3),
    ("arx", 1, 0, 2), ("arx", 1, 0, 0), ("arx", 1, 1, 0), ("gat", 3, 0), ("arr", 5, 2), ("arr", 5, 1),
    ("kvf", 1), ("fin", 6, 3), ("arx", 1, 1, 3), ("rel", 3, 0), ("cmp", 1), ("cmp", 5), ("arx", 1, 1, 2),
    ("arx", 1, 0, 1), ("fin", 4, 2), ("rel", 3, 3), ("gat", 3, 2), ("fin", 6, 1), ("arx", 1, 1, 1),
    ("rel", 3, 2), ("kvf", 2), ("cmp", 7), ("fin", 4, 3), ("fin", 7, 0), ("sel", 2, 2), ("gat", 4, 2),
    ("rel", 4, 2), ("fin", 7, 2), ("fin", 7, 3), ("fin", 7, 1), ("fin", 4, 1), ("fin", 1, 3), ("sel", 2, 1),
    ("gat", 4, 3), ("rel", 4, 3), ("att", 0), ("gat", 4, 1), ("fin", 5, 0), ("rel", 4, 1), ("att", 1),
    ("fin", 5, 2), ("gat", 5, 0), ("rel", 5, 0), ("sel", 2, 3), ("fin", 6, 0), ("fin", 5, 3), ("mixp",),
    ("gat", 5, 2), ("rel", 5, 2), ("fin", 5, 1), ("fin", 1, 0), ("gat", 1, 3), ("gat", 0, 0), ("rel", 1, 3),
    ("arr", 2, 2), ("arr", 2, 1), ("mixs",), ("gat", 5, 3), ("rel", 5, 3), ("arr", 2, 0), ("fin", 4, 0),
    ("fin", 1, 1), ("arr", 2, 3), ("gat", 5, 1), ("rel", 5, 1), ("fin", 1, 2), ("cmp", 2), ("gat", 4, 0),
    ("fin", 2, 1), ("fin", 2, 2), ("fin", 2, 3), ("rel", 4, 0), ("fin", 2, 0), ("gat", 1, 0), ("gat", 1, 2),
    ("gat", 0, 2), ("gat", 1, 1), ("rel", 1, 1), ("gat", 2, 1), ("rel", 2, 1), ("rel", 1, 0), ("gat", 2, 2),
    ("rel", 2, 2), ("gat", 2, 0), ("gat", 2, 3), ("rel", 2, 0), ("rel", 1, 2), ("fin", 0, 1), ("rel", 2, 3),
    ("gat", 0, 1), ("mixf",), ("final", 3), ("final", 2), ("final", 0), ("final", 1),
)


BIG = {"cmp": 0, "att": 8, "mixp": 10}


def fused_kernel(
    n,
    x_ref,
    x_gain,
    routes_row,
    weight_row,
    q_raw,
    k_raw,
    v_raw,
    q_gain,
    k_gain,
    turn_hbm,
    wg_hbm,
    wu_hbm,
    wd_hbm,
    ow_hbm,
    moe,
    mixed,
    dense,
    meta,
    chosen,
    picks,
    scales,
    rows,
    y_send,
    partial,
    red,
    x_got,
    y_got,
    hold,
    sent,
    z_got,
    m_got,
    p_got,
    o_got,
    q_ref,
    turn,
    wg,
    wu,
    wd,
    ow,
    kv_all,
    attended,
    a_part,
    a_red,
    a_send,
    a_got,
    load_sem,
    kvz_out,
    kvz_in,
    kvy_sems,
    dn_out,
    dn_in,
    meta_sems,
    row_y,
    row_c,
    row_x,
    red_sems,
    sum_x,
    sum_y,
    t_out,
    z_in,
    m_in,
    p_in,
    o_in,
    mix_sems,
):
    e = lax.axis_index("ep")
    t = lax.axis_index("tp")
    side = lax.div(t, 2)
    core = lax.rem(t, 2)
    other_side = 1 - side
    other_core = 1 - core
    layer = lax.div(e, 2)
    y = lax.rem(e, 2)
    other_y = 1 - y
    near = layer + 1 - 2 * lax.rem(layer, 2)
    last = n // 2 - 1
    across = last - layer
    inner = jnp.logical_and(layer > 0, layer < last)
    outer = jnp.logical_not(inner)
    half = lax.div(layer, 2)
    far_inner = 2 - half
    far_outer = last * (1 - half)
    x_tp = other_side * 2 + core
    x_peer = (e, x_tp)
    c_peer = (e, side * 2 + other_core)
    y_expert = layer * 2 + other_y
    y_peer = (y_expert, t)
    z_peer = (near * 2 + y, t)
    m_peer = (across * 2 + y, t)
    corner = (near * 2 + y, x_tp)
    cap, width = rows.shape[3], rows.shape[4]
    pairs = attended.shape[0]
    tok = attended.shape[1]
    tokens_here = x_ref.shape[0]
    chunks = dn_in.shape[1]
    part = width // chunks
    groups = (y, other_y)

    def remote(src, dst, send, recv, device):
        return pltpu.make_async_remote_copy(
            src_ref=src, dst_ref=dst, send_sem=send, recv_sem=recv, device_id=device, device_id_type=MESH
        )

    def cols(c):
        return pl.ds(c * part, part)

    loads = [
        pltpu.make_async_copy(a, b, load_sem.at[k])
        for k, (a, b) in enumerate(
            [
                (turn_hbm.at[pl.ds(pl.multiple_of(e * tok, 8), tok)], turn),
                (wg_hbm, wg),
                (wu_hbm, wu),
                (wd_hbm, wd),
                (ow_hbm, ow),
            ]
        )
    ]
    for load in loads:
        load.start()

    far_peers = [(far_inner * 2 + y, t), (far_outer * 2 + y, t)]
    barrier = pltpu.get_barrier_semaphore()
    greeted = [x_peer, c_peer, y_peer, z_peer, corner] + far_peers
    for peer in greeted:
        pl.semaphore_signal(barrier, inc=1, device_id=peer, device_id_type=MESH)

    def kv_z(owner, out, place, device):
        return remote(kv_all.at[:, owner], kv_all.at[:, owner], kvz_out.at[out], kvz_in.at[place], device)

    stops = [layer, near, far_inner, far_outer]

    def kv_y(j):
        owner = stops[j] * 2 + y
        return remote(kv_all.at[:, owner], kv_all.at[:, owner], kvy_sems.at[0, j], kvy_sems.at[1, j], y_peer)

    kv_sends = [
        kv_z(e, 0, 0, z_peer),
        kv_z(e, 1, 1, m_peer),
        kv_z(near * 2 + y, 2, 2, m_peer),
        kv_z(far_inner * 2 + y, 3, 1, z_peer),
        kv_z(far_outer * 2 + y, 4, 2, z_peer),
    ]

    def block(source, target, number, c, device):
        return remote(
            dense.at[source, :, cols(c)],
            dense.at[target, :, cols(c)],
            dn_out.at[number, c],
            dn_in.at[target, c],
            device,
        )

    def to_x(c):
        return block(0, 1, 1, c, x_peer)

    def to_near(c):
        return block(0, 2, 2, c, z_peer)

    def x_to_near(c):
        return block(1, 3, 3, c, z_peer)

    def to_across(c):
        return block(0, 4, 4, c, m_peer)

    def near_to_across(c):
        return block(2, 5, 5, c, m_peer)

    def far_to_near(k, c):
        return block(4 + k, 4 + k, 6 + k, c, z_peer)

    far_slot = jnp.where(inner, 4, 5)

    def card(slot, number, device):
        return remote(meta.at[0], meta.at[slot], meta_sems.at[0, number], meta_sems.at[1, slot], device)

    cards = [
        card(1, 1, x_peer),
        card(2, 2, z_peer),
        card(3, 3, corner),
        card(far_slot, 4, far_peers[0]),
        card(far_slot, 5, far_peers[1]),
    ]

    def row_to_y(b, c):
        return remote(
            y_send.at[b, :, cols(c)], rows.at[b, core, y, :, cols(c)], row_y.at[0, b, c], row_y.at[1, b, c], y_peer
        )

    def row_to_c(b, g, c):
        here = rows.at[b, core, g, :, cols(c)]
        return remote(here, here, row_c.at[0, b, g, c], row_c.at[1, b, g, c], c_peer)

    def row_to_x(k, g, c):
        return remote(
            rows.at[4 + k, core, g, :, cols(c)],
            rows.at[6 + k, core, g, :, cols(c)],
            row_x.at[0, k, g, c],
            row_x.at[1, k, g, c],
            x_peer,
        )

    def reduce_c(b, c):
        return remote(
            partial.at[b, other_core, :, :, cols(c)],
            red.at[b, :, :, cols(c)],
            red_sems.at[0, b, c],
            red_sems.at[1, b, c],
            c_peer,
        )

    def reduce_x(k, c):
        return remote(
            partial.at[6 + k, core, :, :, cols(c)],
            x_got.at[k, :, :, cols(c)],
            sum_x.at[0, k, c],
            sum_x.at[1, k, c],
            x_peer,
        )

    def give_y(b, c):
        return remote(
            partial.at[b, core, other_y, :, cols(c)],
            y_got.at[b, :, cols(c)],
            sum_y.at[0, b, c],
            sum_y.at[1, b, c],
            y_peer,
        )

    def pass_on(b, place, where, arrive, c, device):
        return remote(sent.at[b, :, cols(c)], where.at[place, :, cols(c)], t_out.at[b, c], arrive.at[place, c], device)

    mix_core = remote(a_part.at[:, other_core], a_red, mix_sems.at[0, 0], mix_sems.at[1, 0], c_peer)
    mix_side = remote(a_send, a_got, mix_sems.at[0, 1], mix_sems.at[1, 1], x_peer)

    def wait_for(message):
        kind = message[0]
        c = message[-1]
        k = message[1] if len(message) > 1 else 0
        if kind == "d":
            block(k, k, 0, c, x_peer).wait_recv()
        elif kind == "ry":
            remote(
                y_send.at[k, :, cols(c)],
                rows.at[k, core, other_y, :, cols(c)],
                row_y.at[0, k, c],
                row_y.at[1, k, c],
                y_peer,
            ).wait_recv()
        elif kind == "rc":
            g = groups[message[2]]
            there = rows.at[k, other_core, g, :, cols(c)]
            remote(there, there, row_c.at[0, k, g, c], row_c.at[1, k, g, c], c_peer).wait_recv()
        elif kind == "rx":
            row_to_x(k, groups[message[2]], c).wait_recv()
        elif kind == "red":
            reduce_c(k, c).wait_recv()
        elif kind == "xg":
            reduce_x(k, c).wait_recv()
        elif kind == "gy":
            give_y(k, c).wait_recv()
        elif kind == "zg":
            pass_on(1, k, z_got, z_in, c, z_peer).wait_recv()
        elif kind == "mg":
            pass_on(1, k, m_got, m_in, c, z_peer).wait_recv()
        elif kind == "pg":
            pass_on(1, k, p_got, p_in, c, z_peer).wait_recv()
        elif kind == "og":
            pass_on(1, 0, o_got, o_in, c, z_peer).wait_recv()
        elif kind == "kvz":
            kv_z(stops[k + 1] * 2 + y, 0, k, z_peer).wait_recv()
        elif kind == "kvy":
            owner = stops[k] * 2 + other_y
            remote(
                kv_all.at[:, owner], kv_all.at[:, owner], kvy_sems.at[0, k], kvy_sems.at[1, k], y_peer
            ).wait_recv()
        elif kind == "mc":
            mix_core.wait_recv()
        else:
            mix_side.wait_recv()

    row_id = lax.broadcasted_iota(jnp.int32, (tokens_here, tokens_here), 0)
    col_id = lax.broadcasted_iota(jnp.int32, (tokens_here, tokens_here), 1)
    before = (row_id < col_id).astype(jnp.bfloat16)
    after = (col_id < row_id).astype(jnp.bfloat16)

    def tiles(c, body):
        def run(j, carry):
            body(pl.ds(pl.multiple_of(c * part + j * 512, 512), 512))
            return carry

        lax.fori_loop(0, part // 512, run, 0)

    def build(b):
        named = meta[b]
        spread = []
        for expert in (e, y_expert):
            wanted = expert.astype(jnp.float32)
            hit = jnp.logical_or(named[0:1] == wanted, named[1:2] == wanted)
            spread.append(jnp.broadcast_to(hit.astype(jnp.float32)[:, :tokens_here], (cap, tokens_here)))
        spread = jnp.concatenate(spread, axis=0)
        rank = jnp.dot(spread.astype(jnp.bfloat16), before, preferred_element_type=jnp.float32)
        slot = f32(lax.rem(lax.broadcasted_iota(jnp.int32, rank.shape, 0), cap))
        chosen[b] = (jnp.where(rank == slot, 1.0, 0.0) * spread).astype(jnp.bfloat16)
        columns = jnp.transpose(named)[:tokens_here]
        for place, expert in enumerate((e, y_expert)):
            wanted = expert.astype(jnp.float32)
            hits = [(columns[:, k:k + 1] == wanted).astype(jnp.float32) for k in range(2)]
            scale = hits[0] * columns[:, 2:3] + hits[1] * columns[:, 3:4]
            spread = jnp.broadcast_to(hits[0] + hits[1], (tokens_here, cap))
            rank = jnp.dot(after, spread.astype(jnp.bfloat16), preferred_element_type=jnp.float32)
            slot = f32(lax.broadcasted_iota(jnp.int32, rank.shape, 1))
            picks[b, place] = (jnp.where(rank == slot, 1.0, 0.0) * spread).astype(jnp.bfloat16)
            scales[b, place] = jnp.broadcast_to(scale, (tokens_here, 128))

    def select(b, c):
        table = chosen[b]

        def body(span):
            found = jnp.dot(table, dense[b, :, span], preferred_element_type=jnp.float32).astype(jnp.bfloat16)
            rows[b, core, y, :, span] = found[:cap]
            y_send[b, :, span] = found[cap:]

        tiles(c, body)
        row_to_y(b, c).start()
        row_to_c(b, y, c).start()
        if b >= 4:
            row_to_x(b - 4, y, c).start()

    def finish(b, c):
        def body(span):
            value = f32(partial[b, core, :, :, span]) + f32(red[b, :, :, span])
            if b in (4, 5):
                value = value + f32(x_got[b - 4, :, :, span])
            partial[b, core, :, :, span] = value.astype(jnp.bfloat16)

        tiles(c, body)
        if b >= 6:
            reduce_x(b - 6, c).start()
        else:
            give_y(b, c).start()

    def gather(b, c):
        mine, theirs = picks[b, 0], picks[b, 1]
        scale_mine, scale_theirs = scales[b, 0, :, 0:1], scales[b, 1, :, 0:1]

        def body(span):
            first = jnp.dot(mine, partial[b, core, y, :, span], preferred_element_type=jnp.float32)
            second = jnp.dot(theirs, y_got[b, :, span], preferred_element_type=jnp.float32)
            hold[b, :, span] = first * scale_mine + second * scale_theirs

        tiles(c, body)

    def release(b, c, sources, place, where, arrive, device):
        def body(span):
            value = hold[b, :, span]
            for got, at in sources:
                value = value + f32(got[at, :, span])
            sent[b, :, span] = value.astype(jnp.bfloat16)

        tiles(c, body)
        pass_on(b, place, where, arrive, c, device).start()

    def messages(task, is_inner):
        kind = task[0]
        c = task[-1]
        b = task[1] if len(task) > 1 else 0
        whole = range(chunks)
        if kind in ("F3", "F6", "F5", "F7"):
            return [("d", {"F3": 1, "F6": 4, "F5": 2, "F7": 5}[kind], c)]
        if kind == "sel":
            return [("d", b, c)]
        if kind == "arr":
            return [("ry", b, c)]
        if kind == "arx":
            return [("rx", b, task[2], c)]
        if kind == "cmp":
            return [("rc", b, g, c) for g in range(2) for c in whole]
        if kind == "fin":
            return [("red", b, c)] + ([("xg", b - 4, c)] if b in (4, 5) else [])
        if kind == "gat":
            return [("gy", b, c)]
        if kind == "rel":
            if b == 1:
                return [("pg", 1, c)]
            if is_inner and b in (4, 5):
                return [("zg", b - 4, c)]
            return [("mg", 1, c)] if is_inner and b == 2 else []
        if kind == "final":
            return [("og", c), ("pg", 0, c)] + ([("mg", 0, c)] if is_inner else [])
        if kind == "kvf":
            return [("kvz", b)]
        if kind == "att":
            return [("kvy", j) for j in range(4)]
        return {"mixs": [("mc",)], "mixf": [("mx",)]}.get(kind, [])

    def perform(task, is_inner):
        kind = task[0]
        c = task[-1]
        b = task[1] if len(task) > 1 else 0
        if kind == "D2":
            to_near(c).start()
        elif kind == "F3":
            x_to_near(c).start()
        elif kind == "F6":
            far_to_near(0, c).start()
        elif kind == "F5":
            near_to_across(c).start()
        elif kind == "F7":
            far_to_near(1, c).start()
        elif kind == "meta":
            for slot in range(1, 6):
                card(slot, 0, x_peer).wait_recv()

            def run(slot, carry):
                build(slot)
                return carry

            lax.fori_loop(1, 6, run, 0)
        elif kind == "sel":
            select(b, c)
        elif kind == "arr":
            row_to_c(b, other_y, c).start()
            if b >= 4:
                row_to_x(b - 4, other_y, c).start()
        elif kind == "arx":
            row_to_c(6 + b, groups[task[2]], c).start()
        elif kind == "fin":
            finish(b, c)
        elif kind == "gat":
            gather(b, c)
        elif kind == "rel":
            if b == 1:
                release(b, c, [(p_got, 1)], 0, o_got, o_in, x_peer)
            elif b == 2:
                release(b, c, [(m_got, 1)] if is_inner else [], 0, p_got, p_in, z_peer)
            elif b == 3:
                release(b, c, [], 1, p_got, p_in, z_peer)
            elif is_inner:
                release(b, c, [(z_got, b - 4)], b - 4, m_got, m_in, m_peer)
            else:
                release(b, c, [], b - 4, z_got, z_in, z_peer)
        elif kind == "final":
            def body(span):
                value = hold[0, :, span] + f32(o_got[0, :, span]) + f32(p_got[0, :, span])
                if is_inner:
                    value = value + f32(m_got[0, :, span])
                moe[:, span] = value.astype(jnp.bfloat16)

            tiles(c, body)
        elif kind == "kvs":
            kv_sends[0].start()
            if is_inner:
                kv_sends[1].start()
            kv_y(0).start()
        elif kind == "kvf":
            if is_inner:
                kv_sends[2 + b].start()
            kv_y(b + 1).start()
        elif kind == "mixs":
            a_send[...] = (f32(a_part[other_side, core]) + f32(a_red[other_side])).astype(jnp.bfloat16)
            mix_side.start()
        elif kind == "mixf":
            mixed[...] = (f32(a_part[side, core]) + f32(a_red[side]) + f32(a_got[...])).astype(jnp.bfloat16)

    def plan(order, is_inner):
        seen = {("d", 0, c) for c in range(chunks)}
        pieces, kinds = [[]], []
        for task in order:
            fresh = [message for message in messages(task, is_inner) if message not in seen]
            seen.update(fresh)
            pieces[-1].append((fresh, task))
            if task[0] in BIG:
                kinds.append(BIG[task[0]] + (task[1] if len(task) > 1 else 0))
                pieces.append([])
        return pieces, kinds

    def emit(piece, is_inner):
        for fresh, task in piece:
            for message in fresh:
                wait_for(message)
            if task[0] not in BIG:
                perform(task, is_inner)

    as_float = f32(x_ref[...])
    mean = jnp.mean(as_float * as_float, axis=1, keepdims=True)
    dense[0] = (as_float * lax.rsqrt(mean + NORM_EPS) * x_gain[...]).astype(jnp.bfloat16)
    meta[0] = jnp.zeros(meta.shape[1:], jnp.float32)
    meta[0, 0:2, 0:tokens_here] = f32(routes_row[...])
    meta[0, 2:4, 0:tokens_here] = weight_row[...]

    pl.semaphore_wait(barrier, len(greeted))
    for item in cards:
        item.start()
    for c in range(chunks):
        to_x(c).start()

        @pl.when(inner)
        def _():
            to_across(c).start()

        if c == 0:
            to_near(c).start()
        else:
            @pl.when(outer)
            def _():
                to_near(c).start()

    build(0)
    for c in range(chunks):
        select(0, c)

    loads[0].wait()
    lane = lax.broadcasted_iota(jnp.int32, (tok, 128), 1)
    low = lane < HEAD_DIM
    even = lax.rem(lax.div(lane, HEAD_DIM // 4), 2) == 0
    table = turn[...]
    swapped = pltpu.roll(table, HEAD_DIM, 1)
    cosine = jnp.where(low, table, swapped)
    sine = jnp.where(low, swapped, table)

    def turned(raw, gain):
        flat = f32(raw)
        square = flat * flat
        left = jnp.sum(jnp.where(low, square, 0.0), axis=1, keepdims=True)
        right = jnp.sum(jnp.where(low, 0.0, square), axis=1, keepdims=True)
        mean_square = jnp.where(low, left, right) * (1.0 / HEAD_DIM)
        unit = flat * lax.rsqrt(mean_square + NORM_EPS) * gain
        partner = jnp.where(
            even, -pltpu.roll(unit, 128 - HEAD_DIM // 4, 1), pltpu.roll(unit, HEAD_DIM // 4, 1)
        )
        return unit * cosine + partner * sine

    for pair in range(kv_all.shape[0] // 2):
        span = slice(pair * 128, (pair + 1) * 128)
        k_rows = turned(k_raw[:, span], k_gain[:, span])
        v_rows = f32(v_raw[:, span])
        kv_all[2 * pair, e] = jnp.where(low, k_rows, pltpu.roll(v_rows, HEAD_DIM, 1)).astype(jnp.bfloat16)
        kv_all[2 * pair + 1, e] = jnp.where(low, pltpu.roll(k_rows, HEAD_DIM, 1), v_rows).astype(jnp.bfloat16)

    for pair in range(pairs):
        span = slice(pair * 128, (pair + 1) * 128)
        q_rows = turned(q_raw[:, span], q_gain[:, span])
        q_ref[2 * pair] = jnp.where(low, q_rows, 0.0).astype(jnp.bfloat16)
        q_ref[2 * pair + 1] = jnp.where(low, pltpu.roll(q_rows, HEAD_DIM, 1), 0.0).astype(jnp.bfloat16)

    for load in loads[1:]:
        load.wait()

    def attend(pair):
        kv = kv_all[lax.div(pair * 2 * kv_all.shape[0], pairs * 2)].reshape(n * tok, 128)
        halves = []
        for h in range(2):
            scores = lax.dot_general(
                q_ref[pair * 2 + h], kv, (((1,), (1,)), ((), ())), preferred_element_type=jnp.float32
            ) * (HEAD_DIM ** (-0.5))
            peak = jnp.max(scores, axis=1, keepdims=True)
            weights = jnp.exp(scores - peak)
            total = jnp.sum(weights, axis=1, keepdims=True)
            summed = jnp.dot(weights.astype(jnp.bfloat16), kv, preferred_element_type=jnp.float32)
            halves.append(summed / total)
        joined = jnp.where(low, pltpu.roll(halves[0], HEAD_DIM, 1), halves[1])
        attended[pair] = joined.astype(jnp.bfloat16)

    inner_pieces, inner_kinds = plan(INNER_ORDER, True)
    outer_pieces, outer_kinds = plan(OUTER_ORDER, False)
    count = len(inner_kinds)

    def step(s, carry):
        u = jnp.where(inner, inner_kinds[0], outer_kinds[0])
        for place in range(1, count):
            u = jnp.where(s == place, jnp.where(inner, inner_kinds[place], outer_kinds[place]), u)
        for place in range(count):
            @pl.when(jnp.logical_and(s == place, inner))
            def _():
                emit(inner_pieces[place], True)

            @pl.when(jnp.logical_and(s == place, outer))
            def _():
                emit(outer_pieces[place], False)

        @pl.when(u < 8)
        def _():
            tokens = rows[u].reshape(4 * cap, width)
            gate = jnp.dot(tokens, wg[...], preferred_element_type=jnp.float32)
            up = jnp.dot(tokens, wu[...], preferred_element_type=jnp.float32)
            hidden = (gate / (1.0 + jnp.exp(-gate)) * up).astype(jnp.bfloat16)
            for tile in range(0, width, TILE):
                product = jnp.dot(hidden, wd[:, tile:tile + TILE], preferred_element_type=jnp.float32)
                partial[u, :, :, :, tile:tile + TILE] = product.astype(jnp.bfloat16).reshape(2, 2, cap, TILE)
                if (tile + TILE) % part == 0:
                    reduce_c(u, tile // part).start()

        @pl.when(jnp.logical_and(u >= 8, u < 10))
        def _():
            attend(2 * (u - 8))
            attend(2 * (u - 8) + 1)

        @pl.when(u == 10)
        def _():
            for tile in range(0, width, TILE):
                product = jnp.dot(attended[0], ow[0, :, tile:tile + TILE], preferred_element_type=jnp.float32)
                for p in range(1, pairs):
                    product += jnp.dot(attended[p], ow[p, :, tile:tile + TILE], preferred_element_type=jnp.float32)
                a_part[:, :, :, tile:tile + TILE] = product.astype(jnp.bfloat16).reshape(2, 2, tok // 4, TILE)
            mix_core.start()

        return carry

    lax.fori_loop(0, count, step, 0)

    @pl.when(inner)
    def _():
        emit(inner_pieces[count], True)

    @pl.when(outer)
    def _():
        emit(outer_pieces[count], False)

    mix_core.wait_send()
    mix_side.wait_send()
    for j in range(4):
        kv_y(j).wait_send()
    kv_sends[0].wait_send()
    for item in cards:
        item.wait_send()

    @pl.when(inner)
    def _():
        for item in kv_sends[1:]:
            item.wait_send()

    for c in range(chunks):
        to_x(c).wait_send()
        to_near(c).wait_send()
        x_to_near(c).wait_send()

        @pl.when(inner)
        def _():
            to_across(c).wait_send()
            near_to_across(c).wait_send()
            far_to_near(0, c).wait_send()
            far_to_near(1, c).wait_send()

        for b in range(1, 6):
            pass_on(b, 0, o_got, o_in, c, x_peer).wait_send()
        for k in range(2):
            for g in range(2):
                row_to_x(k, g, c).wait_send()
            reduce_x(k, c).wait_send()
        for b in range(6):
            row_to_y(b, c).wait_send()
            give_y(b, c).wait_send()
        for b in range(8):
            for g in range(2):
                row_to_c(b, g, c).wait_send()
            reduce_c(b, c).wait_send()


def turn_table(tokens):
    quarter = HEAD_DIM // 4
    inverse = np.power(ROPE_BASE, -np.arange(quarter, dtype=np.float64) / quarter)
    places = np.arange(tokens)
    row = (places // GRID_W)[:, None] * inverse
    col = (places % GRID_W)[:, None] * inverse
    angles = np.concatenate([row, row, col, col], axis=1)
    return np.concatenate([np.cos(angles), np.sin(angles)], axis=1).astype(np.float32)


def fused(x, x_gain, routes, route_weight, queries, keys, values, q_gain, k_gain, gate_weight, up_weight, down_weight, out_weight):
    n = lax.axis_size("ep")
    tok_exp, width = x.shape
    cap = 2 * routes.shape[1] * tok_exp // n
    tok = queries.shape[0]
    heads = queries.shape[1] // HEAD_DIM
    kv_count = keys.shape[1] // HEAD_DIM
    pairs = heads // 2
    hidden = gate_weight.shape[1]
    bf = jnp.bfloat16
    vmem = pl.BlockSpec(memory_space=pltpu.VMEM)
    anywhere = pl.BlockSpec(memory_space=pl.ANY)
    dma = pltpu.SemaphoreType.DMA
    return pl.pallas_call(
        functools.partial(fused_kernel, n),
        out_shape=(
            jax.ShapeDtypeStruct((tok_exp, width), bf),
            jax.ShapeDtypeStruct((tok // 4, width), bf),
        ),
        in_specs=[vmem] * 9 + [anywhere] * 5,
        out_specs=(vmem, vmem),
        scratch_shapes=[
            pltpu.VMEM((6, tok_exp, width), bf),
            pltpu.VMEM((6, 8, 128), jnp.float32),
            pltpu.VMEM((6, 2 * cap, tok_exp), bf),
            pltpu.VMEM((6, 2, tok_exp, cap), bf),
            pltpu.VMEM((6, 2, tok_exp, 128), jnp.float32),
            pltpu.VMEM((8, 2, 2, cap, width), bf),
            pltpu.VMEM((6, cap, width), bf),
            pltpu.VMEM((8, 2, 2, cap, width), bf),
            pltpu.VMEM((8, 2, cap, width), bf),
            pltpu.VMEM((2, 2, cap, width), bf),
            pltpu.VMEM((6, cap, width), bf),
            pltpu.VMEM((6, tok_exp, width), jnp.float32),
            pltpu.VMEM((6, tok_exp, width), bf),
            pltpu.VMEM((2, tok_exp, width), bf),
            pltpu.VMEM((2, tok_exp, width), bf),
            pltpu.VMEM((2, tok_exp, width), bf),
            pltpu.VMEM((1, tok_exp, width), bf),
            pltpu.VMEM((heads, tok, 128), bf),
            pltpu.VMEM((tok, 128), jnp.float32),
            pltpu.VMEM((width, hidden), bf),
            pltpu.VMEM((width, hidden), bf),
            pltpu.VMEM((hidden, width), bf),
            pltpu.VMEM((pairs, 128, width), bf),
            pltpu.VMEM((kv_count, n, tok, 128), bf),
            pltpu.VMEM((pairs, tok, 128), bf),
            pltpu.VMEM((2, 2, tok // 4, width), bf),
            pltpu.VMEM((2, tok // 4, width), bf),
            pltpu.VMEM((tok // 4, width), bf),
            pltpu.VMEM((tok // 4, width), bf),
            dma((5,)),
            dma((5,)),
            dma((3,)),
            dma((2, 4)),
            dma((8, CHUNKS)),
            dma((6, CHUNKS)),
            dma((2, 6)),
            dma((2, 6, CHUNKS)),
            dma((2, 8, 2, CHUNKS)),
            dma((2, 2, 2, CHUNKS)),
            dma((2, 8, CHUNKS)),
            dma((2, 2, CHUNKS)),
            dma((2, 6, CHUNKS)),
            dma((6, CHUNKS)),
            dma((2, CHUNKS)),
            dma((2, CHUNKS)),
            dma((2, CHUNKS)),
            dma((1, CHUNKS)),
            dma((2, 2)),
        ],
        compiler_params=pltpu.CompilerParams(
            collective_id=0, has_side_effects=True, vmem_limit_bytes=62 * 1024 * 1024
        ),
    )(
        x,
        x_gain.reshape(1, width),
        jnp.transpose(routes),
        jnp.transpose(route_weight),
        queries,
        keys,
        values,
        q_gain.reshape(1, -1),
        k_gain.reshape(1, -1),
        jnp.asarray(turn_table(n * tok)),
        gate_weight,
        up_weight,
        down_weight,
        out_weight.reshape(pairs, 128, width),
    )


def plain_shards(
    queries,
    keys,
    values,
    query_gain,
    key_gain,
    out_weight,
    expert_input,
    norm_gain,
    routes,
    route_weight,
    gate_weight,
    up_weight,
    down_weight,
):
    tok_mix = queries.shape[0]
    head_count = query_gain.shape[0] // HEAD_DIM
    kv_count = key_gain.shape[0] // HEAD_DIM
    group_size = head_count // kv_count
    offset = lax.axis_index("ep") * tok_mix
    q_turned = head_norm(queries, query_gain, head_count, offset)
    k_turned = head_norm(keys, key_gain, kv_count, offset)
    grouped = q_turned.reshape(tok_mix, kv_count, group_size, HEAD_DIM)
    score_scale = HEAD_DIM ** (-0.5)
    start_state = (
        jnp.full((kv_count, group_size, tok_mix), -jnp.inf, jnp.float32),
        jnp.zeros((kv_count, group_size, tok_mix), jnp.float32),
        jnp.zeros((tok_mix, kv_count, group_size, HEAD_DIM), jnp.float32),
    )
    running = start_state
    key_piece = lax.all_gather(k_turned, "ep", axis=0, tiled=True)
    value_piece = lax.all_gather(values, "ep", axis=0, tiled=True)
    length = key_piece.shape[0]
    block_len = length
    while block_len > 2048 and block_len % 2 == 0:
        block_len = block_len // 2
    key_blocks = key_piece.reshape(length // block_len, block_len, key_piece.shape[1])
    value_blocks = value_piece.reshape(length // block_len, block_len, value_piece.shape[1])

    def advance(inner_state, key_value):
        return (absorb(inner_state, key_value[0], key_value[1], grouped, score_scale), None)

    running, unused = lax.scan(advance, running, (key_blocks, value_blocks))
    final_max, weight_sum, summed = running
    attended = (
        (summed / jnp.transpose(weight_sum, (2, 0, 1))[..., None])
        .reshape(tok_mix, -1)
        .astype(jnp.bfloat16)
    )
    mixed = lax.psum_scatter(
        jnp.dot(attended, out_weight, preferred_element_type=jnp.float32).astype(jnp.bfloat16),
        "tp",
        scatter_dimension=0,
        tiled=True,
    )
    tok_exp = expert_input.shape[0]
    top_count = routes.shape[1]
    expert_count = lax.axis_size("ep")
    capacity = 2 * top_count * tok_exp // expert_count
    as_float = expert_input.astype(jnp.float32)
    normed = (
        as_float
        * lax.rsqrt(jnp.mean(as_float * as_float, axis=-1, keepdims=True) + NORM_EPS)
        * norm_gain
    ).astype(jnp.bfloat16)
    flat_routes = routes.reshape(-1)
    route_hits = (
        flat_routes[:, None] == jnp.arange(expert_count, dtype=jnp.int32)[None, :]
    ).astype(jnp.int32)
    slot_rank = jnp.sum((jnp.cumsum(route_hits, axis=0) - route_hits) * route_hits, axis=1)
    slot_ids = flat_routes * capacity + slot_rank
    placed = jnp.arange(expert_count * capacity, dtype=jnp.int32)[:, None] == slot_ids[None, :]
    placed = jnp.any(placed.reshape(expert_count * capacity, tok_exp, top_count), axis=2).astype(
        jnp.bfloat16
    )
    outbound = jnp.dot(placed, normed, preferred_element_type=jnp.float32).astype(jnp.bfloat16)
    model_width = outbound.shape[1]
    half_cap = capacity // 2
    laid = outbound.reshape(expert_count, capacity, model_width)
    first_half = run_experts(
        laid[:, :half_cap].reshape(expert_count * half_cap, model_width),
        gate_weight,
        up_weight,
        down_weight,
    )
    second_half = run_experts(
        laid[:, half_cap:].reshape(expert_count * half_cap, model_width),
        gate_weight,
        up_weight,
        down_weight,
    )
    back_rows = jnp.concatenate(
        [
            first_half.reshape(expert_count, half_cap, model_width),
            second_half.reshape(expert_count, half_cap, model_width),
        ],
        axis=1,
    )
    back_rows = back_rows.reshape(expert_count * capacity, model_width)
    picked = back_rows[slot_ids.reshape(tok_exp, top_count)]
    moe_out = jnp.sum(picked.astype(jnp.float32) * route_weight[:, :, None], axis=1).astype(
        jnp.bfloat16
    )
    return (mixed, moe_out)


def shards(
    queries,
    keys,
    values,
    query_gain,
    key_gain,
    out_weight,
    expert_input,
    norm_gain,
    routes,
    route_weight,
    gate_weight,
    up_weight,
    down_weight,
):
    tok_exp = expert_input.shape[0]
    top_count = routes.shape[1]
    expert_count = lax.axis_size("ep")
    capacity = 2 * top_count * tok_exp // expert_count
    if capacity % 16 != 0 or lax.axis_size("tp") != 4 or expert_count != 8:
        return plain_shards(
            queries,
            keys,
            values,
            query_gain,
            key_gain,
            out_weight,
            expert_input,
            norm_gain,
            routes,
            route_weight,
            gate_weight,
            up_weight,
            down_weight,
        )
    moe_out, mixed = fused(
        expert_input,
        norm_gain,
        routes,
        route_weight,
        queries,
        keys,
        values,
        query_gain,
        key_gain,
        gate_weight[0],
        up_weight[0],
        down_weight[0],
        out_weight,
    )
    return (mixed, moe_out)


def solution(mesh):
    placed = (
        P("ep", "tp"),
        P("ep", "tp"),
        P("ep", "tp"),
        P("tp"),
        P("tp"),
        P("tp", None),
        P(("ep", "tp"), None),
        P(),
        P(("ep", "tp"), None),
        P(("ep", "tp"), None),
        P("ep", None, "tp"),
        P("ep", None, "tp"),
        P("ep", "tp", None),
    )
    return jax.shard_map(
        shards,
        mesh=mesh,
        in_specs=placed,
        out_specs=(P(("ep", "tp"), None), P(("ep", "tp"), None)),
        check_vma=False,
    )
```

```python
import functools

import jax
import jax.numpy as jnp
import numpy as np
from jax import lax
from jax.experimental import pallas as pl
from jax.experimental.pallas import tpu as pltpu
from jax.sharding import PartitionSpec as P

HEAD_DIM = 64
GRID_W = 128


NORM_EPS = 1e-06
ROPE_BASE = 10000.0


def rotate(vectors, grid_rows, grid_cols):
    quarter = vectors.shape[-1] // 4
    inverse = ROPE_BASE ** (-jnp.arange(quarter, dtype=jnp.float32) / quarter)
    angle_row = grid_rows[:, None] * inverse
    angle_col = grid_cols[:, None] * inverse
    angles = jnp.concatenate([angle_row, angle_row, angle_col, angle_col], axis=-1)[:, None, :]
    part_one, part_two, part_three, part_four = jnp.split(vectors, 4, axis=-1)
    turned = jnp.concatenate([-part_two, part_one, -part_four, part_three], axis=-1)
    return vectors * jnp.cos(angles) + turned * jnp.sin(angles)


def head_norm(raw_rows, gains, head_count, offset):
    row_count = raw_rows.shape[0]
    flat_rows = raw_rows.astype(jnp.float32).reshape(row_count, head_count, -1)
    unit_vec = flat_rows * lax.rsqrt(
        jnp.mean(flat_rows * flat_rows, axis=-1, keepdims=True) + NORM_EPS
    )
    unit_vec = unit_vec * gains.reshape(head_count, -1)
    places = offset + jnp.arange(row_count, dtype=jnp.int32)
    grid_rows = (places // GRID_W).astype(jnp.float32)
    grid_cols = (places % GRID_W).astype(jnp.float32)
    return rotate(unit_vec, grid_rows, grid_cols).astype(jnp.bfloat16).reshape(row_count, -1)


def absorb(running, key_block, value_block, grouped, score_scale):
    run_max, weight_sum, summed = running
    kv_count = grouped.shape[1]
    key_heads = key_block.reshape(key_block.shape[0], kv_count, -1)
    value_heads = value_block.reshape(value_block.shape[0], kv_count, -1)
    scores = (
        jnp.einsum("qhgd,khd->hgqk", grouped, key_heads, preferred_element_type=jnp.float32)
        * score_scale
    )
    new_max = jnp.maximum(run_max, jnp.max(scores, axis=-1))
    rescale = jnp.exp(run_max - new_max)
    weights = jnp.exp(scores - new_max[..., None])
    weight_sum = weight_sum * rescale + jnp.sum(weights, axis=-1)
    update = jnp.einsum(
        "hgqk,khd->qhgd",
        weights.astype(jnp.bfloat16),
        value_heads,
        preferred_element_type=jnp.float32,
    )
    summed = summed * jnp.transpose(rescale, (2, 0, 1))[..., None] + update
    return (new_max, weight_sum, summed)


def run_experts(sending, gate_weight, up_weight, down_weight):
    arrived = lax.all_to_all(sending, "ep", split_axis=0, concat_axis=0, tiled=True)
    shard_rows = lax.all_gather(arrived, "tp", axis=0, tiled=True)
    gate_out = jnp.dot(shard_rows, gate_weight[0], preferred_element_type=jnp.float32)
    up_out = jnp.dot(shard_rows, up_weight[0], preferred_element_type=jnp.float32)
    hidden = (jax.nn.silu(gate_out) * up_out).astype(jnp.bfloat16)
    results = lax.psum_scatter(
        jnp.dot(hidden, down_weight[0], preferred_element_type=jnp.float32).astype(jnp.bfloat16),
        "tp",
        scatter_dimension=0,
        tiled=True,
    )
    return lax.all_to_all(results, "ep", split_axis=0, concat_axis=0, tiled=True)


MESH = pl.DeviceIdType.MESH
TILE = 1024
CHUNKS = 4


def flip(index, pattern, size):
    result = 0
    bit = 1
    while bit < size:
        both = lax.rem(lax.div(index, bit) + lax.div(pattern, bit), 2)
        result = result + both * bit
        bit = bit * 2
    return result


def f32(value):
    return value.astype(jnp.float32)


INNER_ORDER = (
    ("arr", 0, 0), ("F6", 0), ("meta",), ("sel", 4, 0), ("sel", 1, 0), ("F6", 1), ("F5", 0), ("sel", 1, 1),
    ("arr", 0, 3), ("F6", 2), ("sel", 4, 2), ("sel", 4, 1), ("F5", 1), ("F6", 3), ("sel", 1, 2), ("F3", 1),
    ("sel", 5, 0), ("F3", 0), ("arr", 4, 0), ("F3", 3), ("arr", 4, 2), ("F5", 3), ("sel", 4, 3),
    ("sel", 5, 1), ("sel", 2, 3), ("sel", 5, 3), ("sel", 1, 3), ("F3", 2), ("arx", 0, 1, 0), ("F5", 2),
    ("F7", 1), ("arr", 5, 3), ("sel", 3, 1), ("sel", 2, 0), ("arr", 4, 3), ("F7", 2), ("F7", 3),
    ("arx", 0, 0, 0), ("arr", 4, 1), ("sel", 3, 0), ("kvf", 0), ("cmp", 4), ("sel", 5, 2), ("sel", 3, 2),
    ("arx", 1, 0, 0), ("arr", 5, 0), ("arr", 1, 3), ("arr", 1, 2), ("arx", 0, 1, 2), ("arr", 3, 0),
    ("sel", 2, 1), ("arr", 2, 3), ("sel", 3, 3), ("F7", 0), ("arx", 0, 0, 2), ("arx", 0, 0, 1),
    ("arx", 1, 1, 3), ("kvs",), ("arx", 0, 1, 3), ("arr", 0, 1), ("arx", 0, 1, 1), ("kvf", 2), ("arr", 1, 0),
    ("arr", 0, 2), ("arr", 1, 1), ("arx", 0, 0, 3), ("arx", 1, 0, 1), ("arr", 5, 1), ("cmp", 6),
    ("arr", 5, 2), ("arr", 2, 0), ("cmp", 1), ("fin", 6, 1), ("arr", 3, 3), ("arr", 3, 2), ("fin", 6, 0),
    ("arx", 1, 0, 3), ("arr", 3, 1), ("arx", 1, 1, 0), ("arx", 1, 1, 1), ("arx", 1, 1, 2), ("cmp", 3),
    ("arx", 1, 0, 2), ("fin", 6, 3), ("kvf", 1), ("fin", 6, 2), ("cmp", 0), ("fin", 3, 0), ("sel", 2, 2),
    ("fin", 3, 2), ("fin", 4, 0), ("fin", 1, 3), ("D2", 2), ("cmp", 7), ("D2", 1), ("att", 0), ("D2", 3),
    ("fin", 7, 1), ("arr", 2, 1), ("fin", 4, 1), ("fin", 3, 1), ("arr", 2, 2), ("cmp", 5), ("fin", 7, 0),
    ("gat", 3, 2), ("rel", 3, 2), ("gat", 4, 0), ("gat", 3, 0), ("fin", 1, 0), ("fin", 4, 2), ("fin", 3, 3),
    ("cmp", 2), ("rel", 3, 0), ("fin", 5, 1), ("fin", 7, 3), ("gat", 3, 1), ("fin", 2, 2), ("fin", 7, 2),
    ("att", 1), ("fin", 2, 1), ("rel", 3, 1), ("rel", 4, 0), ("mixp",), ("fin", 5, 2), ("fin", 4, 3),
    ("gat", 1, 3), ("gat", 3, 3), ("gat", 4, 2), ("mixs",), ("rel", 4, 2), ("gat", 1, 0), ("fin", 1, 2),
    ("gat", 5, 2), ("fin", 5, 0), ("fin", 5, 3), ("rel", 5, 2), ("fin", 1, 1), ("gat", 5, 1), ("fin", 2, 0),
    ("fin", 0, 3), ("rel", 3, 3), ("rel", 5, 1), ("fin", 2, 3), ("gat", 4, 1), ("gat", 5, 3), ("fin", 0, 0),
    ("gat", 2, 1), ("gat", 4, 3), ("gat", 2, 2), ("rel", 1, 0), ("rel", 2, 2), ("rel", 5, 3), ("gat", 1, 2),
    ("fin", 0, 2), ("gat", 2, 0), ("gat", 1, 1), ("gat", 5, 0), ("rel", 2, 1), ("rel", 1, 1), ("rel", 1, 2),
    ("mixf",), ("rel", 1, 3), ("rel", 5, 0), ("rel", 4, 1), ("fin", 0, 1), ("gat", 2, 3), ("rel", 2, 3),
    ("gat", 0, 1), ("rel", 2, 0), ("rel", 4, 3), ("gat", 0, 3), ("gat", 0, 0), ("gat", 0, 2), ("final", 0),
    ("final", 3), ("final", 2), ("final", 1),
)
OUTER_ORDER = (
    ("meta",), ("arr", 0, 1), ("kvs",), ("arr", 0, 0), ("sel", 2, 0), ("sel", 1, 1), ("arr", 0, 3), ("F3", 1),
    ("sel", 4, 0), ("sel", 4, 1), ("arr", 0, 2), ("sel", 1, 0), ("sel", 1, 2), ("arr", 4, 0), ("sel", 4, 2),
    ("arr", 4, 1), ("F3", 0), ("cmp", 0), ("F3", 3), ("sel", 4, 3), ("arx", 0, 0, 1), ("fin", 0, 0),
    ("fin", 0, 1), ("F3", 2), ("arr", 4, 2), ("arx", 0, 1, 1), ("arx", 0, 0, 2), ("arr", 4, 3), ("fin", 0, 2),
    ("arr", 1, 2), ("arx", 0, 0, 0), ("arx", 0, 0, 3), ("arx", 0, 1, 0), ("sel", 1, 3), ("arx", 0, 1, 2),
    ("arx", 0, 1, 3), ("sel", 3, 1), ("cmp", 6), ("sel", 3, 0), ("sel", 3, 3), ("fin", 6, 0), ("cmp", 4),
    ("fin", 6, 2), ("sel", 3, 2), ("arr", 3, 1), ("sel", 5, 1), ("arr", 3, 3), ("arr", 3, 0), ("fin", 4, 0),
    ("arr", 3, 2), ("sel", 5, 2), ("cmp", 3), ("fin", 4, 2), ("arr", 5, 1), ("sel", 5, 3), ("arx", 1, 0, 1),
    ("gat", 4, 0), ("rel", 4, 0), ("fin", 3, 2), ("arr", 1, 1), ("arr", 5, 2), ("sel", 5, 0), ("fin", 3, 1),
    ("gat", 0, 0), ("arx", 1, 1, 1), ("fin", 3, 0), ("arr", 5, 3), ("gat", 4, 2), ("gat", 3, 2),
    ("fin", 3, 3), ("arx", 1, 0, 2), ("rel", 4, 2), ("arr", 5, 0), ("kvf", 2), ("arx", 1, 0, 0),
    ("gat", 3, 1), ("arx", 1, 1, 2), ("arx", 1, 0, 3), ("rel", 3, 1), ("fin", 6, 1), ("fin", 6, 3),
    ("arx", 1, 1, 3), ("arr", 1, 0), ("arr", 1, 3), ("gat", 3, 0), ("kvf", 1), ("kvf", 0), ("rel", 3, 0),
    ("arx", 1, 1, 0), ("gat", 3, 3), ("rel", 3, 3), ("cmp", 7), ("cmp", 1), ("fin", 4, 1), ("fin", 7, 2),
    ("fin", 7, 1), ("cmp", 5), ("fin", 7, 3), ("sel", 2, 1), ("fin", 7, 0), ("rel", 3, 2), ("fin", 4, 3),
    ("fin", 1, 0), ("att", 0), ("gat", 4, 1), ("rel", 4, 1), ("fin", 5, 2), ("sel", 2, 2), ("arr", 2, 0),
    ("gat", 4, 3), ("rel", 4, 3), ("arr", 2, 1), ("fin", 5, 1), ("sel", 2, 3), ("att", 1), ("gat", 5, 2),
    ("gat", 1, 0), ("rel", 1, 0), ("rel", 5, 2), ("fin", 5, 3), ("mixp",), ("arr", 2, 2), ("gat", 5, 1),
    ("fin", 1, 1), ("arr", 2, 3), ("rel", 5, 1), ("gat", 5, 3), ("fin", 5, 0), ("mixs",), ("fin", 1, 2),
    ("rel", 5, 3), ("cmp", 2), ("fin", 2, 0), ("gat", 5, 0), ("fin", 2, 2), ("fin", 1, 3), ("fin", 0, 3),
    ("rel", 5, 0), ("gat", 0, 2), ("fin", 2, 3), ("fin", 2, 1), ("gat", 0, 1), ("gat", 2, 0), ("rel", 2, 0),
    ("gat", 2, 2), ("gat", 1, 2), ("gat", 1, 1), ("rel", 1, 1), ("rel", 2, 2), ("mixf",), ("rel", 1, 2),
    ("gat", 2, 3), ("rel", 2, 3), ("gat", 2, 1), ("gat", 1, 3), ("rel", 2, 1), ("rel", 1, 3), ("gat", 0, 3),
    ("final", 2), ("final", 0), ("final", 3), ("final", 1),
)


BIG = {"cmp": 0, "att": 8, "mixp": 10}


def fused_kernel(
    n,
    x_hbm,
    x_gain_hbm,
    routes_hbm,
    weight_hbm,
    q_hbm,
    k_hbm,
    v_hbm,
    q_gain_hbm,
    k_gain_hbm,
    turn_hbm,
    wg_hbm,
    wu_hbm,
    wd_hbm,
    ow_hbm,
    moe,
    mixed,
    x_ref,
    x_gain,
    routes_row,
    weight_row,
    q_raw,
    k_raw,
    v_raw,
    q_gain,
    k_gain,
    dense,
    meta,
    chosen,
    picks,
    scales,
    rows,
    y_send,
    partial,
    red,
    x_got,
    y_got,
    hold,
    sent,
    z_got,
    m_got,
    p_got,
    o_got,
    q_ref,
    turn,
    wg,
    wu,
    wd,
    ow,
    kv_all,
    attended,
    a_part,
    a_red,
    a_send,
    a_got,
    load_sem,
    kvz_out,
    kvz_in,
    kvy_sems,
    dn_out,
    dn_in,
    meta_sems,
    row_y,
    row_c,
    row_x,
    red_in,
    sum_x,
    sum_y,
    outs,
    z_in,
    m_in,
    p_in,
    o_in,
    mix_sems,
):
    e = lax.axis_index("ep")
    t = lax.axis_index("tp")
    side = lax.div(t, 2)
    core = lax.rem(t, 2)
    other_side = 1 - side
    other_core = 1 - core
    layer = lax.div(e, 2)
    y = lax.rem(e, 2)
    other_y = 1 - y
    near = layer + 1 - 2 * lax.rem(layer, 2)
    last = n // 2 - 1
    across = last - layer
    inner = jnp.logical_and(layer > 0, layer < last)
    outer = jnp.logical_not(inner)
    half = lax.div(layer, 2)
    far_inner = 2 - half
    far_outer = last * (1 - half)
    x_tp = other_side * 2 + core
    x_peer = (e, x_tp)
    c_peer = (e, side * 2 + other_core)
    y_expert = layer * 2 + other_y
    y_peer = (y_expert, t)
    z_peer = (near * 2 + y, t)
    m_peer = (across * 2 + y, t)
    corner = (near * 2 + y, x_tp)
    cap, width = rows.shape[3], rows.shape[4]
    pairs = attended.shape[0]
    tok = attended.shape[1]
    tokens_here = x_ref.shape[0]
    chunks = dn_in.shape[1]
    part = width // chunks
    groups = (y, other_y)

    def remote(src, dst, send, recv, device):
        return pltpu.make_async_remote_copy(
            src_ref=src, dst_ref=dst, send_sem=send, recv_sem=recv, device_id=device, device_id_type=MESH
        )

    def cols(c):
        return pl.ds(c * part, part)

    far_peers = [(far_inner * 2 + y, t), (far_outer * 2 + y, t)]
    barrier = pltpu.get_barrier_semaphore()
    greeted = [x_peer, c_peer, y_peer, z_peer, corner] + far_peers
    for peer in greeted:
        pl.semaphore_signal(barrier, inc=1, device_id=peer, device_id_type=MESH)

    loads = [
        pltpu.make_async_copy(a, b, load_sem.at[k])
        for k, (a, b) in enumerate(
            [
                (x_hbm, x_ref),
                (x_gain_hbm, x_gain),
                (routes_hbm, routes_row),
                (weight_hbm, weight_row),
                (turn_hbm.at[pl.ds(pl.multiple_of(e * tok, 8), tok)], turn),
                (k_hbm, k_raw),
                (v_hbm, v_raw),
                (k_gain_hbm, k_gain),
                (q_hbm, q_raw),
                (q_gain_hbm, q_gain),
                (wg_hbm, wg),
                (wu_hbm, wu),
                (wd_hbm, wd),
                (ow_hbm, ow),
            ]
        )
    ]
    for load in loads:
        load.start()

    def kv_z(owner, out, place, device):
        return remote(kv_all.at[:, owner], kv_all.at[:, owner], kvz_out.at[min(out, 1)], kvz_in.at[place], device)

    stops = [layer, near, far_inner, far_outer]

    def kv_y(j):
        owner = stops[j] * 2 + y
        return remote(kv_all.at[:, owner], kv_all.at[:, owner], kvy_sems.at[0], kvy_sems.at[1], y_peer)

    kv_sends = [
        kv_z(e, 0, 0, z_peer),
        kv_z(e, 1, 1, m_peer),
        kv_z(near * 2 + y, 2, 2, m_peer),
        kv_z(far_inner * 2 + y, 3, 1, z_peer),
        kv_z(far_outer * 2 + y, 4, 2, z_peer),
    ]

    def block(source, target, number, c, device):
        return remote(
            dense.at[source, :, cols(c)],
            dense.at[target, :, cols(c)],
            dn_out.at[number // 4],
            dn_in.at[target - 1, c],
            device,
        )

    def to_x(c):
        return block(0, 1, 1, c, x_peer)

    def to_near(c):
        return block(0, 2, 2, c, z_peer)

    def x_to_near(c):
        return block(1, 3, 3, c, z_peer)

    def to_across(c):
        return block(0, 4, 4, c, m_peer)

    def near_to_across(c):
        return block(2, 5, 5, c, m_peer)

    def far_to_near(k, c):
        return block(4 + k, 4 + k, 6 + k, c, z_peer)

    far_slot = jnp.where(inner, 4, 5)

    def card(slot, number, device):
        return remote(meta.at[0], meta.at[slot], meta_sems.at[0], meta_sems.at[1], device)

    cards = [
        card(1, 1, x_peer),
        card(2, 2, z_peer),
        card(3, 3, corner),
        card(far_slot, 4, far_peers[0]),
        card(far_slot, 5, far_peers[1]),
    ]

    def row_to_y(b, c):
        return remote(
            y_send.at[b, :, cols(c)], rows.at[b, core, y, :, cols(c)], outs.at[0], row_y.at[b, c], y_peer
        )

    def row_to_c(b, g, c):
        here = rows.at[b, core, g, :, cols(c)]
        return remote(here, here, outs.at[1], row_c.at[b], c_peer)

    def row_to_x(k, g, c):
        return remote(
            rows.at[4 + k, core, g, :, cols(c)],
            rows.at[6 + k, core, g, :, cols(c)],
            outs.at[2],
            row_x.at[k, g, c],
            x_peer,
        )

    def reduce_c(b, c):
        return remote(
            partial.at[b, other_core, :, :, cols(c)],
            red.at[b, :, :, cols(c)],
            outs.at[3],
            red_in.at[b],
            c_peer,
        )

    def reduce_x(k, c):
        return remote(
            partial.at[6 + k, core, :, :, cols(c)],
            x_got.at[k, :, :, cols(c)],
            outs.at[4],
            sum_x.at[k, c],
            x_peer,
        )

    def give_y(b, c):
        return remote(
            partial.at[b, core, other_y, :, cols(c)],
            y_got.at[b, :, cols(c)],
            outs.at[5],
            sum_y.at[b, c],
            y_peer,
        )

    def pass_on(b, place, where, arrive, c, device):
        return remote(sent.at[b, :, cols(c)], where.at[place, :, cols(c)], outs.at[6], arrive.at[place, c], device)

    mix_core = remote(a_part.at[:, other_core], a_red, mix_sems.at[0, 0], mix_sems.at[1, 0], c_peer)
    mix_side = remote(a_send, a_got, mix_sems.at[0, 1], mix_sems.at[1, 1], x_peer)

    def wait_for(message):
        kind = message[0]
        c = message[-1]
        k = message[1] if len(message) > 1 else 0
        if kind == "d":
            block(k, k, 0, c, x_peer).wait_recv()
        elif kind == "ry":
            remote(
                y_send.at[k, :, cols(c)],
                rows.at[k, core, other_y, :, cols(c)],
                outs.at[0],
                row_y.at[k, c],
                y_peer,
            ).wait_recv()
        elif kind == "rc":
            there = rows.at[k, other_core]
            remote(there, there, outs.at[1], row_c.at[k], c_peer).wait_recv()
        elif kind == "rx":
            row_to_x(k, groups[message[2]], c).wait_recv()
        elif kind == "red":
            remote(red.at[k], red.at[k], outs.at[3], red_in.at[k], c_peer).wait_recv()
        elif kind == "xg":
            reduce_x(k, c).wait_recv()
        elif kind == "gy":
            give_y(k, c).wait_recv()
        elif kind == "zg":
            pass_on(1, k, z_got, z_in, c, z_peer).wait_recv()
        elif kind == "mg":
            pass_on(1, k, m_got, m_in, c, z_peer).wait_recv()
        elif kind == "pg":
            pass_on(1, k, p_got, p_in, c, z_peer).wait_recv()
        elif kind == "og":
            pass_on(1, 0, o_got, o_in, c, z_peer).wait_recv()
        elif kind == "kvz":
            kv_z(stops[k + 1] * 2 + y, 0, k, z_peer).wait_recv()
        elif kind == "kvy":
            four = kv_all.at[:, 0:4]
            remote(four, four, kvy_sems.at[0], kvy_sems.at[1], y_peer).wait_recv()
        elif kind == "mc":
            mix_core.wait_recv()
        else:
            mix_side.wait_recv()

    row_id = lax.broadcasted_iota(jnp.int32, (tokens_here, tokens_here), 0)
    col_id = lax.broadcasted_iota(jnp.int32, (tokens_here, tokens_here), 1)
    before = (row_id < col_id).astype(jnp.bfloat16)
    after = (col_id < row_id).astype(jnp.bfloat16)

    def tiles(c, body):
        def run(j, carry):
            body(pl.ds(pl.multiple_of(c * part + j * 512, 512), 512))
            return carry

        lax.fori_loop(0, part // 512, run, 0)

    def build(b):
        named = meta[b]
        spread = []
        for expert in (e, y_expert):
            wanted = expert.astype(jnp.float32)
            hit = jnp.logical_or(named[0:1] == wanted, named[1:2] == wanted)
            spread.append(jnp.broadcast_to(hit.astype(jnp.float32)[:, :tokens_here], (cap, tokens_here)))
        spread = jnp.concatenate(spread, axis=0)
        rank = jnp.dot(spread.astype(jnp.bfloat16), before, preferred_element_type=jnp.float32)
        slot = f32(lax.rem(lax.broadcasted_iota(jnp.int32, rank.shape, 0), cap))
        chosen[b] = (jnp.where(rank == slot, 1.0, 0.0) * spread).astype(jnp.bfloat16)
        columns = jnp.transpose(named)[:tokens_here]
        for place, expert in enumerate((e, y_expert)):
            wanted = expert.astype(jnp.float32)
            hits = [(columns[:, k:k + 1] == wanted).astype(jnp.float32) for k in range(2)]
            scale = hits[0] * columns[:, 2:3] + hits[1] * columns[:, 3:4]
            spread = jnp.broadcast_to(hits[0] + hits[1], (tokens_here, cap))
            rank = jnp.dot(after, spread.astype(jnp.bfloat16), preferred_element_type=jnp.float32)
            slot = f32(lax.broadcasted_iota(jnp.int32, rank.shape, 1))
            picks[b, place] = (jnp.where(rank == slot, 1.0, 0.0) * spread).astype(jnp.bfloat16)
            scales[b, place] = jnp.broadcast_to(scale, (tokens_here, 128))

    def select(b, c):
        table = chosen[b]

        def body(span):
            found = jnp.dot(table, dense[b, :, span], preferred_element_type=jnp.float32).astype(jnp.bfloat16)
            rows[b, core, y, :, span] = found[:cap]
            y_send[b, :, span] = found[cap:]

        tiles(c, body)
        row_to_y(b, c).start()
        row_to_c(b, y, c).start()
        if b >= 4:
            row_to_x(b - 4, y, c).start()

    def finish(b, c):
        def body(span):
            value = f32(partial[b, core, :, :, span]) + f32(red[b, :, :, span])
            if b in (4, 5):
                value = value + f32(x_got[b - 4, :, :, span])
            partial[b, core, :, :, span] = value.astype(jnp.bfloat16)

        tiles(c, body)
        if b >= 6:
            reduce_x(b - 6, c).start()
        else:
            give_y(b, c).start()

    def gather(b, c):
        mine, theirs = picks[b, 0], picks[b, 1]
        scale_mine, scale_theirs = scales[b, 0, :, 0:1], scales[b, 1, :, 0:1]

        def body(span):
            first = jnp.dot(mine, partial[b, core, y, :, span], preferred_element_type=jnp.float32)
            second = jnp.dot(theirs, y_got[b, :, span], preferred_element_type=jnp.float32)
            hold[b, :, span] = first * scale_mine + second * scale_theirs

        tiles(c, body)

    def release(b, c, sources, place, where, arrive, device):
        def body(span):
            value = hold[b, :, span]
            for got, at in sources:
                value = value + f32(got[at, :, span])
            sent[b, :, span] = value.astype(jnp.bfloat16)

        tiles(c, body)
        pass_on(b, place, where, arrive, c, device).start()

    def messages(task, is_inner):
        kind = task[0]
        c = task[-1]
        b = task[1] if len(task) > 1 else 0
        if kind in ("F3", "F6", "F5", "F7"):
            return [("d", {"F3": 1, "F6": 4, "F5": 2, "F7": 5}[kind], c)]
        if kind == "sel":
            return [("d", b, c)]
        if kind == "arr":
            return [("ry", b, c)]
        if kind == "arx":
            return [("rx", b, task[2], c)]
        if kind == "cmp":
            return [("rc", b, 0)]
        if kind == "fin":
            return [("red", b, 0)] + ([("xg", b - 4, c)] if b in (4, 5) else [])
        if kind == "gat":
            return [("gy", b, c)]
        if kind == "rel":
            if b == 1:
                return [("pg", 1, c)]
            if is_inner and b in (4, 5):
                return [("zg", b - 4, c)]
            return [("mg", 1, c)] if is_inner and b == 2 else []
        if kind == "final":
            return [("og", c), ("pg", 0, c)] + ([("mg", 0, c)] if is_inner else [])
        if kind == "kvf":
            return [("kvz", b)]
        if kind == "att":
            return [("kvy", 0)]
        return {"mixs": [("mc",)], "mixf": [("mx",)]}.get(kind, [])

    def perform(task, is_inner):
        kind = task[0]
        c = task[-1]
        b = task[1] if len(task) > 1 else 0
        if kind == "D2":
            to_near(c).start()
        elif kind == "F3":
            x_to_near(c).start()
        elif kind == "F6":
            far_to_near(0, c).start()
        elif kind == "F5":
            near_to_across(c).start()
        elif kind == "F7":
            far_to_near(1, c).start()
        elif kind == "meta":
            remote(meta.at[1:6], meta.at[1:6], meta_sems.at[0], meta_sems.at[1], x_peer).wait_recv()

            def run(slot, carry):
                build(slot)
                return carry

            lax.fori_loop(1, 6, run, 0)
        elif kind == "sel":
            select(b, c)
        elif kind == "arr":
            row_to_c(b, other_y, c).start()
            if b >= 4:
                row_to_x(b - 4, other_y, c).start()
        elif kind == "arx":
            row_to_c(6 + b, groups[task[2]], c).start()
        elif kind == "fin":
            finish(b, c)
        elif kind == "gat":
            gather(b, c)
        elif kind == "rel":
            if b == 1:
                release(b, c, [(p_got, 1)], 0, o_got, o_in, x_peer)
            elif b == 2:
                release(b, c, [(m_got, 1)] if is_inner else [], 0, p_got, p_in, z_peer)
            elif b == 3:
                release(b, c, [], 1, p_got, p_in, z_peer)
            elif is_inner:
                release(b, c, [(z_got, b - 4)], b - 4, m_got, m_in, m_peer)
            else:
                release(b, c, [], b - 4, z_got, z_in, z_peer)
        elif kind == "final":
            def body(span):
                value = hold[0, :, span] + f32(o_got[0, :, span]) + f32(p_got[0, :, span])
                if is_inner:
                    value = value + f32(m_got[0, :, span])
                moe[:, span] = value.astype(jnp.bfloat16)

            tiles(c, body)
        elif kind == "kvs":
            kv_sends[0].start()
            if is_inner:
                kv_sends[1].start()
            kv_y(0).start()
        elif kind == "kvf":
            if is_inner:
                kv_sends[2 + b].start()
            kv_y(b + 1).start()
        elif kind == "mixs":
            a_send[...] = (f32(a_part[other_side, core]) + f32(a_red[other_side])).astype(jnp.bfloat16)
            mix_side.start()
        elif kind == "mixf":
            mixed[...] = (f32(a_part[side, core]) + f32(a_red[side]) + f32(a_got[...])).astype(jnp.bfloat16)

    def plan(order, is_inner):
        seen = {("d", 0, c) for c in range(chunks)}
        pieces, kinds = [[]], []
        for task in order:
            fresh = [message for message in messages(task, is_inner) if message not in seen]
            seen.update(fresh)
            pieces[-1].append((fresh, task))
            if task[0] in BIG:
                kinds.append(BIG[task[0]] + (task[1] if len(task) > 1 else 0))
                pieces.append([])
        return pieces, kinds

    def emit(piece, is_inner):
        for fresh, task in piece:
            for message in fresh:
                wait_for(message)
            if task[0] not in BIG:
                perform(task, is_inner)

    for load in loads[:4]:
        load.wait()
    as_float = f32(x_ref[...])
    mean = jnp.mean(as_float * as_float, axis=1, keepdims=True)
    dense[0] = (as_float * lax.rsqrt(mean + NORM_EPS) * x_gain[...]).astype(jnp.bfloat16)
    meta[0] = jnp.zeros(meta.shape[1:], jnp.float32)
    meta[0, 0:2, 0:tokens_here] = f32(routes_row[...])
    meta[0, 2:4, 0:tokens_here] = weight_row[...]

    pl.semaphore_wait(barrier, len(greeted))
    for item in cards:
        item.start()
    for c in range(chunks):
        to_x(c).start()

        @pl.when(inner)
        def _():
            to_across(c).start()

        if c == 0:
            to_near(c).start()
        else:
            @pl.when(outer)
            def _():
                to_near(c).start()

    build(0)
    for c in range(chunks):
        select(0, c)

    for load in loads[4:10]:
        load.wait()
    lane = lax.broadcasted_iota(jnp.int32, (tok, 128), 1)
    low = lane < HEAD_DIM
    even = lax.rem(lax.div(lane, HEAD_DIM // 4), 2) == 0
    table = turn[...]
    swapped = pltpu.roll(table, HEAD_DIM, 1)
    cosine = jnp.where(low, table, swapped)
    sine = jnp.where(low, swapped, table)

    def turned(raw, gain):
        flat = f32(raw)
        square = flat * flat
        left = jnp.sum(jnp.where(low, square, 0.0), axis=1, keepdims=True)
        right = jnp.sum(jnp.where(low, 0.0, square), axis=1, keepdims=True)
        mean_square = jnp.where(low, left, right) * (1.0 / HEAD_DIM)
        unit = flat * lax.rsqrt(mean_square + NORM_EPS) * gain
        partner = jnp.where(
            even, -pltpu.roll(unit, 128 - HEAD_DIM // 4, 1), pltpu.roll(unit, HEAD_DIM // 4, 1)
        )
        return unit * cosine + partner * sine

    for pair in range(kv_all.shape[0] // 2):
        span = slice(pair * 128, (pair + 1) * 128)
        k_rows = turned(k_raw[:, span], k_gain[:, span])
        v_rows = f32(v_raw[:, span])
        kv_all[2 * pair, e] = jnp.where(low, k_rows, pltpu.roll(v_rows, HEAD_DIM, 1)).astype(jnp.bfloat16)
        kv_all[2 * pair + 1, e] = jnp.where(low, pltpu.roll(k_rows, HEAD_DIM, 1), v_rows).astype(jnp.bfloat16)

    for pair in range(pairs):
        span = slice(pair * 128, (pair + 1) * 128)
        q_rows = turned(q_raw[:, span], q_gain[:, span])
        q_ref[2 * pair] = jnp.where(low, q_rows, 0.0).astype(jnp.bfloat16)
        q_ref[2 * pair + 1] = jnp.where(low, pltpu.roll(q_rows, HEAD_DIM, 1), 0.0).astype(jnp.bfloat16)

    for load in loads[10:]:
        load.wait()

    def attend(pair):
        kv = kv_all[lax.div(pair * 2 * kv_all.shape[0], pairs * 2)].reshape(n * tok, 128)
        halves = []
        for h in range(2):
            scores = lax.dot_general(
                q_ref[pair * 2 + h], kv, (((1,), (1,)), ((), ())), preferred_element_type=jnp.float32
            ) * (HEAD_DIM ** (-0.5))
            peak = jnp.max(scores, axis=1, keepdims=True)
            weights = jnp.exp(scores - peak)
            total = jnp.sum(weights, axis=1, keepdims=True)
            summed = jnp.dot(weights.astype(jnp.bfloat16), kv, preferred_element_type=jnp.float32)
            halves.append(summed / total)
        joined = jnp.where(low, pltpu.roll(halves[0], HEAD_DIM, 1), halves[1])
        attended[pair] = joined.astype(jnp.bfloat16)

    inner_pieces, inner_kinds = plan(INNER_ORDER, True)
    outer_pieces, outer_kinds = plan(OUTER_ORDER, False)
    count = len(inner_kinds)

    def step(s, carry):
        u = jnp.where(inner, inner_kinds[0], outer_kinds[0])
        for place in range(1, count):
            u = jnp.where(s == place, jnp.where(inner, inner_kinds[place], outer_kinds[place]), u)
        for place in range(count):
            @pl.when(jnp.logical_and(s == place, inner))
            def _():
                emit(inner_pieces[place], True)

            @pl.when(jnp.logical_and(s == place, outer))
            def _():
                emit(outer_pieces[place], False)

        @pl.when(u < 8)
        def _():
            tokens = rows[u].reshape(4 * cap, width)
            gate = jnp.dot(tokens, wg[...], preferred_element_type=jnp.float32)
            up = jnp.dot(tokens, wu[...], preferred_element_type=jnp.float32)
            hidden = (gate / (1.0 + jnp.exp(-gate)) * up).astype(jnp.bfloat16)
            for tile in range(0, width, TILE):
                product = jnp.dot(hidden, wd[:, tile:tile + TILE], preferred_element_type=jnp.float32)
                partial[u, :, :, :, tile:tile + TILE] = product.astype(jnp.bfloat16).reshape(2, 2, cap, TILE)
                if (tile + TILE) % part == 0:
                    reduce_c(u, tile // part).start()

        @pl.when(jnp.logical_and(u >= 8, u < 10))
        def _():
            attend(2 * (u - 8))
            attend(2 * (u - 8) + 1)

        @pl.when(u == 10)
        def _():
            for tile in range(0, width, TILE):
                product = jnp.dot(attended[0], ow[0, :, tile:tile + TILE], preferred_element_type=jnp.float32)
                for p in range(1, pairs):
                    product += jnp.dot(attended[p], ow[p, :, tile:tile + TILE], preferred_element_type=jnp.float32)
                a_part[:, :, :, tile:tile + TILE] = product.astype(jnp.bfloat16).reshape(2, 2, tok // 4, TILE)
            mix_core.start()

        return carry

    lax.fori_loop(0, count, step, 0)

    @pl.when(inner)
    def _():
        emit(inner_pieces[count], True)

    @pl.when(outer)
    def _():
        emit(outer_pieces[count], False)

    mix_core.wait_send()
    mix_side.wait_send()

    def sent_all(ref, sem):
        remote(ref, ref, sem, meta_sems.at[1], x_peer).wait_send()

    sent_all(kv_all.at[:, 0:4], kvy_sems.at[0])
    kv_sends[0].wait_send()
    sent_all(meta.at[0:5], meta_sems.at[0])
    sent_all(dense.at[0:3], dn_out.at[0])

    @pl.when(inner)
    def _():
        sent_all(kv_all.at[:, 0:4], kvz_out.at[1])
        sent_all(dense.at[0:4], dn_out.at[1])

    sent_all(y_send, outs.at[0])
    sent_all(rows.at[:, core], outs.at[1])
    sent_all(rows.at[4:6, core], outs.at[2])
    sent_all(partial.at[:, other_core], outs.at[3])
    sent_all(partial.at[6:8, core], outs.at[4])
    sent_all(partial.at[0:6, core, other_y], outs.at[5])
    sent_all(sent.at[1:6], outs.at[6])


def turn_table(tokens):
    quarter = HEAD_DIM // 4
    inverse = np.power(ROPE_BASE, -np.arange(quarter, dtype=np.float64) / quarter)
    places = np.arange(tokens)
    row = (places // GRID_W)[:, None] * inverse
    col = (places % GRID_W)[:, None] * inverse
    angles = np.concatenate([row, row, col, col], axis=1)
    return np.concatenate([np.cos(angles), np.sin(angles)], axis=1).astype(np.float32)


def fused(x, x_gain, routes, route_weight, queries, keys, values, q_gain, k_gain, gate_weight, up_weight, down_weight, out_weight):
    n = lax.axis_size("ep")
    tok_exp, width = x.shape
    cap = 2 * routes.shape[1] * tok_exp // n
    tok = queries.shape[0]
    heads = queries.shape[1] // HEAD_DIM
    kv_count = keys.shape[1] // HEAD_DIM
    pairs = heads // 2
    hidden = gate_weight.shape[1]
    bf = jnp.bfloat16
    vmem = pl.BlockSpec(memory_space=pltpu.VMEM)
    anywhere = pl.BlockSpec(memory_space=pl.ANY)
    dma = pltpu.SemaphoreType.DMA
    return pl.pallas_call(
        functools.partial(fused_kernel, n),
        out_shape=(
            pltpu.VMEM((tok_exp, width), bf),
            pltpu.VMEM((tok // 4, width), bf),
        ),
        in_specs=[anywhere] * 14,
        out_specs=(vmem, vmem),
        scratch_shapes=[
            pltpu.VMEM((tok_exp, width), bf),
            pltpu.VMEM((1, width), jnp.float32),
            pltpu.VMEM((routes.shape[1], tok_exp), jnp.int32),
            pltpu.VMEM((routes.shape[1], tok_exp), jnp.float32),
            pltpu.VMEM((tok, heads * HEAD_DIM), bf),
            pltpu.VMEM((tok, kv_count * HEAD_DIM), bf),
            pltpu.VMEM((tok, kv_count * HEAD_DIM), bf),
            pltpu.VMEM((1, heads * HEAD_DIM), jnp.float32),
            pltpu.VMEM((1, kv_count * HEAD_DIM), jnp.float32),
            pltpu.VMEM((6, tok_exp, width), bf),
            pltpu.VMEM((6, 8, 128), jnp.float32),
            pltpu.VMEM((6, 2 * cap, tok_exp), bf),
            pltpu.VMEM((6, 2, tok_exp, cap), bf),
            pltpu.VMEM((6, 2, tok_exp, 128), jnp.float32),
            pltpu.VMEM((8, 2, 2, cap, width), bf),
            pltpu.VMEM((6, cap, width), bf),
            pltpu.VMEM((8, 2, 2, cap, width), bf),
            pltpu.VMEM((8, 2, cap, width), bf),
            pltpu.VMEM((2, 2, cap, width), bf),
            pltpu.VMEM((6, cap, width), bf),
            pltpu.VMEM((6, tok_exp, width), jnp.float32),
            pltpu.VMEM((6, tok_exp, width), bf),
            pltpu.VMEM((2, tok_exp, width), bf),
            pltpu.VMEM((2, tok_exp, width), bf),
            pltpu.VMEM((2, tok_exp, width), bf),
            pltpu.VMEM((1, tok_exp, width), bf),
            pltpu.VMEM((heads, tok, 128), bf),
            pltpu.VMEM((tok, 128), jnp.float32),
            pltpu.VMEM((width, hidden), bf),
            pltpu.VMEM((width, hidden), bf),
            pltpu.VMEM((hidden, width), bf),
            pltpu.VMEM((pairs, 128, width), bf),
            pltpu.VMEM((kv_count, n, tok, 128), bf),
            pltpu.VMEM((pairs, tok, 128), bf),
            pltpu.VMEM((2, 2, tok // 4, width), bf),
            pltpu.VMEM((2, tok // 4, width), bf),
            pltpu.VMEM((tok // 4, width), bf),
            pltpu.VMEM((tok // 4, width), bf),
            dma((14,)),
            dma((2,)),
            dma((3,)),
            dma((2,)),
            dma((2,)),
            dma((5, CHUNKS)),
            dma((2,)),
            dma((6, CHUNKS)),
            dma((8,)),
            dma((2, 2, CHUNKS)),
            dma((8,)),
            dma((2, CHUNKS)),
            dma((6, CHUNKS)),
            dma((7,)),
            dma((2, CHUNKS)),
            dma((2, CHUNKS)),
            dma((2, CHUNKS)),
            dma((1, CHUNKS)),
            dma((2, 2)),
        ],
        compiler_params=pltpu.CompilerParams(
            collective_id=0, has_side_effects=True, vmem_limit_bytes=62 * 1024 * 1024
        ),
    )(
        x,
        x_gain.reshape(1, width),
        jnp.transpose(routes),
        jnp.transpose(route_weight),
        queries,
        keys,
        values,
        q_gain.reshape(1, -1),
        k_gain.reshape(1, -1),
        jnp.asarray(turn_table(n * tok)),
        gate_weight,
        up_weight,
        down_weight,
        out_weight.reshape(pairs, 128, width),
    )


def plain_shards(
    queries,
    keys,
    values,
    query_gain,
    key_gain,
    out_weight,
    expert_input,
    norm_gain,
    routes,
    route_weight,
    gate_weight,
    up_weight,
    down_weight,
):
    tok_mix = queries.shape[0]
    head_count = query_gain.shape[0] // HEAD_DIM
    kv_count = key_gain.shape[0] // HEAD_DIM
    group_size = head_count // kv_count
    offset = lax.axis_index("ep") * tok_mix
    q_turned = head_norm(queries, query_gain, head_count, offset)
    k_turned = head_norm(keys, key_gain, kv_count, offset)
    grouped = q_turned.reshape(tok_mix, kv_count, group_size, HEAD_DIM)
    score_scale = HEAD_DIM ** (-0.5)
    start_state = (
        jnp.full((kv_count, group_size, tok_mix), -jnp.inf, jnp.float32),
        jnp.zeros((kv_count, group_size, tok_mix), jnp.float32),
        jnp.zeros((tok_mix, kv_count, group_size, HEAD_DIM), jnp.float32),
    )
    running = start_state
    key_piece = lax.all_gather(k_turned, "ep", axis=0, tiled=True)
    value_piece = lax.all_gather(values, "ep", axis=0, tiled=True)
    length = key_piece.shape[0]
    block_len = length
    while block_len > 2048 and block_len % 2 == 0:
        block_len = block_len // 2
    key_blocks = key_piece.reshape(length // block_len, block_len, key_piece.shape[1])
    value_blocks = value_piece.reshape(length // block_len, block_len, value_piece.shape[1])

    def advance(inner_state, key_value):
        return (absorb(inner_state, key_value[0], key_value[1], grouped, score_scale), None)

    running, unused = lax.scan(advance, running, (key_blocks, value_blocks))
    final_max, weight_sum, summed = running
    attended = (
        (summed / jnp.transpose(weight_sum, (2, 0, 1))[..., None])
        .reshape(tok_mix, -1)
        .astype(jnp.bfloat16)
    )
    mixed = lax.psum_scatter(
        jnp.dot(attended, out_weight, preferred_element_type=jnp.float32).astype(jnp.bfloat16),
        "tp",
        scatter_dimension=0,
        tiled=True,
    )
    tok_exp = expert_input.shape[0]
    top_count = routes.shape[1]
    expert_count = lax.axis_size("ep")
    capacity = 2 * top_count * tok_exp // expert_count
    as_float = expert_input.astype(jnp.float32)
    normed = (
        as_float
        * lax.rsqrt(jnp.mean(as_float * as_float, axis=-1, keepdims=True) + NORM_EPS)
        * norm_gain
    ).astype(jnp.bfloat16)
    flat_routes = routes.reshape(-1)
    route_hits = (
        flat_routes[:, None] == jnp.arange(expert_count, dtype=jnp.int32)[None, :]
    ).astype(jnp.int32)
    slot_rank = jnp.sum((jnp.cumsum(route_hits, axis=0) - route_hits) * route_hits, axis=1)
    slot_ids = flat_routes * capacity + slot_rank
    placed = jnp.arange(expert_count * capacity, dtype=jnp.int32)[:, None] == slot_ids[None, :]
    placed = jnp.any(placed.reshape(expert_count * capacity, tok_exp, top_count), axis=2).astype(
        jnp.bfloat16
    )
    outbound = jnp.dot(placed, normed, preferred_element_type=jnp.float32).astype(jnp.bfloat16)
    model_width = outbound.shape[1]
    half_cap = capacity // 2
    laid = outbound.reshape(expert_count, capacity, model_width)
    first_half = run_experts(
        laid[:, :half_cap].reshape(expert_count * half_cap, model_width),
        gate_weight,
        up_weight,
        down_weight,
    )
    second_half = run_experts(
        laid[:, half_cap:].reshape(expert_count * half_cap, model_width),
        gate_weight,
        up_weight,
        down_weight,
    )
    back_rows = jnp.concatenate(
        [
            first_half.reshape(expert_count, half_cap, model_width),
            second_half.reshape(expert_count, half_cap, model_width),
        ],
        axis=1,
    )
    back_rows = back_rows.reshape(expert_count * capacity, model_width)
    picked = back_rows[slot_ids.reshape(tok_exp, top_count)]
    moe_out = jnp.sum(picked.astype(jnp.float32) * route_weight[:, :, None], axis=1).astype(
        jnp.bfloat16
    )
    return (mixed, moe_out)


def shards(
    queries,
    keys,
    values,
    query_gain,
    key_gain,
    out_weight,
    expert_input,
    norm_gain,
    routes,
    route_weight,
    gate_weight,
    up_weight,
    down_weight,
):
    tok_exp = expert_input.shape[0]
    top_count = routes.shape[1]
    expert_count = lax.axis_size("ep")
    capacity = 2 * top_count * tok_exp // expert_count
    if capacity % 16 != 0 or lax.axis_size("tp") != 4 or expert_count != 8:
        return plain_shards(
            queries,
            keys,
            values,
            query_gain,
            key_gain,
            out_weight,
            expert_input,
            norm_gain,
            routes,
            route_weight,
            gate_weight,
            up_weight,
            down_weight,
        )
    moe_out, mixed = fused(
        expert_input,
        norm_gain,
        routes,
        route_weight,
        queries,
        keys,
        values,
        query_gain,
        key_gain,
        gate_weight[0],
        up_weight[0],
        down_weight[0],
        out_weight,
    )
    return (mixed, moe_out)


def solution(mesh):
    placed = (
        P("ep", "tp"),
        P("ep", "tp"),
        P("ep", "tp"),
        P("tp"),
        P("tp"),
        P("tp", None),
        P(("ep", "tp"), None),
        P(),
        P(("ep", "tp"), None),
        P(("ep", "tp"), None),
        P("ep", None, "tp"),
        P("ep", None, "tp"),
        P("ep", "tp", None),
    )
    return jax.shard_map(
        shards,
        mesh=mesh,
        in_specs=placed,
        out_specs=(P(("ep", "tp"), None), P(("ep", "tp"), None)),
        check_vma=False,
    )
```

```python
import functools

import jax
import jax.numpy as jnp
import numpy as np
from jax import lax
from jax.experimental import pallas as pl
from jax.experimental.pallas import tpu as pltpu
from jax.sharding import PartitionSpec as P

HEAD_DIM = 64
GRID_W = 128


NORM_EPS = 1e-06
ROPE_BASE = 10000.0


def rotate(vectors, grid_rows, grid_cols):
    quarter = vectors.shape[-1] // 4
    inverse = ROPE_BASE ** (-jnp.arange(quarter, dtype=jnp.float32) / quarter)
    angle_row = grid_rows[:, None] * inverse
    angle_col = grid_cols[:, None] * inverse
    angles = jnp.concatenate([angle_row, angle_row, angle_col, angle_col], axis=-1)[:, None, :]
    part_one, part_two, part_three, part_four = jnp.split(vectors, 4, axis=-1)
    turned = jnp.concatenate([-part_two, part_one, -part_four, part_three], axis=-1)
    return vectors * jnp.cos(angles) + turned * jnp.sin(angles)


def head_norm(raw_rows, gains, head_count, offset):
    row_count = raw_rows.shape[0]
    flat_rows = raw_rows.astype(jnp.float32).reshape(row_count, head_count, -1)
    unit_vec = flat_rows * lax.rsqrt(
        jnp.mean(flat_rows * flat_rows, axis=-1, keepdims=True) + NORM_EPS
    )
    unit_vec = unit_vec * gains.reshape(head_count, -1)
    places = offset + jnp.arange(row_count, dtype=jnp.int32)
    grid_rows = (places // GRID_W).astype(jnp.float32)
    grid_cols = (places % GRID_W).astype(jnp.float32)
    return rotate(unit_vec, grid_rows, grid_cols).astype(jnp.bfloat16).reshape(row_count, -1)


def absorb(running, key_block, value_block, grouped, score_scale):
    run_max, weight_sum, summed = running
    kv_count = grouped.shape[1]
    key_heads = key_block.reshape(key_block.shape[0], kv_count, -1)
    value_heads = value_block.reshape(value_block.shape[0], kv_count, -1)
    scores = (
        jnp.einsum("qhgd,khd->hgqk", grouped, key_heads, preferred_element_type=jnp.float32)
        * score_scale
    )
    new_max = jnp.maximum(run_max, jnp.max(scores, axis=-1))
    rescale = jnp.exp(run_max - new_max)
    weights = jnp.exp(scores - new_max[..., None])
    weight_sum = weight_sum * rescale + jnp.sum(weights, axis=-1)
    update = jnp.einsum(
        "hgqk,khd->qhgd",
        weights.astype(jnp.bfloat16),
        value_heads,
        preferred_element_type=jnp.float32,
    )
    summed = summed * jnp.transpose(rescale, (2, 0, 1))[..., None] + update
    return (new_max, weight_sum, summed)


def run_experts(sending, gate_weight, up_weight, down_weight):
    arrived = lax.all_to_all(sending, "ep", split_axis=0, concat_axis=0, tiled=True)
    shard_rows = lax.all_gather(arrived, "tp", axis=0, tiled=True)
    gate_out = jnp.dot(shard_rows, gate_weight[0], preferred_element_type=jnp.float32)
    up_out = jnp.dot(shard_rows, up_weight[0], preferred_element_type=jnp.float32)
    hidden = (jax.nn.silu(gate_out) * up_out).astype(jnp.bfloat16)
    results = lax.psum_scatter(
        jnp.dot(hidden, down_weight[0], preferred_element_type=jnp.float32).astype(jnp.bfloat16),
        "tp",
        scatter_dimension=0,
        tiled=True,
    )
    return lax.all_to_all(results, "ep", split_axis=0, concat_axis=0, tiled=True)


MESH = pl.DeviceIdType.MESH
TILE = 1024
CHUNKS = 4


def flip(index, pattern, size):
    result = 0
    bit = 1
    while bit < size:
        both = lax.rem(lax.div(index, bit) + lax.div(pattern, bit), 2)
        result = result + both * bit
        bit = bit * 2
    return result


def f32(value):
    return value.astype(jnp.float32)


INNER_ORDER = (
    ("F6", 0), ("meta",), ("sel", 1, 0), ("sel", 4, 0), ("F6", 1), ("sel", 2, 1), ("sel", 2, 0),
    ("sel", 4, 1), ("F5", 1), ("arr", 0, 2), ("F6", 2), ("F6", 3), ("F5", 0), ("sel", 4, 3), ("sel", 4, 2),
    ("F3", 2), ("sel", 2, 3), ("sel", 1, 2), ("sel", 1, 3), ("arx", 0, 0, 0), ("arr", 2, 0), ("F5", 3),
    ("arr", 4, 2), ("sel", 2, 2), ("F7", 1), ("F3", 1), ("F5", 2), ("arr", 4, 0), ("arr", 2, 1),
    ("sel", 5, 0), ("sel", 5, 1), ("F3", 3), ("F3", 0), ("sel", 3, 0), ("arx", 1, 0, 0), ("arr", 4, 1),
    ("arr", 0, 1), ("sel", 5, 2), ("sel", 3, 2), ("arr", 5, 0), ("sel", 5, 3), ("arr", 2, 3), ("arr", 3, 0),
    ("F7", 3), ("F7", 2), ("arr", 2, 2), ("sel", 1, 1), ("sel", 3, 1), ("F7", 0), ("kvs",), ("arx", 0, 0, 2),
    ("arr", 5, 2), ("arx", 1, 0, 2), ("arr", 4, 3), ("sel", 3, 3), ("arx", 0, 1, 1), ("kvf", 1),
    ("arr", 5, 3), ("arx", 1, 0, 3), ("cmp", 4), ("arx", 0, 1, 0), ("arx", 0, 0, 1), ("arx", 0, 1, 3),
    ("arr", 1, 2), ("cmp", 2), ("arx", 1, 1, 0), ("arr", 0, 0), ("arr", 3, 2), ("fin", 2, 2), ("arr", 3, 1),
    ("arr", 1, 3), ("arx", 0, 0, 3), ("kvf", 0), ("arr", 3, 3), ("arr", 1, 0), ("arx", 0, 1, 2),
    ("arr", 5, 1), ("arr", 1, 1), ("cmp", 6), ("arr", 0, 3), ("cmp", 3), ("fin", 2, 3), ("arx", 1, 1, 3),
    ("arx", 1, 1, 2), ("kvf", 2), ("fin", 6, 3), ("arx", 1, 1, 1), ("fin", 6, 0), ("arx", 1, 0, 1), ("D2", 2),
    ("cmp", 5), ("fin", 3, 3), ("cmp", 7), ("fin", 4, 3), ("D2", 1), ("fin", 3, 2), ("fin", 3, 1),
    ("fin", 7, 0), ("fin", 7, 1), ("fin", 3, 0), ("att", 0), ("cmp", 1), ("fin", 7, 3), ("gat", 3, 3),
    ("fin", 2, 0), ("cmp", 0), ("D2", 3), ("fin", 4, 0), ("gat", 3, 0), ("fin", 6, 2), ("gat", 3, 2),
    ("fin", 1, 1), ("gat", 3, 1), ("fin", 1, 3), ("fin", 7, 2), ("fin", 2, 1), ("att", 1), ("fin", 5, 1),
    ("mixp",), ("gat", 4, 0), ("rel", 3, 0), ("rel", 3, 3), ("gat", 4, 3), ("rel", 3, 1), ("fin", 5, 3),
    ("fin", 0, 0), ("rel", 4, 0), ("rel", 4, 3), ("fin", 6, 1), ("gat", 2, 2), ("fin", 5, 2), ("fin", 1, 0),
    ("mixs",), ("gat", 1, 1), ("rel", 3, 2), ("gat", 5, 3), ("gat", 1, 3), ("gat", 2, 0), ("fin", 0, 2),
    ("rel", 5, 3), ("fin", 4, 1), ("fin", 4, 2), ("fin", 5, 0), ("gat", 2, 3), ("rel", 1, 1), ("gat", 5, 2),
    ("rel", 5, 2), ("gat", 5, 1), ("fin", 0, 1), ("rel", 2, 3), ("rel", 5, 1), ("gat", 1, 0), ("gat", 0, 2),
    ("gat", 0, 0), ("gat", 2, 1), ("rel", 1, 0), ("gat", 4, 2), ("fin", 1, 2), ("gat", 4, 1), ("gat", 5, 0),
    ("fin", 0, 3), ("rel", 2, 2), ("rel", 5, 0), ("gat", 0, 1), ("rel", 1, 3), ("rel", 4, 2), ("rel", 4, 1),
    ("gat", 1, 2), ("rel", 2, 1), ("mixf",), ("gat", 0, 3), ("rel", 1, 2), ("rel", 2, 0), ("final", 0),
    ("final", 1), ("final", 2), ("final", 3),
)
OUTER_ORDER = (
    ("meta",), ("sel", 2, 0), ("kvs",), ("sel", 1, 1), ("arr", 0, 2), ("arr", 0, 0), ("sel", 4, 0),
    ("arr", 0, 3), ("arr", 0, 1), ("sel", 1, 0), ("sel", 4, 1), ("cmp", 0), ("arr", 4, 0), ("sel", 4, 2),
    ("F3", 0), ("sel", 1, 3), ("F3", 2), ("arr", 4, 1), ("sel", 4, 3), ("arx", 0, 0, 0), ("arr", 4, 2),
    ("F3", 1), ("sel", 1, 2), ("arr", 2, 0), ("arx", 0, 1, 0), ("arx", 0, 0, 2), ("sel", 3, 2), ("arr", 4, 3),
    ("fin", 0, 2), ("arx", 0, 0, 3), ("arx", 0, 1, 2), ("F3", 3), ("arx", 0, 0, 1), ("sel", 5, 1),
    ("arx", 0, 1, 1), ("fin", 0, 1), ("arx", 0, 1, 3), ("fin", 0, 0), ("cmp", 6), ("arr", 5, 1), ("cmp", 4),
    ("fin", 6, 0), ("sel", 3, 3), ("sel", 3, 1), ("fin", 6, 1), ("sel", 3, 0), ("arr", 1, 1), ("fin", 6, 3),
    ("fin", 4, 0), ("sel", 5, 3), ("arr", 3, 1), ("arr", 3, 3), ("arr", 3, 2), ("arr", 3, 0), ("fin", 4, 1),
    ("gat", 4, 0), ("arr", 1, 3), ("sel", 5, 2), ("cmp", 3), ("fin", 4, 3), ("sel", 5, 0), ("rel", 4, 0),
    ("gat", 4, 1), ("fin", 3, 1), ("arr", 5, 3), ("fin", 3, 2), ("arr", 1, 0), ("arr", 1, 2), ("kvf", 0),
    ("rel", 4, 1), ("arr", 5, 2), ("cmp", 1), ("arr", 5, 0), ("arx", 1, 0, 1), ("fin", 3, 3), ("fin", 6, 2),
    ("gat", 4, 3), ("gat", 0, 0), ("gat", 3, 1), ("rel", 4, 3), ("arx", 1, 0, 3), ("arx", 1, 1, 2),
    ("gat", 3, 2), ("rel", 3, 1), ("arx", 1, 1, 3), ("arx", 1, 1, 1), ("gat", 0, 1), ("arx", 1, 0, 0),
    ("arx", 1, 0, 2), ("arx", 1, 1, 0), ("rel", 3, 2), ("kvf", 2), ("kvf", 1), ("cmp", 7), ("cmp", 5),
    ("fin", 7, 3), ("fin", 4, 2), ("fin", 7, 2), ("gat", 3, 3), ("fin", 7, 1), ("fin", 3, 0), ("rel", 3, 3),
    ("sel", 2, 1), ("sel", 2, 2), ("att", 0), ("gat", 4, 2), ("rel", 4, 2), ("fin", 5, 3), ("fin", 7, 0),
    ("gat", 3, 0), ("rel", 3, 0), ("att", 1), ("fin", 5, 2), ("sel", 2, 3), ("mixp",), ("gat", 5, 3),
    ("arr", 2, 2), ("arr", 2, 1), ("rel", 5, 3), ("fin", 1, 3), ("gat", 0, 2), ("fin", 5, 1), ("fin", 1, 1),
    ("gat", 5, 2), ("mixs",), ("arr", 2, 3), ("fin", 5, 0), ("rel", 5, 2), ("cmp", 2), ("gat", 1, 3),
    ("fin", 1, 0), ("gat", 5, 1), ("rel", 5, 1), ("fin", 2, 2), ("gat", 5, 0), ("rel", 5, 0), ("fin", 2, 0),
    ("gat", 1, 0), ("fin", 2, 1), ("gat", 1, 1), ("fin", 1, 2), ("rel", 1, 1), ("gat", 2, 2), ("fin", 2, 3),
    ("rel", 2, 2), ("rel", 1, 0), ("gat", 2, 0), ("rel", 2, 0), ("gat", 1, 2), ("rel", 1, 3), ("fin", 0, 3),
    ("gat", 2, 1), ("rel", 1, 2), ("gat", 2, 3), ("rel", 2, 1), ("rel", 2, 3), ("gat", 0, 3), ("mixf",),
    ("final", 1), ("final", 2), ("final", 3), ("final", 0),
)


BIG = {"cmp": 0, "att": 8, "mixp": 10}


def fused_kernel(
    n,
    x_hbm,
    x_gain_hbm,
    routes_hbm,
    weight_hbm,
    q_hbm,
    k_hbm,
    v_hbm,
    q_gain_hbm,
    k_gain_hbm,
    turn_hbm,
    wg_hbm,
    wu_hbm,
    wd_hbm,
    ow_hbm,
    moe,
    mixed,
    x_ref,
    x_gain,
    routes_row,
    weight_row,
    q_raw,
    k_raw,
    v_raw,
    q_gain,
    k_gain,
    dense,
    meta,
    chosen,
    picks,
    scales,
    rows,
    y_send,
    partial,
    red,
    x_got,
    y_got,
    hold,
    sent,
    z_got,
    m_got,
    p_got,
    o_got,
    q_ref,
    turn,
    wg,
    wu,
    wd,
    ow,
    kv_all,
    attended,
    a_part,
    a_red,
    a_send,
    a_got,
    load_sem,
    kvz_out,
    kvz_in,
    kvy_sems,
    dn_out,
    dn_in,
    meta_sems,
    row_y,
    row_c,
    row_x,
    red_in,
    sum_x,
    sum_y,
    outs,
    z_in,
    m_in,
    p_in,
    o_in,
    mix_sems,
):
    e = lax.axis_index("ep")
    t = lax.axis_index("tp")
    side = lax.div(t, 2)
    core = lax.rem(t, 2)
    other_side = 1 - side
    other_core = 1 - core
    layer = lax.div(e, 2)
    y = lax.rem(e, 2)
    other_y = 1 - y
    near = layer + 1 - 2 * lax.rem(layer, 2)
    last = n // 2 - 1
    across = last - layer
    inner = jnp.logical_and(layer > 0, layer < last)
    outer = jnp.logical_not(inner)
    half = lax.div(layer, 2)
    far_inner = 2 - half
    far_outer = last * (1 - half)
    x_tp = other_side * 2 + core
    x_peer = (e, x_tp)
    c_peer = (e, side * 2 + other_core)
    y_expert = layer * 2 + other_y
    y_peer = (y_expert, t)
    z_peer = (near * 2 + y, t)
    m_peer = (across * 2 + y, t)
    corner = (near * 2 + y, x_tp)
    cap, width = rows.shape[3], rows.shape[4]
    pairs = attended.shape[0]
    tok = attended.shape[1]
    tokens_here = x_ref.shape[0]
    chunks = dn_in.shape[1]
    part = width // chunks
    groups = (y, other_y)

    def remote(src, dst, send, recv, device):
        return pltpu.make_async_remote_copy(
            src_ref=src, dst_ref=dst, send_sem=send, recv_sem=recv, device_id=device, device_id_type=MESH
        )

    def cols(c):
        return pl.ds(c * part, part)

    far_peers = [(far_inner * 2 + y, t), (far_outer * 2 + y, t)]
    barrier = pltpu.get_barrier_semaphore()
    greeted = [x_peer, c_peer, y_peer, z_peer, corner] + far_peers
    for peer in greeted:
        pl.semaphore_signal(barrier, inc=1, device_id=peer, device_id_type=MESH)

    loads = [
        pltpu.make_async_copy(a, b, load_sem.at[k])
        for k, (a, b) in enumerate(
            [
                (x_hbm, x_ref),
                (x_gain_hbm, x_gain),
                (routes_hbm, routes_row),
                (weight_hbm, weight_row),
                (turn_hbm.at[pl.ds(pl.multiple_of(e * tok, 8), tok)], turn),
                (k_hbm, k_raw),
                (v_hbm, v_raw),
                (k_gain_hbm, k_gain),
                (q_hbm, q_raw),
                (q_gain_hbm, q_gain),
                (wg_hbm, wg),
                (wu_hbm, wu),
                (wd_hbm, wd),
                (ow_hbm, ow),
            ]
        )
    ]
    for load in loads:
        load.start()

    def kv_z(owner, out, place, device):
        return remote(kv_all.at[:, owner], kv_all.at[:, owner], kvz_out.at[min(out, 1)], kvz_in.at[place], device)

    stops = [layer, near, far_inner, far_outer]

    def kv_y(j):
        owner = stops[j] * 2 + y
        return remote(kv_all.at[:, owner], kv_all.at[:, owner], kvy_sems.at[0], kvy_sems.at[1], y_peer)

    kv_sends = [
        kv_z(e, 0, 0, z_peer),
        kv_z(e, 1, 1, m_peer),
        kv_z(near * 2 + y, 2, 2, m_peer),
        kv_z(far_inner * 2 + y, 3, 1, z_peer),
        kv_z(far_outer * 2 + y, 4, 2, z_peer),
    ]

    def block(source, target, number, c, device):
        return remote(
            dense.at[source, :, cols(c)],
            dense.at[target, :, cols(c)],
            dn_out.at[number // 4],
            dn_in.at[target - 1, c],
            device,
        )

    def to_x(c):
        return block(0, 1, 1, c, x_peer)

    def to_near(c):
        return block(0, 2, 2, c, z_peer)

    def x_to_near(c):
        return block(1, 3, 3, c, z_peer)

    def to_across(c):
        return block(0, 4, 4, c, m_peer)

    def near_to_across(c):
        return block(2, 5, 5, c, m_peer)

    def far_to_near(k, c):
        return block(4 + k, 4 + k, 6 + k, c, z_peer)

    far_slot = jnp.where(inner, 4, 5)

    def card(slot, number, device):
        return remote(meta.at[0], meta.at[slot], meta_sems.at[0], meta_sems.at[1], device)

    cards = [
        card(1, 1, x_peer),
        card(2, 2, z_peer),
        card(3, 3, corner),
        card(far_slot, 4, far_peers[0]),
        card(far_slot, 5, far_peers[1]),
    ]

    def row_to_y(b, c):
        return remote(
            y_send.at[b, :, cols(c)], rows.at[b, core, y, :, cols(c)], outs.at[0], row_y.at[b, c], y_peer
        )

    def row_to_c(b, g, c):
        here = rows.at[b, core, g, :, cols(c)]
        return remote(here, here, outs.at[1], row_c.at[b], c_peer)

    def row_to_x(k, g, c):
        return remote(
            rows.at[4 + k, core, g, :, cols(c)],
            rows.at[6 + k, core, g, :, cols(c)],
            outs.at[2],
            row_x.at[k, g, c],
            x_peer,
        )

    def reduce_c(b, c):
        return remote(
            partial.at[b, other_core, :, :, cols(c)],
            red.at[b, :, :, cols(c)],
            outs.at[3],
            red_in.at[b],
            c_peer,
        )

    def reduce_x(k, c):
        return remote(
            partial.at[6 + k, core, :, :, cols(c)],
            x_got.at[k, :, :, cols(c)],
            outs.at[4],
            sum_x.at[k, c],
            x_peer,
        )

    def give_y(b, c):
        return remote(
            partial.at[b, core, other_y, :, cols(c)],
            y_got.at[b, :, cols(c)],
            outs.at[5],
            sum_y.at[b, c],
            y_peer,
        )

    def pass_on(b, place, where, arrive, c, device):
        return remote(sent.at[b, :, cols(c)], where.at[place, :, cols(c)], outs.at[6], arrive.at[place, c], device)

    mix_core = remote(a_part.at[:, other_core], a_red, mix_sems.at[0, 0], mix_sems.at[1, 0], c_peer)
    mix_side = remote(a_send, a_got, mix_sems.at[0, 1], mix_sems.at[1, 1], x_peer)

    def wait_for(message):
        kind = message[0]
        c = message[-1]
        k = message[1] if len(message) > 1 else 0
        if kind == "d":
            block(k, k, 0, c, x_peer).wait_recv()
        elif kind == "ry":
            remote(
                y_send.at[k, :, cols(c)],
                rows.at[k, core, other_y, :, cols(c)],
                outs.at[0],
                row_y.at[k, c],
                y_peer,
            ).wait_recv()
        elif kind == "rc":
            there = rows.at[k, other_core]
            remote(there, there, outs.at[1], row_c.at[k], c_peer).wait_recv()
        elif kind == "rx":
            row_to_x(k, groups[message[2]], c).wait_recv()
        elif kind == "red":
            remote(red.at[k], red.at[k], outs.at[3], red_in.at[k], c_peer).wait_recv()
        elif kind == "xg":
            reduce_x(k, c).wait_recv()
        elif kind == "gy":
            give_y(k, c).wait_recv()
        elif kind == "zg":
            pass_on(1, k, z_got, z_in, c, z_peer).wait_recv()
        elif kind == "mg":
            pass_on(1, k, m_got, m_in, c, z_peer).wait_recv()
        elif kind == "pg":
            pass_on(1, k, p_got, p_in, c, z_peer).wait_recv()
        elif kind == "og":
            pass_on(1, 0, o_got, o_in, c, z_peer).wait_recv()
        elif kind == "kvz":
            kv_z(stops[k + 1] * 2 + y, 0, k, z_peer).wait_recv()
        elif kind == "kvy":
            four = kv_all.at[:, 0:4]
            remote(four, four, kvy_sems.at[0], kvy_sems.at[1], y_peer).wait_recv()
        elif kind == "mc":
            mix_core.wait_recv()
        else:
            mix_side.wait_recv()

    row_id = lax.broadcasted_iota(jnp.int32, (tokens_here, tokens_here), 0)
    col_id = lax.broadcasted_iota(jnp.int32, (tokens_here, tokens_here), 1)
    before = (row_id < col_id).astype(jnp.bfloat16)
    after = (col_id < row_id).astype(jnp.bfloat16)

    def tiles(c, body):
        def run(j, carry):
            body(pl.ds(pl.multiple_of(c * part + j * 512, 512), 512))
            return carry

        lax.fori_loop(0, part // 512, run, 0)

    def build(b):
        named = meta[b]
        spread = []
        for expert in (e, y_expert):
            wanted = expert.astype(jnp.float32)
            hit = jnp.logical_or(named[0:1] == wanted, named[1:2] == wanted)
            spread.append(jnp.broadcast_to(hit.astype(jnp.float32)[:, :tokens_here], (cap, tokens_here)))
        spread = jnp.concatenate(spread, axis=0)
        rank = jnp.dot(spread.astype(jnp.bfloat16), before, preferred_element_type=jnp.float32)
        slot = f32(lax.rem(lax.broadcasted_iota(jnp.int32, rank.shape, 0), cap))
        chosen[b] = (jnp.where(rank == slot, 1.0, 0.0) * spread).astype(jnp.bfloat16)
        columns = jnp.transpose(named)[:tokens_here]
        for place, expert in enumerate((e, y_expert)):
            wanted = expert.astype(jnp.float32)
            hits = [(columns[:, k:k + 1] == wanted).astype(jnp.float32) for k in range(2)]
            scale = hits[0] * columns[:, 2:3] + hits[1] * columns[:, 3:4]
            spread = jnp.broadcast_to(hits[0] + hits[1], (tokens_here, cap))
            rank = jnp.dot(after, spread.astype(jnp.bfloat16), preferred_element_type=jnp.float32)
            slot = f32(lax.broadcasted_iota(jnp.int32, rank.shape, 1))
            picks[b, place] = (jnp.where(rank == slot, 1.0, 0.0) * spread).astype(jnp.bfloat16)
            scales[b, place] = jnp.broadcast_to(scale, (tokens_here, 128))

    def select(b, c):
        table = chosen[b]

        def body(span):
            found = jnp.dot(table, dense[b, :, span], preferred_element_type=jnp.float32).astype(jnp.bfloat16)
            rows[b, core, y, :, span] = found[:cap]
            y_send[b, :, span] = found[cap:]

        tiles(c, body)
        row_to_y(b, c).start()
        row_to_c(b, y, c).start()
        if b >= 4:
            row_to_x(b - 4, y, c).start()

    def finish(b, c):
        def body(span):
            value = f32(partial[b, core, :, :, span]) + f32(red[b, :, :, span])
            if b in (4, 5):
                value = value + f32(x_got[b - 4, :, :, span])
            partial[b, core, :, :, span] = value.astype(jnp.bfloat16)

        tiles(c, body)
        if b >= 6:
            reduce_x(b - 6, c).start()
        else:
            give_y(b, c).start()

    def gather(b, c):
        mine, theirs = picks[b, 0], picks[b, 1]
        scale_mine, scale_theirs = scales[b, 0, :, 0:1], scales[b, 1, :, 0:1]

        def body(span):
            first = jnp.dot(mine, partial[b, core, y, :, span], preferred_element_type=jnp.float32)
            second = jnp.dot(theirs, y_got[b, :, span], preferred_element_type=jnp.float32)
            hold[b, :, span] = first * scale_mine + second * scale_theirs

        tiles(c, body)

    def release(b, c, sources, place, where, arrive, device):
        def body(span):
            value = hold[b, :, span]
            for got, at in sources:
                value = value + f32(got[at, :, span])
            sent[b, :, span] = value.astype(jnp.bfloat16)

        tiles(c, body)
        pass_on(b, place, where, arrive, c, device).start()

    def messages(task, is_inner):
        kind = task[0]
        c = task[-1]
        b = task[1] if len(task) > 1 else 0
        if kind in ("F3", "F6", "F5", "F7"):
            return [("d", {"F3": 1, "F6": 4, "F5": 2, "F7": 5}[kind], c)]
        if kind == "sel":
            return [("d", b, c)]
        if kind == "arr":
            return [("ry", b, c)]
        if kind == "arx":
            return [("rx", b, task[2], c)]
        if kind == "cmp":
            return [("rc", b, 0)]
        if kind == "fin":
            return [("red", b, 0)] + ([("xg", b - 4, c)] if b in (4, 5) else [])
        if kind == "gat":
            return [("gy", b, c)]
        if kind == "rel":
            if b == 1:
                return [("pg", 1, c)]
            if is_inner and b in (4, 5):
                return [("zg", b - 4, c)]
            return [("mg", 1, c)] if is_inner and b == 2 else []
        if kind == "final":
            return [("og", c), ("pg", 0, c)] + ([("mg", 0, c)] if is_inner else [])
        if kind == "kvf":
            return [("kvz", b)]
        if kind == "att":
            return [("kvy", 0)]
        return {"mixs": [("mc",)], "mixf": [("mx",)]}.get(kind, [])

    def perform(task, is_inner):
        kind = task[0]
        c = task[-1]
        b = task[1] if len(task) > 1 else 0
        if kind == "D2":
            to_near(c).start()
        elif kind == "F3":
            x_to_near(c).start()
        elif kind == "F6":
            far_to_near(0, c).start()
        elif kind == "F5":
            near_to_across(c).start()
        elif kind == "F7":
            far_to_near(1, c).start()
        elif kind == "meta":
            remote(meta.at[1:6], meta.at[1:6], meta_sems.at[0], meta_sems.at[1], x_peer).wait_recv()

            def run(slot, carry):
                build(slot)
                return carry

            lax.fori_loop(1, 6, run, 0)
        elif kind == "sel":
            select(b, c)
        elif kind == "arr":
            row_to_c(b, other_y, c).start()
            if b >= 4:
                row_to_x(b - 4, other_y, c).start()
        elif kind == "arx":
            row_to_c(6 + b, groups[task[2]], c).start()
        elif kind == "fin":
            finish(b, c)
        elif kind == "gat":
            gather(b, c)
        elif kind == "rel":
            if b == 1:
                release(b, c, [(p_got, 1)], 0, o_got, o_in, x_peer)
            elif b == 2:
                release(b, c, [(m_got, 1)] if is_inner else [], 0, p_got, p_in, z_peer)
            elif b == 3:
                release(b, c, [], 1, p_got, p_in, z_peer)
            elif is_inner:
                release(b, c, [(z_got, b - 4)], b - 4, m_got, m_in, m_peer)
            else:
                release(b, c, [], b - 4, z_got, z_in, z_peer)
        elif kind == "final":
            def body(span):
                value = hold[0, :, span] + f32(o_got[0, :, span]) + f32(p_got[0, :, span])
                if is_inner:
                    value = value + f32(m_got[0, :, span])
                moe[:, span] = value.astype(jnp.bfloat16)

            tiles(c, body)
        elif kind == "kvs":
            kv_sends[0].start()
            if is_inner:
                kv_sends[1].start()
            kv_y(0).start()
        elif kind == "kvf":
            if is_inner:
                kv_sends[2 + b].start()
            kv_y(b + 1).start()
        elif kind == "mixs":
            a_send[...] = (f32(a_part[other_side, core]) + f32(a_red[other_side])).astype(jnp.bfloat16)
            mix_side.start()
        elif kind == "mixf":
            mixed[...] = (f32(a_part[side, core]) + f32(a_red[side]) + f32(a_got[...])).astype(jnp.bfloat16)

    def plan(order, is_inner):
        seen = {("d", 0, c) for c in range(chunks)}
        pieces, kinds = [[]], []
        for task in order:
            fresh = [message for message in messages(task, is_inner) if message not in seen]
            seen.update(fresh)
            pieces[-1].append((fresh, task))
            if task[0] in BIG:
                kinds.append(BIG[task[0]] + (task[1] if len(task) > 1 else 0))
                pieces.append([])
        return pieces, kinds

    def emit(piece, is_inner):
        for fresh, task in piece:
            for message in fresh:
                wait_for(message)
            if task[0] not in BIG:
                perform(task, is_inner)

    for load in loads[:4]:
        load.wait()
    as_float = f32(x_ref[...])
    mean = jnp.mean(as_float * as_float, axis=1, keepdims=True)
    dense[0] = (as_float * lax.rsqrt(mean + NORM_EPS) * x_gain[...]).astype(jnp.bfloat16)
    meta[0] = jnp.zeros(meta.shape[1:], jnp.float32)
    meta[0, 0:2, 0:tokens_here] = f32(routes_row[...])
    meta[0, 2:4, 0:tokens_here] = weight_row[...]

    pl.semaphore_wait(barrier, len(greeted))
    for item in cards:
        item.start()
    for c in range(chunks):
        to_x(c).start()

        @pl.when(inner)
        def _():
            to_across(c).start()

        if c == 0:
            to_near(c).start()
        else:
            @pl.when(outer)
            def _():
                to_near(c).start()

    build(0)
    for c in range(chunks):
        select(0, c)

    for load in loads[4:10]:
        load.wait()
    lane = lax.broadcasted_iota(jnp.int32, (tok, 128), 1)
    low = lane < HEAD_DIM
    even = lax.rem(lax.div(lane, HEAD_DIM // 4), 2) == 0
    table = turn[...]
    swapped = pltpu.roll(table, HEAD_DIM, 1)
    cosine = jnp.where(low, table, swapped)
    sine = jnp.where(low, swapped, table)

    def turned(raw, gain):
        flat = f32(raw)
        square = flat * flat
        left = jnp.sum(jnp.where(low, square, 0.0), axis=1, keepdims=True)
        right = jnp.sum(jnp.where(low, 0.0, square), axis=1, keepdims=True)
        mean_square = jnp.where(low, left, right) * (1.0 / HEAD_DIM)
        unit = flat * lax.rsqrt(mean_square + NORM_EPS) * gain
        partner = jnp.where(
            even, -pltpu.roll(unit, 128 - HEAD_DIM // 4, 1), pltpu.roll(unit, HEAD_DIM // 4, 1)
        )
        return unit * cosine + partner * sine

    for pair in range(kv_all.shape[0] // 2):
        span = slice(pair * 128, (pair + 1) * 128)
        k_rows = turned(k_raw[:, span], k_gain[:, span])
        v_rows = f32(v_raw[:, span])
        kv_all[2 * pair, e] = jnp.where(low, k_rows, pltpu.roll(v_rows, HEAD_DIM, 1)).astype(jnp.bfloat16)
        kv_all[2 * pair + 1, e] = jnp.where(low, pltpu.roll(k_rows, HEAD_DIM, 1), v_rows).astype(jnp.bfloat16)

    for pair in range(pairs):
        span = slice(pair * 128, (pair + 1) * 128)
        q_rows = turned(q_raw[:, span], q_gain[:, span])
        q_ref[2 * pair] = jnp.where(low, q_rows, 0.0).astype(jnp.bfloat16)
        q_ref[2 * pair + 1] = jnp.where(low, pltpu.roll(q_rows, HEAD_DIM, 1), 0.0).astype(jnp.bfloat16)

    for load in loads[10:]:
        load.wait()

    def attend(pair):
        kv = kv_all[lax.div(pair * 2 * kv_all.shape[0], pairs * 2)].reshape(n * tok, 128)
        halves = []
        for h in range(2):
            scores = lax.dot_general(
                q_ref[pair * 2 + h], kv, (((1,), (1,)), ((), ())), preferred_element_type=jnp.float32
            ) * (HEAD_DIM ** (-0.5))
            peak = jnp.max(scores, axis=1, keepdims=True)
            weights = jnp.exp(scores - peak)
            total = jnp.sum(weights, axis=1, keepdims=True)
            summed = jnp.dot(weights.astype(jnp.bfloat16), kv, preferred_element_type=jnp.float32)
            halves.append(summed / total)
        joined = jnp.where(low, pltpu.roll(halves[0], HEAD_DIM, 1), halves[1])
        attended[pair] = joined.astype(jnp.bfloat16)

    inner_pieces, inner_kinds = plan(INNER_ORDER, True)
    outer_pieces, outer_kinds = plan(OUTER_ORDER, False)
    count = len(inner_kinds)

    def step(s, carry):
        u = jnp.where(inner, inner_kinds[0], outer_kinds[0])
        for place in range(1, count):
            u = jnp.where(s == place, jnp.where(inner, inner_kinds[place], outer_kinds[place]), u)
        for place in range(count):
            @pl.when(jnp.logical_and(s == place, inner))
            def _():
                emit(inner_pieces[place], True)

            @pl.when(jnp.logical_and(s == place, outer))
            def _():
                emit(outer_pieces[place], False)

        @pl.when(u < 8)
        def _():
            tokens = rows[u].reshape(4 * cap, width)
            gate = jnp.dot(tokens, wg[...], preferred_element_type=jnp.float32)
            up = jnp.dot(tokens, wu[...], preferred_element_type=jnp.float32)
            hidden = (gate / (1.0 + jnp.exp(-gate)) * up).astype(jnp.bfloat16)
            for tile in range(0, width, TILE):
                product = jnp.dot(hidden, wd[:, tile:tile + TILE], preferred_element_type=jnp.float32)
                partial[u, :, :, :, tile:tile + TILE] = product.astype(jnp.bfloat16).reshape(2, 2, cap, TILE)
                if (tile + TILE) % part == 0:
                    reduce_c(u, tile // part).start()

        @pl.when(jnp.logical_and(u >= 8, u < 10))
        def _():
            attend(2 * (u - 8))
            attend(2 * (u - 8) + 1)

        @pl.when(u == 10)
        def _():
            for tile in range(0, width, TILE):
                product = jnp.dot(attended[0], ow[0, :, tile:tile + TILE], preferred_element_type=jnp.float32)
                for p in range(1, pairs):
                    product += jnp.dot(attended[p], ow[p, :, tile:tile + TILE], preferred_element_type=jnp.float32)
                a_part[:, :, :, tile:tile + TILE] = product.astype(jnp.bfloat16).reshape(2, 2, tok // 4, TILE)
            mix_core.start()

        return carry

    lax.fori_loop(0, count, step, 0)

    @pl.when(inner)
    def _():
        emit(inner_pieces[count], True)

    @pl.when(outer)
    def _():
        emit(outer_pieces[count], False)

    mix_core.wait_send()
    mix_side.wait_send()

    def sent_all(ref, sem):
        remote(ref, ref, sem, meta_sems.at[1], x_peer).wait_send()

    sent_all(kv_all.at[:, 0:4], kvy_sems.at[0])
    kv_sends[0].wait_send()
    sent_all(meta.at[0:5], meta_sems.at[0])
    sent_all(dense.at[0:3], dn_out.at[0])

    @pl.when(inner)
    def _():
        sent_all(kv_all.at[:, 0:4], kvz_out.at[1])
        sent_all(dense.at[0:4], dn_out.at[1])

    sent_all(y_send, outs.at[0])
    sent_all(rows.at[:, core], outs.at[1])
    sent_all(rows.at[4:6, core], outs.at[2])
    sent_all(partial.at[:, other_core], outs.at[3])
    sent_all(partial.at[6:8, core], outs.at[4])
    sent_all(partial.at[0:6, core, other_y], outs.at[5])
    sent_all(sent.at[1:6], outs.at[6])


def turn_table(tokens):
    quarter = HEAD_DIM // 4
    inverse = np.power(ROPE_BASE, -np.arange(quarter, dtype=np.float64) / quarter)
    places = np.arange(tokens)
    row = (places // GRID_W)[:, None] * inverse
    col = (places % GRID_W)[:, None] * inverse
    angles = np.concatenate([row, row, col, col], axis=1)
    return np.concatenate([np.cos(angles), np.sin(angles)], axis=1).astype(np.float32)


def fused(x, x_gain, routes, route_weight, queries, keys, values, q_gain, k_gain, gate_weight, up_weight, down_weight, out_weight):
    n = lax.axis_size("ep")
    tok_exp, width = x.shape
    cap = 2 * routes.shape[1] * tok_exp // n
    tok = queries.shape[0]
    heads = queries.shape[1] // HEAD_DIM
    kv_count = keys.shape[1] // HEAD_DIM
    pairs = heads // 2
    hidden = gate_weight.shape[1]
    bf = jnp.bfloat16
    vmem = pl.BlockSpec(memory_space=pltpu.VMEM)
    anywhere = pl.BlockSpec(memory_space=pl.ANY)
    dma = pltpu.SemaphoreType.DMA
    return pl.pallas_call(
        functools.partial(fused_kernel, n),
        out_shape=(
            pltpu.VMEM((tok_exp, width), bf),
            pltpu.VMEM((tok // 4, width), bf),
        ),
        in_specs=[anywhere] * 14,
        out_specs=(vmem, vmem),
        scratch_shapes=[
            pltpu.VMEM((tok_exp, width), bf),
            pltpu.VMEM((1, width), jnp.float32),
            pltpu.VMEM((routes.shape[1], tok_exp), jnp.int32),
            pltpu.VMEM((routes.shape[1], tok_exp), jnp.float32),
            pltpu.VMEM((tok, heads * HEAD_DIM), bf),
            pltpu.VMEM((tok, kv_count * HEAD_DIM), bf),
            pltpu.VMEM((tok, kv_count * HEAD_DIM), bf),
            pltpu.VMEM((1, heads * HEAD_DIM), jnp.float32),
            pltpu.VMEM((1, kv_count * HEAD_DIM), jnp.float32),
            pltpu.VMEM((6, tok_exp, width), bf),
            pltpu.VMEM((6, 8, 128), jnp.float32),
            pltpu.VMEM((6, 2 * cap, tok_exp), bf),
            pltpu.VMEM((6, 2, tok_exp, cap), bf),
            pltpu.VMEM((6, 2, tok_exp, 128), jnp.float32),
            pltpu.VMEM((8, 2, 2, cap, width), bf),
            pltpu.VMEM((6, cap, width), bf),
            pltpu.VMEM((8, 2, 2, cap, width), bf),
            pltpu.VMEM((8, 2, cap, width), bf),
            pltpu.VMEM((2, 2, cap, width), bf),
            pltpu.VMEM((6, cap, width), bf),
            pltpu.VMEM((6, tok_exp, width), jnp.float32),
            pltpu.VMEM((6, tok_exp, width), bf),
            pltpu.VMEM((2, tok_exp, width), bf),
            pltpu.VMEM((2, tok_exp, width), bf),
            pltpu.VMEM((2, tok_exp, width), bf),
            pltpu.VMEM((1, tok_exp, width), bf),
            pltpu.VMEM((heads, tok, 128), bf),
            pltpu.VMEM((tok, 128), jnp.float32),
            pltpu.VMEM((width, hidden), bf),
            pltpu.VMEM((width, hidden), bf),
            pltpu.VMEM((hidden, width), bf),
            pltpu.VMEM((pairs, 128, width), bf),
            pltpu.VMEM((kv_count, n, tok, 128), bf),
            pltpu.VMEM((pairs, tok, 128), bf),
            pltpu.VMEM((2, 2, tok // 4, width), bf),
            pltpu.VMEM((2, tok // 4, width), bf),
            pltpu.VMEM((tok // 4, width), bf),
            pltpu.VMEM((tok // 4, width), bf),
            dma((14,)),
            dma((2,)),
            dma((3,)),
            dma((2,)),
            dma((2,)),
            dma((5, CHUNKS)),
            dma((2,)),
            dma((6, CHUNKS)),
            dma((8,)),
            dma((2, 2, CHUNKS)),
            dma((8,)),
            dma((2, CHUNKS)),
            dma((6, CHUNKS)),
            dma((7,)),
            dma((2, CHUNKS)),
            dma((2, CHUNKS)),
            dma((2, CHUNKS)),
            dma((1, CHUNKS)),
            dma((2, 2)),
        ],
        compiler_params=pltpu.CompilerParams(
            collective_id=0, has_side_effects=True, vmem_limit_bytes=62 * 1024 * 1024
        ),
    )(
        x,
        x_gain.reshape(1, width),
        jnp.transpose(routes),
        jnp.transpose(route_weight),
        queries,
        keys,
        values,
        q_gain.reshape(1, -1),
        k_gain.reshape(1, -1),
        jnp.asarray(turn_table(n * tok)),
        gate_weight,
        up_weight,
        down_weight,
        out_weight.reshape(pairs, 128, width),
    )


def plain_shards(
    queries,
    keys,
    values,
    query_gain,
    key_gain,
    out_weight,
    expert_input,
    norm_gain,
    routes,
    route_weight,
    gate_weight,
    up_weight,
    down_weight,
):
    tok_mix = queries.shape[0]
    head_count = query_gain.shape[0] // HEAD_DIM
    kv_count = key_gain.shape[0] // HEAD_DIM
    group_size = head_count // kv_count
    offset = lax.axis_index("ep") * tok_mix
    q_turned = head_norm(queries, query_gain, head_count, offset)
    k_turned = head_norm(keys, key_gain, kv_count, offset)
    grouped = q_turned.reshape(tok_mix, kv_count, group_size, HEAD_DIM)
    score_scale = HEAD_DIM ** (-0.5)
    start_state = (
        jnp.full((kv_count, group_size, tok_mix), -jnp.inf, jnp.float32),
        jnp.zeros((kv_count, group_size, tok_mix), jnp.float32),
        jnp.zeros((tok_mix, kv_count, group_size, HEAD_DIM), jnp.float32),
    )
    running = start_state
    key_piece = lax.all_gather(k_turned, "ep", axis=0, tiled=True)
    value_piece = lax.all_gather(values, "ep", axis=0, tiled=True)
    length = key_piece.shape[0]
    block_len = length
    while block_len > 2048 and block_len % 2 == 0:
        block_len = block_len // 2
    key_blocks = key_piece.reshape(length // block_len, block_len, key_piece.shape[1])
    value_blocks = value_piece.reshape(length // block_len, block_len, value_piece.shape[1])

    def advance(inner_state, key_value):
        return (absorb(inner_state, key_value[0], key_value[1], grouped, score_scale), None)

    running, unused = lax.scan(advance, running, (key_blocks, value_blocks))
    final_max, weight_sum, summed = running
    attended = (
        (summed / jnp.transpose(weight_sum, (2, 0, 1))[..., None])
        .reshape(tok_mix, -1)
        .astype(jnp.bfloat16)
    )
    mixed = lax.psum_scatter(
        jnp.dot(attended, out_weight, preferred_element_type=jnp.float32).astype(jnp.bfloat16),
        "tp",
        scatter_dimension=0,
        tiled=True,
    )
    tok_exp = expert_input.shape[0]
    top_count = routes.shape[1]
    expert_count = lax.axis_size("ep")
    capacity = 2 * top_count * tok_exp // expert_count
    as_float = expert_input.astype(jnp.float32)
    normed = (
        as_float
        * lax.rsqrt(jnp.mean(as_float * as_float, axis=-1, keepdims=True) + NORM_EPS)
        * norm_gain
    ).astype(jnp.bfloat16)
    flat_routes = routes.reshape(-1)
    route_hits = (
        flat_routes[:, None] == jnp.arange(expert_count, dtype=jnp.int32)[None, :]
    ).astype(jnp.int32)
    slot_rank = jnp.sum((jnp.cumsum(route_hits, axis=0) - route_hits) * route_hits, axis=1)
    slot_ids = flat_routes * capacity + slot_rank
    placed = jnp.arange(expert_count * capacity, dtype=jnp.int32)[:, None] == slot_ids[None, :]
    placed = jnp.any(placed.reshape(expert_count * capacity, tok_exp, top_count), axis=2).astype(
        jnp.bfloat16
    )
    outbound = jnp.dot(placed, normed, preferred_element_type=jnp.float32).astype(jnp.bfloat16)
    model_width = outbound.shape[1]
    half_cap = capacity // 2
    laid = outbound.reshape(expert_count, capacity, model_width)
    first_half = run_experts(
        laid[:, :half_cap].reshape(expert_count * half_cap, model_width),
        gate_weight,
        up_weight,
        down_weight,
    )
    second_half = run_experts(
        laid[:, half_cap:].reshape(expert_count * half_cap, model_width),
        gate_weight,
        up_weight,
        down_weight,
    )
    back_rows = jnp.concatenate(
        [
            first_half.reshape(expert_count, half_cap, model_width),
            second_half.reshape(expert_count, half_cap, model_width),
        ],
        axis=1,
    )
    back_rows = back_rows.reshape(expert_count * capacity, model_width)
    picked = back_rows[slot_ids.reshape(tok_exp, top_count)]
    moe_out = jnp.sum(picked.astype(jnp.float32) * route_weight[:, :, None], axis=1).astype(
        jnp.bfloat16
    )
    return (mixed, moe_out)


def shards(
    queries,
    keys,
    values,
    query_gain,
    key_gain,
    out_weight,
    expert_input,
    norm_gain,
    routes,
    route_weight,
    gate_weight,
    up_weight,
    down_weight,
):
    tok_exp = expert_input.shape[0]
    top_count = routes.shape[1]
    expert_count = lax.axis_size("ep")
    capacity = 2 * top_count * tok_exp // expert_count
    if capacity % 16 != 0 or lax.axis_size("tp") != 4 or expert_count != 8:
        return plain_shards(
            queries,
            keys,
            values,
            query_gain,
            key_gain,
            out_weight,
            expert_input,
            norm_gain,
            routes,
            route_weight,
            gate_weight,
            up_weight,
            down_weight,
        )
    moe_out, mixed = fused(
        expert_input,
        norm_gain,
        routes,
        route_weight,
        queries,
        keys,
        values,
        query_gain,
        key_gain,
        gate_weight[0],
        up_weight[0],
        down_weight[0],
        out_weight,
    )
    return (mixed, moe_out)


def solution(mesh):
    placed = (
        P("ep", "tp"),
        P("ep", "tp"),
        P("ep", "tp"),
        P("tp"),
        P("tp"),
        P("tp", None),
        P(("ep", "tp"), None),
        P(),
        P(("ep", "tp"), None),
        P(("ep", "tp"), None),
        P("ep", None, "tp"),
        P("ep", None, "tp"),
        P("ep", "tp", None),
    )
    return jax.shard_map(
        shards,
        mesh=mesh,
        in_specs=placed,
        out_specs=(P(("ep", "tp"), None), P(("ep", "tp"), None)),
        check_vma=False,
    )
```

```python
import functools

import jax
import jax.numpy as jnp
import numpy as np
from jax import lax
from jax.experimental import pallas as pl
from jax.experimental.pallas import tpu as pltpu
from jax.sharding import PartitionSpec as P

HEAD_DIM = 64
GRID_W = 128


NORM_EPS = 1e-06
ROPE_BASE = 10000.0


def rotate(vectors, grid_rows, grid_cols):
    quarter = vectors.shape[-1] // 4
    inverse = ROPE_BASE ** (-jnp.arange(quarter, dtype=jnp.float32) / quarter)
    angle_row = grid_rows[:, None] * inverse
    angle_col = grid_cols[:, None] * inverse
    angles = jnp.concatenate([angle_row, angle_row, angle_col, angle_col], axis=-1)[:, None, :]
    part_one, part_two, part_three, part_four = jnp.split(vectors, 4, axis=-1)
    turned = jnp.concatenate([-part_two, part_one, -part_four, part_three], axis=-1)
    return vectors * jnp.cos(angles) + turned * jnp.sin(angles)


def head_norm(raw_rows, gains, head_count, offset):
    row_count = raw_rows.shape[0]
    flat_rows = raw_rows.astype(jnp.float32).reshape(row_count, head_count, -1)
    unit_vec = flat_rows * lax.rsqrt(
        jnp.mean(flat_rows * flat_rows, axis=-1, keepdims=True) + NORM_EPS
    )
    unit_vec = unit_vec * gains.reshape(head_count, -1)
    places = offset + jnp.arange(row_count, dtype=jnp.int32)
    grid_rows = (places // GRID_W).astype(jnp.float32)
    grid_cols = (places % GRID_W).astype(jnp.float32)
    return rotate(unit_vec, grid_rows, grid_cols).astype(jnp.bfloat16).reshape(row_count, -1)


def absorb(running, key_block, value_block, grouped, score_scale):
    run_max, weight_sum, summed = running
    kv_count = grouped.shape[1]
    key_heads = key_block.reshape(key_block.shape[0], kv_count, -1)
    value_heads = value_block.reshape(value_block.shape[0], kv_count, -1)
    scores = (
        jnp.einsum("qhgd,khd->hgqk", grouped, key_heads, preferred_element_type=jnp.float32)
        * score_scale
    )
    new_max = jnp.maximum(run_max, jnp.max(scores, axis=-1))
    rescale = jnp.exp(run_max - new_max)
    weights = jnp.exp(scores - new_max[..., None])
    weight_sum = weight_sum * rescale + jnp.sum(weights, axis=-1)
    update = jnp.einsum(
        "hgqk,khd->qhgd",
        weights.astype(jnp.bfloat16),
        value_heads,
        preferred_element_type=jnp.float32,
    )
    summed = summed * jnp.transpose(rescale, (2, 0, 1))[..., None] + update
    return (new_max, weight_sum, summed)


def run_experts(sending, gate_weight, up_weight, down_weight):
    arrived = lax.all_to_all(sending, "ep", split_axis=0, concat_axis=0, tiled=True)
    shard_rows = lax.all_gather(arrived, "tp", axis=0, tiled=True)
    gate_out = jnp.dot(shard_rows, gate_weight[0], preferred_element_type=jnp.float32)
    up_out = jnp.dot(shard_rows, up_weight[0], preferred_element_type=jnp.float32)
    hidden = (jax.nn.silu(gate_out) * up_out).astype(jnp.bfloat16)
    results = lax.psum_scatter(
        jnp.dot(hidden, down_weight[0], preferred_element_type=jnp.float32).astype(jnp.bfloat16),
        "tp",
        scatter_dimension=0,
        tiled=True,
    )
    return lax.all_to_all(results, "ep", split_axis=0, concat_axis=0, tiled=True)


MESH = pl.DeviceIdType.MESH
TILE = 1024
CHUNKS = 4


def flip(index, pattern, size):
    result = 0
    bit = 1
    while bit < size:
        both = lax.rem(lax.div(index, bit) + lax.div(pattern, bit), 2)
        result = result + both * bit
        bit = bit * 2
    return result


def f32(value):
    return value.astype(jnp.float32)


INNER_ORDER = (
    ("F6", 0), ("meta",), ("arr", 0, 1), ("sel", 1, 0), ("F6", 1), ("sel", 4, 1), ("sel", 2, 0), ("F6", 2),
    ("sel", 4, 0), ("F5", 0), ("sel", 1, 1), ("F6", 3), ("sel", 4, 3), ("arr", 4, 0), ("F5", 2), ("F3", 1),
    ("arr", 0, 2), ("sel", 4, 2), ("arr", 1, 0), ("arx", 0, 0, 0), ("sel", 5, 0), ("F5", 3), ("sel", 1, 3),
    ("arr", 1, 1), ("arr", 4, 3), ("F3", 2), ("sel", 5, 2), ("sel", 1, 2), ("arr", 0, 3), ("kvf", 0),
    ("sel", 2, 1), ("arr", 4, 2), ("arr", 1, 3), ("F7", 2), ("arx", 0, 0, 2), ("F3", 3), ("sel", 3, 0),
    ("F3", 0), ("arx", 0, 0, 1), ("F5", 1), ("F7", 0), ("arr", 2, 0), ("arr", 1, 2), ("F7", 3), ("sel", 3, 1),
    ("arx", 0, 1, 3), ("arr", 4, 1), ("sel", 5, 3), ("sel", 3, 3), ("arx", 1, 0, 0), ("arx", 0, 1, 1),
    ("arx", 0, 1, 0), ("arr", 5, 2), ("arx", 0, 0, 3), ("arx", 0, 1, 2), ("sel", 5, 1), ("arr", 3, 1),
    ("sel", 3, 2), ("cmp", 6), ("sel", 2, 2), ("arr", 5, 3), ("arr", 5, 0), ("arx", 1, 1, 2), ("F7", 1),
    ("cmp", 1), ("kvf", 2), ("arr", 5, 1), ("arr", 3, 3), ("arr", 3, 2), ("arx", 1, 0, 3), ("arx", 1, 0, 2),
    ("kvs",), ("fin", 6, 2), ("arx", 1, 0, 1), ("sel", 2, 3), ("arx", 1, 1, 3), ("arr", 3, 0), ("arr", 2, 1),
    ("cmp", 3), ("fin", 1, 3), ("arr", 0, 0), ("cmp", 4), ("D2", 2), ("arx", 1, 1, 1), ("fin", 1, 1),
    ("fin", 3, 2), ("fin", 6, 3), ("kvf", 1), ("arr", 2, 2), ("arx", 1, 1, 0), ("fin", 3, 3), ("fin", 6, 1),
    ("kvg", 0), ("arr", 2, 3), ("kvp",), ("fin", 4, 2), ("cmp", 7), ("cmp", 0), ("gat", 3, 2), ("fin", 7, 3),
    ("fin", 3, 1), ("fin", 6, 0), ("fin", 3, 0), ("kvg", 1), ("fin", 1, 0), ("cmp", 2), ("kvg", 2),
    ("fin", 4, 3), ("fin", 0, 0), ("gat", 3, 3), ("gat", 4, 2), ("fin", 7, 2), ("fin", 1, 2), ("att", 0),
    ("D2", 1), ("fin", 2, 3), ("fin", 0, 3), ("gat", 1, 0), ("cmp", 5), ("att", 1), ("D2", 3), ("rel", 3, 3),
    ("gat", 1, 2), ("rel", 1, 0), ("gat", 3, 0), ("fin", 2, 0), ("fin", 7, 1), ("gat", 3, 1), ("fin", 5, 2),
    ("gat", 1, 1), ("gat", 0, 0), ("fin", 2, 1), ("gat", 4, 3), ("gat", 1, 3), ("rel", 4, 2), ("fin", 7, 0),
    ("gat", 0, 3), ("gat", 2, 1), ("rel", 4, 3), ("fin", 5, 1), ("rel", 3, 1), ("fin", 4, 0), ("mixp",),
    ("fin", 5, 0), ("rel", 3, 2), ("rel", 1, 2), ("gat", 5, 1), ("fin", 4, 1), ("rel", 3, 0), ("gat", 5, 2),
    ("rel", 5, 1), ("rel", 1, 3), ("rel", 1, 1), ("mixs",), ("fin", 2, 2), ("fin", 5, 3), ("gat", 5, 0),
    ("rel", 5, 0), ("fin", 0, 1), ("gat", 4, 0), ("rel", 2, 1), ("rel", 5, 2), ("gat", 4, 1), ("gat", 2, 0),
    ("rel", 2, 0), ("gat", 5, 3), ("rel", 5, 3), ("fin", 0, 2), ("gat", 2, 2), ("rel", 2, 2), ("rel", 4, 0),
    ("gat", 0, 2), ("gat", 2, 3), ("rel", 4, 1), ("rel", 2, 3), ("gat", 0, 1), ("mixf",), ("final", 0),
    ("final", 2), ("final", 1), ("final", 3),
)
OUTER_ORDER = (
    ("kvs",), ("arr", 0, 0), ("arr", 0, 1), ("meta",), ("F3", 0), ("sel", 1, 1), ("F3", 1), ("sel", 1, 0),
    ("F3", 2), ("sel", 4, 0), ("sel", 4, 1), ("arr", 0, 3), ("arx", 0, 0, 0), ("arr", 4, 0), ("arr", 4, 1),
    ("arx", 0, 0, 1), ("sel", 4, 2), ("arx", 0, 1, 0), ("sel", 4, 3), ("F3", 3), ("arr", 4, 2), ("arr", 4, 3),
    ("arx", 0, 0, 2), ("sel", 1, 2), ("arx", 0, 0, 3), ("arx", 0, 1, 2), ("arr", 1, 0), ("arx", 0, 1, 1),
    ("sel", 3, 2), ("arx", 0, 1, 3), ("sel", 2, 0), ("sel", 3, 1), ("sel", 1, 3), ("cmp", 6), ("arr", 3, 2),
    ("arr", 0, 2), ("sel", 5, 2), ("fin", 6, 1), ("cmp", 4), ("fin", 6, 2), ("arx", 1, 0, 2), ("arr", 1, 1),
    ("kvp",), ("sel", 3, 3), ("sel", 3, 0), ("cmp", 0), ("fin", 4, 1), ("sel", 5, 0), ("arr", 3, 3),
    ("arr", 1, 2), ("arr", 3, 1), ("arr", 3, 0), ("fin", 4, 2), ("arr", 5, 2), ("sel", 5, 3), ("cmp", 3),
    ("gat", 4, 1), ("arr", 5, 0), ("arr", 2, 0), ("arr", 1, 3), ("rel", 4, 1), ("sel", 5, 1), ("arr", 5, 3),
    ("fin", 3, 0), ("arx", 1, 0, 3), ("arx", 1, 1, 2), ("gat", 4, 2), ("fin", 3, 3), ("rel", 4, 2),
    ("cmp", 1), ("arr", 5, 1), ("arx", 1, 0, 1), ("fin", 3, 1), ("fin", 6, 3), ("fin", 6, 0), ("fin", 3, 2),
    ("gat", 3, 0), ("rel", 3, 0), ("arx", 1, 1, 0), ("arx", 1, 1, 3), ("kvf", 0), ("arx", 1, 0, 0),
    ("arx", 1, 1, 1), ("gat", 3, 3), ("gat", 3, 1), ("rel", 3, 1), ("rel", 3, 3), ("fin", 1, 1), ("cmp", 7),
    ("fin", 4, 3), ("cmp", 5), ("fin", 7, 1), ("gat", 3, 2), ("fin", 4, 0), ("fin", 1, 3), ("rel", 3, 2),
    ("fin", 7, 0), ("sel", 2, 2), ("att", 0), ("gat", 4, 3), ("gat", 4, 0), ("rel", 4, 3), ("fin", 7, 2),
    ("sel", 2, 1), ("rel", 4, 0), ("fin", 7, 3), ("fin", 5, 1), ("att", 1), ("fin", 5, 0), ("sel", 2, 3),
    ("arr", 2, 2), ("fin", 1, 2), ("mixp",), ("gat", 5, 1), ("rel", 5, 1), ("fin", 5, 2), ("gat", 1, 3),
    ("rel", 1, 3), ("mixs",), ("gat", 5, 0), ("arr", 2, 3), ("rel", 5, 0), ("arr", 2, 1), ("fin", 5, 3),
    ("cmp", 2), ("fin", 1, 0), ("gat", 5, 2), ("rel", 5, 2), ("fin", 2, 2), ("fin", 2, 0), ("gat", 1, 1),
    ("gat", 1, 2), ("fin", 2, 1), ("fin", 0, 0), ("gat", 5, 3), ("fin", 0, 2), ("rel", 5, 3), ("fin", 0, 1),
    ("fin", 2, 3), ("rel", 1, 1), ("gat", 2, 2), ("rel", 2, 2), ("gat", 2, 1), ("gat", 1, 0), ("rel", 1, 0),
    ("rel", 2, 1), ("fin", 0, 3), ("gat", 2, 0), ("rel", 1, 2), ("rel", 2, 0), ("gat", 0, 2), ("gat", 0, 0),
    ("gat", 2, 3), ("rel", 2, 3), ("gat", 0, 3), ("gat", 0, 1), ("mixf",), ("final", 0), ("final", 3),
    ("final", 1), ("final", 2),
)


BIG = {"cmp": 0, "att": 8, "mixp": 10}


def fused_kernel(
    n,
    x_hbm,
    x_gain_hbm,
    routes_hbm,
    weight_hbm,
    q_hbm,
    k_hbm,
    v_hbm,
    q_gain_hbm,
    k_gain_hbm,
    turn_hbm,
    wg_hbm,
    wu_hbm,
    wd_hbm,
    ow_hbm,
    moe,
    mixed,
    x_ref,
    x_gain,
    routes_row,
    weight_row,
    q_raw,
    k_raw,
    v_raw,
    q_gain,
    k_gain,
    dense,
    meta,
    chosen,
    picks,
    scales,
    rows,
    y_send,
    partial,
    red,
    x_got,
    y_got,
    hold,
    sent,
    z_got,
    m_got,
    p_got,
    o_got,
    q_ref,
    turn,
    wg,
    wu,
    wd,
    ow,
    kv_all,
    attended,
    a_part,
    a_red,
    a_send,
    a_got,
    load_sem,
    kvz_out,
    kvz_in,
    kvy_sems,
    dn_out,
    dn_in,
    meta_sems,
    row_y,
    row_c,
    row_x,
    red_in,
    sum_x,
    sum_y,
    outs,
    z_in,
    m_in,
    p_in,
    o_in,
    mix_sems,
):
    e = lax.axis_index("ep")
    t = lax.axis_index("tp")
    side = lax.div(t, 2)
    core = lax.rem(t, 2)
    other_side = 1 - side
    other_core = 1 - core
    layer = lax.div(e, 2)
    y = lax.rem(e, 2)
    other_y = 1 - y
    near = layer + 1 - 2 * lax.rem(layer, 2)
    last = n // 2 - 1
    across = last - layer
    inner = jnp.logical_and(layer > 0, layer < last)
    outer = jnp.logical_not(inner)
    half = lax.div(layer, 2)
    far_inner = 2 - half
    far_outer = last * (1 - half)
    x_tp = other_side * 2 + core
    x_peer = (e, x_tp)
    c_peer = (e, side * 2 + other_core)
    y_expert = layer * 2 + other_y
    y_peer = (y_expert, t)
    z_peer = (near * 2 + y, t)
    m_peer = (across * 2 + y, t)
    corner = (near * 2 + y, x_tp)
    cap, width = rows.shape[3], rows.shape[4]
    pairs = attended.shape[0]
    tok = attended.shape[1]
    tokens_here = x_ref.shape[0]
    chunks = dn_in.shape[1]
    part = width // chunks
    groups = (y, other_y)

    def remote(src, dst, send, recv, device):
        return pltpu.make_async_remote_copy(
            src_ref=src, dst_ref=dst, send_sem=send, recv_sem=recv, device_id=device, device_id_type=MESH
        )

    def cols(c):
        return pl.ds(c * part, part)

    far_peers = [(far_inner * 2 + y, t), (far_outer * 2 + y, t)]
    barrier = pltpu.get_barrier_semaphore()
    greeted = [x_peer, c_peer, y_peer, z_peer, corner] + far_peers
    for peer in greeted:
        pl.semaphore_signal(barrier, inc=1, device_id=peer, device_id_type=MESH)

    loads = [
        pltpu.make_async_copy(a, b, load_sem.at[k])
        for k, (a, b) in enumerate(
            [
                (x_hbm, x_ref),
                (x_gain_hbm, x_gain),
                (routes_hbm, routes_row),
                (weight_hbm, weight_row),
                (turn_hbm.at[pl.ds(pl.multiple_of(e * tok, 8), tok)], turn),
                (k_hbm, k_raw),
                (v_hbm, v_raw),
                (k_gain_hbm, k_gain),
                (q_hbm, q_raw),
                (q_gain_hbm, q_gain),
                (wg_hbm, wg),
                (wu_hbm, wu),
                (wd_hbm, wd),
                (ow_hbm, ow),
            ]
        )
    ]
    for load in loads:
        load.start()

    stops = [layer, near, far_inner, far_outer]

    def kv_move(owner, out, arrive, device):
        return remote(kv_all.at[:, owner], kv_all.at[:, owner], out, arrive, device)

    def kv_hop(stop, column, place, device):
        first = 0 if stop == 0 and column == 0 and place == 0 else 1
        return kv_move(stops[stop] * 2 + (y, other_y)[column], kvz_out.at[first], kvz_in.at[column, place], device)

    def kv_y(j):
        return kv_move(stops[j] * 2 + y, kvy_sems.at[0, 0], kvy_sems.at[1, j], y_peer)

    def block(source, target, number, c, device):
        return remote(
            dense.at[source, :, cols(c)],
            dense.at[target, :, cols(c)],
            dn_out.at[number // 4],
            dn_in.at[target - 1, c],
            device,
        )

    def to_x(c):
        return block(0, 1, 1, c, x_peer)

    def to_near(c):
        return block(0, 2, 2, c, z_peer)

    def x_to_near(c):
        return block(1, 3, 3, c, z_peer)

    def to_across(c):
        return block(0, 4, 4, c, m_peer)

    def near_to_across(c):
        return block(2, 5, 5, c, m_peer)

    def far_to_near(k, c):
        return block(4 + k, 4 + k, 6 + k, c, z_peer)

    far_slot = jnp.where(inner, 4, 5)

    def card(slot, number, device):
        return remote(meta.at[0], meta.at[slot], meta_sems.at[0], meta_sems.at[1], device)

    cards = [
        card(1, 1, x_peer),
        card(2, 2, z_peer),
        card(3, 3, corner),
        card(far_slot, 4, far_peers[0]),
        card(far_slot, 5, far_peers[1]),
    ]

    def row_to_y(b, c):
        return remote(
            y_send.at[b, :, cols(c)], rows.at[b, core, y, :, cols(c)], outs.at[0], row_y.at[b, c], y_peer
        )

    def row_to_c(b, g, c):
        here = rows.at[b, core, g, :, cols(c)]
        return remote(here, here, outs.at[1], row_c.at[b], c_peer)

    def row_to_x(k, g, c):
        return remote(
            rows.at[4 + k, core, g, :, cols(c)],
            rows.at[6 + k, core, g, :, cols(c)],
            outs.at[2],
            row_x.at[k, g, c],
            x_peer,
        )

    def reduce_c(b, c):
        return remote(
            partial.at[b, other_core, :, :, cols(c)],
            red.at[b, :, :, cols(c)],
            outs.at[3],
            red_in.at[b],
            c_peer,
        )

    def reduce_x(k, c):
        return remote(
            partial.at[6 + k, core, :, :, cols(c)],
            x_got.at[k, :, :, cols(c)],
            outs.at[4],
            sum_x.at[k, c],
            x_peer,
        )

    def give_y(b, c):
        return remote(
            partial.at[b, core, other_y, :, cols(c)],
            y_got.at[b, :, cols(c)],
            outs.at[5],
            sum_y.at[b, c],
            y_peer,
        )

    def pass_on(b, place, where, arrive, c, device):
        return remote(sent.at[b, :, cols(c)], where.at[place, :, cols(c)], outs.at[6], arrive.at[place, c], device)

    mix_core = remote(a_part.at[:, other_core], a_red, mix_sems.at[0, 0], mix_sems.at[1, 0], c_peer)
    mix_side = remote(a_send, a_got, mix_sems.at[0, 1], mix_sems.at[1, 1], x_peer)

    def wait_for(message):
        kind = message[0]
        c = message[-1]
        k = message[1] if len(message) > 1 else 0
        if kind == "d":
            block(k, k, 0, c, x_peer).wait_recv()
        elif kind == "ry":
            remote(
                y_send.at[k, :, cols(c)],
                rows.at[k, core, other_y, :, cols(c)],
                outs.at[0],
                row_y.at[k, c],
                y_peer,
            ).wait_recv()
        elif kind == "rc":
            there = rows.at[k, other_core]
            remote(there, there, outs.at[1], row_c.at[k], c_peer).wait_recv()
        elif kind == "rx":
            row_to_x(k, groups[message[2]], c).wait_recv()
        elif kind == "red":
            remote(red.at[k], red.at[k], outs.at[3], red_in.at[k], c_peer).wait_recv()
        elif kind == "xg":
            reduce_x(k, c).wait_recv()
        elif kind == "gy":
            give_y(k, c).wait_recv()
        elif kind == "zg":
            pass_on(1, k, z_got, z_in, c, z_peer).wait_recv()
        elif kind == "mg":
            pass_on(1, k, m_got, m_in, c, z_peer).wait_recv()
        elif kind == "pg":
            pass_on(1, k, p_got, p_in, c, z_peer).wait_recv()
        elif kind == "og":
            pass_on(1, 0, o_got, o_in, c, z_peer).wait_recv()
        elif kind == "kvz":
            kv_hop(k + 1, 0, k, z_peer).wait_recv()
        elif kind == "kvw":
            kv_hop(k + 1, 1, k, z_peer).wait_recv()
        elif kind == "kvy":
            kv_move(stops[k] * 2 + other_y, kvy_sems.at[0, 0], kvy_sems.at[1, k], y_peer).wait_recv()
        elif kind == "mc":
            mix_core.wait_recv()
        else:
            mix_side.wait_recv()

    row_id = lax.broadcasted_iota(jnp.int32, (tokens_here, tokens_here), 0)
    col_id = lax.broadcasted_iota(jnp.int32, (tokens_here, tokens_here), 1)
    before = (row_id < col_id).astype(jnp.bfloat16)
    after = (col_id < row_id).astype(jnp.bfloat16)

    def tiles(c, body):
        def run(j, carry):
            body(pl.ds(pl.multiple_of(c * part + j * 512, 512), 512))
            return carry

        lax.fori_loop(0, part // 512, run, 0)

    def build(b):
        named = meta[b]
        spread = []
        for expert in (e, y_expert):
            wanted = expert.astype(jnp.float32)
            hit = jnp.logical_or(named[0:1] == wanted, named[1:2] == wanted)
            spread.append(jnp.broadcast_to(hit.astype(jnp.float32)[:, :tokens_here], (cap, tokens_here)))
        spread = jnp.concatenate(spread, axis=0)
        rank = jnp.dot(spread.astype(jnp.bfloat16), before, preferred_element_type=jnp.float32)
        slot = f32(lax.rem(lax.broadcasted_iota(jnp.int32, rank.shape, 0), cap))
        chosen[b] = (jnp.where(rank == slot, 1.0, 0.0) * spread).astype(jnp.bfloat16)
        columns = jnp.transpose(named)[:tokens_here]
        for place, expert in enumerate((e, y_expert)):
            wanted = expert.astype(jnp.float32)
            hits = [(columns[:, k:k + 1] == wanted).astype(jnp.float32) for k in range(2)]
            scale = hits[0] * columns[:, 2:3] + hits[1] * columns[:, 3:4]
            spread = jnp.broadcast_to(hits[0] + hits[1], (tokens_here, cap))
            rank = jnp.dot(after, spread.astype(jnp.bfloat16), preferred_element_type=jnp.float32)
            slot = f32(lax.broadcasted_iota(jnp.int32, rank.shape, 1))
            picks[b, place] = (jnp.where(rank == slot, 1.0, 0.0) * spread).astype(jnp.bfloat16)
            scales[b, place] = jnp.broadcast_to(scale, (tokens_here, 128))

    def select(b, c):
        table = chosen[b]

        def body(span):
            found = jnp.dot(table, dense[b, :, span], preferred_element_type=jnp.float32).astype(jnp.bfloat16)
            rows[b, core, y, :, span] = found[:cap]
            y_send[b, :, span] = found[cap:]

        tiles(c, body)
        row_to_y(b, c).start()
        row_to_c(b, y, c).start()
        if b >= 4:
            row_to_x(b - 4, y, c).start()

    def finish(b, c):
        def body(span):
            value = f32(partial[b, core, :, :, span]) + f32(red[b, :, :, span])
            if b in (4, 5):
                value = value + f32(x_got[b - 4, :, :, span])
            partial[b, core, :, :, span] = value.astype(jnp.bfloat16)

        tiles(c, body)
        if b >= 6:
            reduce_x(b - 6, c).start()
        else:
            give_y(b, c).start()

    def gather(b, c):
        mine, theirs = picks[b, 0], picks[b, 1]
        scale_mine, scale_theirs = scales[b, 0, :, 0:1], scales[b, 1, :, 0:1]

        def body(span):
            first = jnp.dot(mine, partial[b, core, y, :, span], preferred_element_type=jnp.float32)
            second = jnp.dot(theirs, y_got[b, :, span], preferred_element_type=jnp.float32)
            hold[b, :, span] = first * scale_mine + second * scale_theirs

        tiles(c, body)

    def release(b, c, sources, place, where, arrive, device):
        def body(span):
            value = hold[b, :, span]
            for got, at in sources:
                value = value + f32(got[at, :, span])
            sent[b, :, span] = value.astype(jnp.bfloat16)

        tiles(c, body)
        pass_on(b, place, where, arrive, c, device).start()

    def messages(task, is_inner):
        kind = task[0]
        c = task[-1]
        b = task[1] if len(task) > 1 else 0
        if kind in ("F3", "F6", "F5", "F7"):
            return [("d", {"F3": 1, "F6": 4, "F5": 2, "F7": 5}[kind], c)]
        if kind == "sel":
            return [("d", b, c)]
        if kind == "arr":
            return [("ry", b, c)]
        if kind == "arx":
            return [("rx", b, task[2], c)]
        if kind == "cmp":
            return [("rc", b, 0)]
        if kind == "fin":
            return [("red", b, 0)] + ([("xg", b - 4, c)] if b in (4, 5) else [])
        if kind == "gat":
            return [("gy", b, c)]
        if kind == "rel":
            if b == 1:
                return [("pg", 1, c)]
            if is_inner and b in (4, 5):
                return [("zg", b - 4, c)]
            return [("mg", 1, c)] if is_inner and b == 2 else []
        if kind == "final":
            return [("og", c), ("pg", 0, c)] + ([("mg", 0, c)] if is_inner else [])
        if kind == "kvf":
            return [("kvz", b)]
        if kind == "kvp":
            return [("kvy", 0)]
        if kind == "kvg":
            return [("kvw", b)]
        if kind == "att":
            return [] if is_inner else [("kvz", 1), ("kvz", 2), ("kvw", 1), ("kvw", 2), ("kvy", 1)]
        return {"mixs": [("mc",)], "mixf": [("mx",)]}.get(kind, [])

    def perform(task, is_inner):
        kind = task[0]
        c = task[-1]
        b = task[1] if len(task) > 1 else 0
        if kind == "D2":
            to_near(c).start()
        elif kind == "F3":
            x_to_near(c).start()
        elif kind == "F6":
            far_to_near(0, c).start()
        elif kind == "F5":
            near_to_across(c).start()
        elif kind == "F7":
            far_to_near(1, c).start()
        elif kind == "meta":
            remote(meta.at[1:6], meta.at[1:6], meta_sems.at[0], meta_sems.at[1], x_peer).wait_recv()

            def run(slot, carry):
                build(slot)
                return carry

            lax.fori_loop(1, 6, run, 0)
        elif kind == "sel":
            select(b, c)
        elif kind == "arr":
            row_to_c(b, other_y, c).start()
            if b >= 4:
                row_to_x(b - 4, other_y, c).start()
        elif kind == "arx":
            row_to_c(6 + b, groups[task[2]], c).start()
        elif kind == "fin":
            finish(b, c)
        elif kind == "gat":
            gather(b, c)
        elif kind == "rel":
            if b == 1:
                release(b, c, [(p_got, 1)], 0, o_got, o_in, x_peer)
            elif b == 2:
                release(b, c, [(m_got, 1)] if is_inner else [], 0, p_got, p_in, z_peer)
            elif b == 3:
                release(b, c, [], 1, p_got, p_in, z_peer)
            elif is_inner:
                release(b, c, [(z_got, b - 4)], b - 4, m_got, m_in, m_peer)
            else:
                release(b, c, [], b - 4, z_got, z_in, z_peer)
        elif kind == "final":
            def body(span):
                value = hold[0, :, span] + f32(o_got[0, :, span]) + f32(p_got[0, :, span])
                if is_inner:
                    value = value + f32(m_got[0, :, span])
                moe[:, span] = value.astype(jnp.bfloat16)

            tiles(c, body)
        elif kind == "kvs":
            kv_hop(0, 0, 0, z_peer).start()
            if is_inner:
                kv_hop(0, 0, 1, m_peer).start()
            kv_y(0).start()
        elif kind == "kvp":
            if is_inner:
                kv_hop(0, 1, 1, m_peer).start()
            else:
                kv_hop(0, 1, 0, z_peer).start()
        elif kind in ("kvf", "kvg"):
            column = int(kind == "kvg")
            if not is_inner:
                kv_y(1).start()
            elif b == 0:
                kv_hop(1, column, 2, m_peer).start()
            else:
                kv_hop(1 + b, column, b, z_peer).start()
        elif kind == "mixs":
            a_send[...] = (f32(a_part[other_side, core]) + f32(a_red[other_side])).astype(jnp.bfloat16)
            mix_side.start()
        elif kind == "mixf":
            mixed[...] = (f32(a_part[side, core]) + f32(a_red[side]) + f32(a_got[...])).astype(jnp.bfloat16)

    def plan(order, is_inner):
        seen = {("d", 0, c) for c in range(chunks)}
        pieces, kinds = [[]], []
        for task in order:
            fresh = [message for message in messages(task, is_inner) if message not in seen]
            seen.update(fresh)
            pieces[-1].append((fresh, task))
            if task[0] in BIG:
                kinds.append(BIG[task[0]] + (task[1] if len(task) > 1 else 0))
                pieces.append([])
        return pieces, kinds

    def emit(piece, is_inner):
        for fresh, task in piece:
            for message in fresh:
                wait_for(message)
            if task[0] not in BIG:
                perform(task, is_inner)

    for load in loads[:4]:
        load.wait()
    as_float = f32(x_ref[...])
    mean = jnp.mean(as_float * as_float, axis=1, keepdims=True)
    dense[0] = (as_float * lax.rsqrt(mean + NORM_EPS) * x_gain[...]).astype(jnp.bfloat16)
    meta[0] = jnp.zeros(meta.shape[1:], jnp.float32)
    meta[0, 0:2, 0:tokens_here] = f32(routes_row[...])
    meta[0, 2:4, 0:tokens_here] = weight_row[...]

    pl.semaphore_wait(barrier, len(greeted))
    for item in cards:
        item.start()
    for c in range(chunks):
        to_x(c).start()

        @pl.when(inner)
        def _():
            to_across(c).start()

        if c == 0:
            to_near(c).start()
        else:
            @pl.when(outer)
            def _():
                to_near(c).start()

    build(0)
    for c in range(chunks):
        select(0, c)

    for load in loads[4:10]:
        load.wait()
    lane = lax.broadcasted_iota(jnp.int32, (tok, 128), 1)
    low = lane < HEAD_DIM
    even = lax.rem(lax.div(lane, HEAD_DIM // 4), 2) == 0
    table = turn[...]
    swapped = pltpu.roll(table, HEAD_DIM, 1)
    cosine = jnp.where(low, table, swapped)
    sine = jnp.where(low, swapped, table)

    def turned(raw, gain):
        flat = f32(raw)
        square = flat * flat
        left = jnp.sum(jnp.where(low, square, 0.0), axis=1, keepdims=True)
        right = jnp.sum(jnp.where(low, 0.0, square), axis=1, keepdims=True)
        mean_square = jnp.where(low, left, right) * (1.0 / HEAD_DIM)
        unit = flat * lax.rsqrt(mean_square + NORM_EPS) * gain
        partner = jnp.where(
            even, -pltpu.roll(unit, 128 - HEAD_DIM // 4, 1), pltpu.roll(unit, HEAD_DIM // 4, 1)
        )
        return unit * cosine + partner * sine

    for pair in range(kv_all.shape[0] // 2):
        span = slice(pair * 128, (pair + 1) * 128)
        k_rows = turned(k_raw[:, span], k_gain[:, span])
        v_rows = f32(v_raw[:, span])
        kv_all[2 * pair, e] = jnp.where(low, k_rows, pltpu.roll(v_rows, HEAD_DIM, 1)).astype(jnp.bfloat16)
        kv_all[2 * pair + 1, e] = jnp.where(low, pltpu.roll(k_rows, HEAD_DIM, 1), v_rows).astype(jnp.bfloat16)

    for pair in range(pairs):
        span = slice(pair * 128, (pair + 1) * 128)
        q_rows = turned(q_raw[:, span], q_gain[:, span])
        q_ref[2 * pair] = jnp.where(low, q_rows, 0.0).astype(jnp.bfloat16)
        q_ref[2 * pair + 1] = jnp.where(low, pltpu.roll(q_rows, HEAD_DIM, 1), 0.0).astype(jnp.bfloat16)

    for load in loads[10:]:
        load.wait()

    def attend(pair):
        kv = kv_all[lax.div(pair * 2 * kv_all.shape[0], pairs * 2)].reshape(n * tok, 128)
        halves = []
        for h in range(2):
            scores = lax.dot_general(
                q_ref[pair * 2 + h], kv, (((1,), (1,)), ((), ())), preferred_element_type=jnp.float32
            ) * (HEAD_DIM ** (-0.5))
            peak = jnp.max(scores, axis=1, keepdims=True)
            weights = jnp.exp(scores - peak)
            total = jnp.sum(weights, axis=1, keepdims=True)
            summed = jnp.dot(weights.astype(jnp.bfloat16), kv, preferred_element_type=jnp.float32)
            halves.append(summed / total)
        joined = jnp.where(low, pltpu.roll(halves[0], HEAD_DIM, 1), halves[1])
        attended[pair] = joined.astype(jnp.bfloat16)

    inner_pieces, inner_kinds = plan(INNER_ORDER, True)
    outer_pieces, outer_kinds = plan(OUTER_ORDER, False)
    count = len(inner_kinds)

    def step(s, carry):
        u = jnp.where(inner, inner_kinds[0], outer_kinds[0])
        for place in range(1, count):
            u = jnp.where(s == place, jnp.where(inner, inner_kinds[place], outer_kinds[place]), u)
        for place in range(count):
            @pl.when(jnp.logical_and(s == place, inner))
            def _():
                emit(inner_pieces[place], True)

            @pl.when(jnp.logical_and(s == place, outer))
            def _():
                emit(outer_pieces[place], False)

        @pl.when(u < 8)
        def _():
            tokens = rows[u].reshape(4 * cap, width)
            gate = jnp.dot(tokens, wg[...], preferred_element_type=jnp.float32)
            up = jnp.dot(tokens, wu[...], preferred_element_type=jnp.float32)
            hidden = (gate / (1.0 + jnp.exp(-gate)) * up).astype(jnp.bfloat16)
            for tile in range(0, width, TILE):
                product = jnp.dot(hidden, wd[:, tile:tile + TILE], preferred_element_type=jnp.float32)
                partial[u, :, :, :, tile:tile + TILE] = product.astype(jnp.bfloat16).reshape(2, 2, cap, TILE)
                if (tile + TILE) % part == 0:
                    reduce_c(u, tile // part).start()

        @pl.when(jnp.logical_and(u >= 8, u < 10))
        def _():
            attend(2 * (u - 8))
            attend(2 * (u - 8) + 1)

        @pl.when(u == 10)
        def _():
            for tile in range(0, width, TILE):
                product = jnp.dot(attended[0], ow[0, :, tile:tile + TILE], preferred_element_type=jnp.float32)
                for p in range(1, pairs):
                    product += jnp.dot(attended[p], ow[p, :, tile:tile + TILE], preferred_element_type=jnp.float32)
                a_part[:, :, :, tile:tile + TILE] = product.astype(jnp.bfloat16).reshape(2, 2, tok // 4, TILE)
            mix_core.start()

        return carry

    lax.fori_loop(0, count, step, 0)

    @pl.when(inner)
    def _():
        emit(inner_pieces[count], True)

    @pl.when(outer)
    def _():
        emit(outer_pieces[count], False)

    mix_core.wait_send()
    mix_side.wait_send()

    def sent_all(ref, sem):
        remote(ref, ref, sem, meta_sems.at[1], x_peer).wait_send()

    sent_all(kv_all.at[:, 0], kvz_out.at[0])
    sent_all(meta.at[0:5], meta_sems.at[0])
    sent_all(dense.at[0:3], dn_out.at[0])

    @pl.when(inner)
    def _():
        sent_all(kv_all.at[:, 0], kvy_sems.at[0, 0])
        sent_all(kv_all, kvz_out.at[1])
        sent_all(dense.at[0:4], dn_out.at[1])

    @pl.when(outer)
    def _():
        sent_all(kv_all.at[:, 0:2], kvy_sems.at[0, 0])
        sent_all(kv_all.at[:, 0], kvz_out.at[1])

    sent_all(y_send, outs.at[0])
    sent_all(rows.at[:, core], outs.at[1])
    sent_all(rows.at[4:6, core], outs.at[2])
    sent_all(partial.at[:, other_core], outs.at[3])
    sent_all(partial.at[6:8, core], outs.at[4])
    sent_all(partial.at[0:6, core, other_y], outs.at[5])
    sent_all(sent.at[1:6], outs.at[6])


def turn_table(tokens):
    quarter = HEAD_DIM // 4
    inverse = np.power(ROPE_BASE, -np.arange(quarter, dtype=np.float64) / quarter)
    places = np.arange(tokens)
    row = (places // GRID_W)[:, None] * inverse
    col = (places % GRID_W)[:, None] * inverse
    angles = np.concatenate([row, row, col, col], axis=1)
    return np.concatenate([np.cos(angles), np.sin(angles)], axis=1).astype(np.float32)


def fused(x, x_gain, routes, route_weight, queries, keys, values, q_gain, k_gain, gate_weight, up_weight, down_weight, out_weight):
    n = lax.axis_size("ep")
    tok_exp, width = x.shape
    cap = 2 * routes.shape[1] * tok_exp // n
    tok = queries.shape[0]
    heads = queries.shape[1] // HEAD_DIM
    kv_count = keys.shape[1] // HEAD_DIM
    pairs = heads // 2
    hidden = gate_weight.shape[1]
    bf = jnp.bfloat16
    vmem = pl.BlockSpec(memory_space=pltpu.VMEM)
    anywhere = pl.BlockSpec(memory_space=pl.ANY)
    dma = pltpu.SemaphoreType.DMA
    return pl.pallas_call(
        functools.partial(fused_kernel, n),
        out_shape=(
            pltpu.VMEM((tok_exp, width), bf),
            pltpu.VMEM((tok // 4, width), bf),
        ),
        in_specs=[anywhere] * 14,
        out_specs=(vmem, vmem),
        scratch_shapes=[
            pltpu.VMEM((tok_exp, width), bf),
            pltpu.VMEM((1, width), jnp.float32),
            pltpu.VMEM((routes.shape[1], tok_exp), jnp.int32),
            pltpu.VMEM((routes.shape[1], tok_exp), jnp.float32),
            pltpu.VMEM((tok, heads * HEAD_DIM), bf),
            pltpu.VMEM((tok, kv_count * HEAD_DIM), bf),
            pltpu.VMEM((tok, kv_count * HEAD_DIM), bf),
            pltpu.VMEM((1, heads * HEAD_DIM), jnp.float32),
            pltpu.VMEM((1, kv_count * HEAD_DIM), jnp.float32),
            pltpu.VMEM((6, tok_exp, width), bf),
            pltpu.VMEM((6, 8, 128), jnp.float32),
            pltpu.VMEM((6, 2 * cap, tok_exp), bf),
            pltpu.VMEM((6, 2, tok_exp, cap), bf),
            pltpu.VMEM((6, 2, tok_exp, 128), jnp.float32),
            pltpu.VMEM((8, 2, 2, cap, width), bf),
            pltpu.VMEM((6, cap, width), bf),
            pltpu.VMEM((8, 2, 2, cap, width), bf),
            pltpu.VMEM((8, 2, cap, width), bf),
            pltpu.VMEM((2, 2, cap, width), bf),
            pltpu.VMEM((6, cap, width), bf),
            pltpu.VMEM((6, tok_exp, width), jnp.float32),
            pltpu.VMEM((6, tok_exp, width), bf),
            pltpu.VMEM((2, tok_exp, width), bf),
            pltpu.VMEM((2, tok_exp, width), bf),
            pltpu.VMEM((2, tok_exp, width), bf),
            pltpu.VMEM((1, tok_exp, width), bf),
            pltpu.VMEM((heads, tok, 128), bf),
            pltpu.VMEM((tok, 128), jnp.float32),
            pltpu.VMEM((width, hidden), bf),
            pltpu.VMEM((width, hidden), bf),
            pltpu.VMEM((hidden, width), bf),
            pltpu.VMEM((pairs, 128, width), bf),
            pltpu.VMEM((kv_count, n, tok, 128), bf),
            pltpu.VMEM((pairs, tok, 128), bf),
            pltpu.VMEM((2, 2, tok // 4, width), bf),
            pltpu.VMEM((2, tok // 4, width), bf),
            pltpu.VMEM((tok // 4, width), bf),
            pltpu.VMEM((tok // 4, width), bf),
            dma((14,)),
            dma((2,)),
            dma((2, 3)),
            dma((2, 2)),
            dma((2,)),
            dma((5, CHUNKS)),
            dma((2,)),
            dma((6, CHUNKS)),
            dma((8,)),
            dma((2, 2, CHUNKS)),
            dma((8,)),
            dma((2, CHUNKS)),
            dma((6, CHUNKS)),
            dma((7,)),
            dma((2, CHUNKS)),
            dma((2, CHUNKS)),
            dma((2, CHUNKS)),
            dma((1, CHUNKS)),
            dma((2, 2)),
        ],
        compiler_params=pltpu.CompilerParams(
            collective_id=0, has_side_effects=True, vmem_limit_bytes=62 * 1024 * 1024
        ),
    )(
        x,
        x_gain.reshape(1, width),
        jnp.transpose(routes),
        jnp.transpose(route_weight),
        queries,
        keys,
        values,
        q_gain.reshape(1, -1),
        k_gain.reshape(1, -1),
        jnp.asarray(turn_table(n * tok)),
        gate_weight,
        up_weight,
        down_weight,
        out_weight.reshape(pairs, 128, width),
    )


def plain_shards(
    queries,
    keys,
    values,
    query_gain,
    key_gain,
    out_weight,
    expert_input,
    norm_gain,
    routes,
    route_weight,
    gate_weight,
    up_weight,
    down_weight,
):
    tok_mix = queries.shape[0]
    head_count = query_gain.shape[0] // HEAD_DIM
    kv_count = key_gain.shape[0] // HEAD_DIM
    group_size = head_count // kv_count
    offset = lax.axis_index("ep") * tok_mix
    q_turned = head_norm(queries, query_gain, head_count, offset)
    k_turned = head_norm(keys, key_gain, kv_count, offset)
    grouped = q_turned.reshape(tok_mix, kv_count, group_size, HEAD_DIM)
    score_scale = HEAD_DIM ** (-0.5)
    start_state = (
        jnp.full((kv_count, group_size, tok_mix), -jnp.inf, jnp.float32),
        jnp.zeros((kv_count, group_size, tok_mix), jnp.float32),
        jnp.zeros((tok_mix, kv_count, group_size, HEAD_DIM), jnp.float32),
    )
    running = start_state
    key_piece = lax.all_gather(k_turned, "ep", axis=0, tiled=True)
    value_piece = lax.all_gather(values, "ep", axis=0, tiled=True)
    length = key_piece.shape[0]
    block_len = length
    while block_len > 2048 and block_len % 2 == 0:
        block_len = block_len // 2
    key_blocks = key_piece.reshape(length // block_len, block_len, key_piece.shape[1])
    value_blocks = value_piece.reshape(length // block_len, block_len, value_piece.shape[1])

    def advance(inner_state, key_value):
        return (absorb(inner_state, key_value[0], key_value[1], grouped, score_scale), None)

    running, unused = lax.scan(advance, running, (key_blocks, value_blocks))
    final_max, weight_sum, summed = running
    attended = (
        (summed / jnp.transpose(weight_sum, (2, 0, 1))[..., None])
        .reshape(tok_mix, -1)
        .astype(jnp.bfloat16)
    )
    mixed = lax.psum_scatter(
        jnp.dot(attended, out_weight, preferred_element_type=jnp.float32).astype(jnp.bfloat16),
        "tp",
        scatter_dimension=0,
        tiled=True,
    )
    tok_exp = expert_input.shape[0]
    top_count = routes.shape[1]
    expert_count = lax.axis_size("ep")
    capacity = 2 * top_count * tok_exp // expert_count
    as_float = expert_input.astype(jnp.float32)
    normed = (
        as_float
        * lax.rsqrt(jnp.mean(as_float * as_float, axis=-1, keepdims=True) + NORM_EPS)
        * norm_gain
    ).astype(jnp.bfloat16)
    flat_routes = routes.reshape(-1)
    route_hits = (
        flat_routes[:, None] == jnp.arange(expert_count, dtype=jnp.int32)[None, :]
    ).astype(jnp.int32)
    slot_rank = jnp.sum((jnp.cumsum(route_hits, axis=0) - route_hits) * route_hits, axis=1)
    slot_ids = flat_routes * capacity + slot_rank
    placed = jnp.arange(expert_count * capacity, dtype=jnp.int32)[:, None] == slot_ids[None, :]
    placed = jnp.any(placed.reshape(expert_count * capacity, tok_exp, top_count), axis=2).astype(
        jnp.bfloat16
    )
    outbound = jnp.dot(placed, normed, preferred_element_type=jnp.float32).astype(jnp.bfloat16)
    model_width = outbound.shape[1]
    half_cap = capacity // 2
    laid = outbound.reshape(expert_count, capacity, model_width)
    first_half = run_experts(
        laid[:, :half_cap].reshape(expert_count * half_cap, model_width),
        gate_weight,
        up_weight,
        down_weight,
    )
    second_half = run_experts(
        laid[:, half_cap:].reshape(expert_count * half_cap, model_width),
        gate_weight,
        up_weight,
        down_weight,
    )
    back_rows = jnp.concatenate(
        [
            first_half.reshape(expert_count, half_cap, model_width),
            second_half.reshape(expert_count, half_cap, model_width),
        ],
        axis=1,
    )
    back_rows = back_rows.reshape(expert_count * capacity, model_width)
    picked = back_rows[slot_ids.reshape(tok_exp, top_count)]
    moe_out = jnp.sum(picked.astype(jnp.float32) * route_weight[:, :, None], axis=1).astype(
        jnp.bfloat16
    )
    return (mixed, moe_out)


def shards(
    queries,
    keys,
    values,
    query_gain,
    key_gain,
    out_weight,
    expert_input,
    norm_gain,
    routes,
    route_weight,
    gate_weight,
    up_weight,
    down_weight,
):
    tok_exp = expert_input.shape[0]
    top_count = routes.shape[1]
    expert_count = lax.axis_size("ep")
    capacity = 2 * top_count * tok_exp // expert_count
    if capacity % 16 != 0 or lax.axis_size("tp") != 4 or expert_count != 8:
        return plain_shards(
            queries,
            keys,
            values,
            query_gain,
            key_gain,
            out_weight,
            expert_input,
            norm_gain,
            routes,
            route_weight,
            gate_weight,
            up_weight,
            down_weight,
        )
    moe_out, mixed = fused(
        expert_input,
        norm_gain,
        routes,
        route_weight,
        queries,
        keys,
        values,
        query_gain,
        key_gain,
        gate_weight[0],
        up_weight[0],
        down_weight[0],
        out_weight,
    )
    return (mixed, moe_out)


def solution(mesh):
    placed = (
        P("ep", "tp"),
        P("ep", "tp"),
        P("ep", "tp"),
        P("tp"),
        P("tp"),
        P("tp", None),
        P(("ep", "tp"), None),
        P(),
        P(("ep", "tp"), None),
        P(("ep", "tp"), None),
        P("ep", None, "tp"),
        P("ep", None, "tp"),
        P("ep", "tp", None),
    )
    return jax.shard_map(
        shards,
        mesh=mesh,
        in_specs=placed,
        out_specs=(P(("ep", "tp"), None), P(("ep", "tp"), None)),
        check_vma=False,
    )
```
